32 devices in a mesh: sp: 16 (over z, y, x), tp: 2 (over core).
Axes of the slice: x: 2, y: 2, z: 4, core: 2. Of those that a mesh axis runs over, the one named last changes fastest.
Arguments:
- stream: bfloat16 [2048, 2048], P(('sp', 'tp')), may hold values from -6 to 6
- wide_head_query: bfloat16 [2048, 1024], P('sp', 'tp'), may hold values from -6 to 6
- broad_attention_lookup_vectors: bfloat16 [2048, 1024], P('sp', 'tp'), may hold values from -6 to 6
- values_wide: bfloat16 [2048, 2048], P('sp', 'tp'), may hold values from -6 to 6
- query_narrow: bfloat16 [2048, 512], P('sp', 'tp'), may hold values from -6 to 6
- keys_narrow: bfloat16 [2048, 512], P('sp', 'tp'), may hold values from -6 to 6
- values_narrow: bfloat16 [2048, 1024], P('sp', 'tp'), may hold values from -6 to 6
- gate_wide: bfloat16 [2048, 2048], P('sp', 'tp'), may hold values from -6 to 6
- gate_narrow: bfloat16 [2048, 1024], P('sp', 'tp'), may hold values from -6 to 6
- log_decay: float32 [2, 8, 2048], P(None, 'tp', 'sp'), may hold values from -1.2 to 0, as said below
- gain_wide: bfloat16 [2048], P('tp'), may hold values from 0.099609375 to 1.8984375
- gain_narrow: bfloat16 [1024], P('tp'), may hold values from 0.099609375 to 1.8984375
- out_wide: bfloat16 [2048, 2048], P('tp'), may hold values from -0.109375 to 0.109375
- out_narrow: bfloat16 [1024, 2048], P('tp'), may hold values from -0.109375 to 0.109375
- gain_mix: bfloat16 [2048], replicated, may hold values from 0.099609375 to 1.8984375
- gain_pre: bfloat16 [2048], replicated, may hold values from 0.099609375 to 1.8984375
- gain_post: bfloat16 [2048], replicated, may hold values from 0.099609375 to 1.8984375
- weight_gate: bfloat16 [2048, 5120], P('sp', 'tp'), may hold values from -0.125 to 0.125
- weight_lin: bfloat16 [2048, 5120], P('sp', 'tp'), may hold values from -0.125 to 0.125
- weight_down: bfloat16 [2048, 5120], P('sp', 'tp'), may hold values from -0.078125 to 0.078125
- taps_gate: bfloat16 [3, 5120], P(None, 'tp'), may hold values from -3 to 3
- taps_lin: bfloat16 [3, 5120], P(None, 'tp'), may hold values from -3 to 3
Outputs:
- stream_out: bfloat16 [2048, 2048], P(('sp', 'tp'))
The draws below stay inside these ranges and needn't reach their ends.
Inputs may be any that keep to these rules, and one draw needn't show every extreme that they name: `log_decay`: the natural logarithm of the factor by which one head's retained state is multiplied at one position.
All inputs are finite; a program needn't handle non-finite values.
Results may differ from the reference program's by a relative error of at most 0.023.
Values may be sent and summed in bfloat16 or wider, within the bound.
A program may use at most 128 MiB of HBM per device.

```python
import math
import jax
import jax.numpy as jnp
from jax import lax

D = 2048
HEADS = 8
KW = 128
VW = 256
KN = 64
VN = 128
FF = 5120
CONV = 3
BLOCK = 128
TOKENS = 2048
N_TP = 2


def draw_log_decay(key, part):
    keys = jax.random.split(jax.random.fold_in(key, 11), 6)
    fast_share = 0.5
    fast = jax.random.uniform(keys[0], (2, HEADS, 1), jnp.float32) < fast_share
    fast_rate = jnp.exp(jax.random.uniform(keys[1], (2, HEADS, 1), jnp.float32, math.log(1.0 / 60.0), math.log(1.0 / 20.0)))
    slow_rate = jnp.exp(jax.random.uniform(keys[2], (2, HEADS, 1), jnp.float32, math.log(0.15), math.log(0.6))) / TOKENS
    forgetting_speed = jnp.where(fast, fast_rate, slow_rate)
    layer_groups_list = TOKENS // BLOCK
    multiplier_coefficient = jnp.exp(jax.random.uniform(keys[3], (2, HEADS, layer_groups_list), jnp.float32, math.log(0.5), math.log(2.0)))
    multiplier_coefficient = jnp.repeat(multiplier_coefficient, BLOCK, axis=2)
    spots = jax.random.randint(keys[4], (2, HEADS, 2), 0, TOKENS)
    layer_number_total = jnp.log(1.0 - jax.random.uniform(keys[5], (2, HEADS, 2), jnp.float32, 0.2, 0.4))
    agreeing_tally = spots[..., None] == jnp.arange(TOKENS, dtype=jnp.int32)[None, None, None, :]
    segment_span = jnp.sum(jnp.where(agreeing_tally, layer_number_total[..., None], 0.0), axis=2)
    return (-forgetting_speed * multiplier_coefficient + segment_span).astype(jnp.float32)


def steps_of(rng, extent, cuts, least, high):
    level, own = 1.0, jax.random.fold_in(rng, 6)
    for axis_at, parts in cuts:
        draws = jnp.exp(jax.random.uniform(jax.random.fold_in(own, axis_at), (parts,), jnp.float32, least / len(cuts), high / len(cuts)))
        level = level * jnp.repeat(draws, extent[axis_at] // parts).reshape([-1 if axis == axis_at else 1 for axis in range(len(extent))])
    return level


def bell_draw(stream_key, dims, deviation, bound, cuts=(), kind=jnp.bfloat16):
    values = jax.random.normal(stream_key, dims, jnp.float32) * deviation
    if len(cuts) > 0:
        values = steps_of(stream_key, dims, cuts, -0.22, 0.18) * values
    return jnp.clip(values, min=-bound, max=bound).astype(kind)


def setup_inputs(seed: int = 0) -> dict:
    seeds = jax.random.split(jax.random.key(seed), 23)
    stream = bell_draw(seeds[0], (TOKENS, D), 1.0, 6.0, ((0, 32),))
    wide_head_query = bell_draw(seeds[1], (TOKENS, HEADS * KW), 1.0, 6.0, ((0, 16), (1, 2)))
    broad_attention_lookup_vectors = bell_draw(seeds[2], (TOKENS, HEADS * KW), 1.0, 6.0, ((0, 16), (1, 2)))
    values_wide = bell_draw(seeds[3], (TOKENS, HEADS * VW), 1.0, 6.0, ((0, 16), (1, 2)))
    query_narrow = bell_draw(seeds[4], (TOKENS, HEADS * KN), 1.0, 6.0, ((0, 16), (1, 2)))
    keys_narrow = bell_draw(seeds[5], (TOKENS, HEADS * KN), 1.0, 6.0, ((0, 16), (1, 2)))
    values_narrow = bell_draw(seeds[6], (TOKENS, HEADS * VN), 1.0, 6.0, ((0, 16), (1, 2)))
    gate_wide = bell_draw(seeds[7], (TOKENS, HEADS * VW), 1.0, 6.0, ((0, 16), (1, 2)))
    gate_narrow = bell_draw(seeds[8], (TOKENS, HEADS * VN), 1.0, 6.0, ((0, 16), (1, 2)))
    log_decay = draw_log_decay(jax.random.fold_in(seeds[22], 71), 0)
    gain_wide = jnp.clip(1.0 + 0.18 * jax.random.normal(seeds[10], (HEADS * VW,), jnp.float32), 0.099609375, 1.8984375).astype(jnp.bfloat16)
    gain_narrow = jnp.clip(1.0 + 0.18 * jax.random.normal(seeds[11], (HEADS * VN,), jnp.float32), 0.099609375, 1.8984375).astype(jnp.bfloat16)
    out_wide = bell_draw(seeds[12], (HEADS * VW, D), (HEADS * (VW + VN)) ** -0.5, 0.109375, ((0, 2),))
    out_narrow = bell_draw(seeds[13], (HEADS * VN, D), (HEADS * (VW + VN)) ** -0.5, 0.109375, ((0, 2),))
    gain_mix = jnp.clip(1.0 + 0.18 * jax.random.normal(seeds[14], (D,), jnp.float32), 0.099609375, 1.8984375).astype(jnp.bfloat16)
    gain_pre = jnp.clip(1.0 + 0.18 * jax.random.normal(seeds[15], (D,), jnp.float32), 0.099609375, 1.8984375).astype(jnp.bfloat16)
    gain_post = jnp.clip(1.0 + 0.18 * jax.random.normal(seeds[16], (D,), jnp.float32), 0.099609375, 1.8984375).astype(jnp.bfloat16)
    weight_gate = bell_draw(seeds[17], (D, FF), D ** -0.5, 0.125, ((0, 16), (1, 2)))
    weight_lin = bell_draw(seeds[18], (D, FF), D ** -0.5, 0.125, ((0, 16), (1, 2)))
    weight_down = bell_draw(seeds[19], (D, FF), FF ** -0.5, 0.078125, ((0, 16), (1, 2)))
    taps_gate = bell_draw(seeds[20], (CONV, FF), 0.58, 3.0, ((1, 2),))
    taps_lin = bell_draw(seeds[21], (CONV, FF), 0.58, 3.0, ((1, 2),))
    return dict(stream=stream, wide_head_query=wide_head_query, broad_attention_lookup_vectors=broad_attention_lookup_vectors, values_wide=values_wide, query_narrow=query_narrow, keys_narrow=keys_narrow, values_narrow=values_narrow, gate_wide=gate_wide, gate_narrow=gate_narrow, log_decay=log_decay, gain_wide=gain_wide, gain_narrow=gain_narrow, out_wide=out_wide, out_narrow=out_narrow, gain_mix=gain_mix, gain_pre=gain_pre, gain_post=gain_post, weight_gate=weight_gate, weight_lin=weight_lin, weight_down=weight_down, taps_gate=taps_gate, taps_lin=taps_lin)


EPS = 1e-06
THETA = 10000.0

def rotate(block, positions):
    width = block.shape[-1]
    half = width // 2
    frequency = THETA ** (-(jnp.arange(half, dtype=jnp.float32) * 2.0 / width))
    angles = positions.astype(jnp.float32)[:, None] * frequency[None, :]
    cosine = jnp.cos(angles)[:, None, :]
    sine = jnp.sin(angles)[:, None, :]
    values = block.astype(jnp.float32)
    first = values[..., :half]
    second = values[..., half:]
    return jnp.concatenate([first * cosine - second * sine, second * cosine + first * sine], axis=-1)

def block_step(state, inputs):
    query, keys, values, log_rate = inputs
    running = jnp.cumsum(log_rate, axis=1)
    length = running.shape[1]
    index = jnp.arange(length)
    lower = (index[:, None] >= index[None, :])[None]
    spread = jnp.where(lower, jnp.exp(jnp.where(lower, running[:, :, None] - running[:, None, :], 0.0)), 0.0)
    query_f = query.astype(jnp.float32)
    values_f = values.astype(jnp.float32)
    scores = jnp.einsum('ihd,jhd->hij', query_f, keys.astype(jnp.float32), precision=lax.Precision.HIGHEST) * spread
    scores = lax.optimization_barrier(scores.astype(jnp.bfloat16)).astype(jnp.float32)
    inner = jnp.einsum('hij,jhe->ihe', scores, values_f, precision=lax.Precision.HIGHEST)
    lifted = query_f * jnp.exp(running).T[:, :, None]
    cross = jnp.einsum('ihd,hde->ihe', lifted, state, precision=lax.Precision.HIGHEST)
    tail = running[:, -1:]
    scaled = keys.astype(jnp.float32) * jnp.exp(tail - running).T[:, :, None]
    scaled = lax.optimization_barrier(scaled.astype(jnp.bfloat16)).astype(jnp.float32)
    update = jnp.einsum('jhd,jhe->hde', scaled, values_f, precision=lax.Precision.HIGHEST)
    state = state * jnp.exp(tail)[:, :, None] + update
    return (state, inner + cross)

def retain(query, keys, values, log_rate, head_dim, value_dim):
    total = query.shape[0]
    heads = query.shape[1] // head_dim
    positions = jnp.arange(total, dtype=jnp.int32)
    rotated_query = rotate(query.reshape(total, heads, head_dim), positions).astype(jnp.bfloat16)
    rotated_keys = (rotate(keys.reshape(total, heads, head_dim), positions) * head_dim ** (-0.5)).astype(jnp.bfloat16)
    layer_groups_list = total // BLOCK

    def split(array):
        return array.reshape(layer_groups_list, BLOCK, heads, array.shape[-1])
    rates = jnp.transpose(log_rate.reshape(heads, layer_groups_list, BLOCK), (1, 0, 2))
    start = jnp.zeros((heads, head_dim, value_dim), jnp.float32)
    inputs = (split(rotated_query), split(rotated_keys), split(values.reshape(total, heads, value_dim)), rates)
    _, outs = lax.scan(block_step, start, inputs)
    return outs.reshape(total, heads, value_dim)

def gate_heads(retained, gain, gate):
    mean = lax.optimization_barrier(jnp.mean(retained, axis=-1, keepdims=True))
    centred = retained - mean
    variance = lax.optimization_barrier(jnp.mean(centred * centred, axis=-1, keepdims=True))
    normed = (centred * lax.rsqrt(variance + EPS)).reshape(retained.shape[0], -1)
    return (normed * gain.astype(jnp.float32) * jax.nn.silu(gate.astype(jnp.float32))).astype(jnp.bfloat16)

def scale_rows(rows, gain):
    return rows * lax.rsqrt(lax.optimization_barrier(jnp.mean(rows * rows, axis=-1, keepdims=True)) + EPS) * gain.astype(jnp.float32)

def causal_taps(upward, taps):
    width = taps.shape[0]
    total = upward.shape[0]
    padded_rows = jnp.concatenate([jnp.zeros((width - 1, upward.shape[1]), upward.dtype), upward], axis=0).astype(jnp.float32)
    smooth = jnp.zeros((total, upward.shape[1]), jnp.float32)
    for tap_index in range(width):
        smooth = smooth + taps[tap_index].astype(jnp.float32)[None, :] * padded_rows[tap_index:tap_index + total]
    return smooth

def reference(stream, wide_head_query, broad_attention_lookup_vectors, values_wide, query_narrow, keys_narrow, values_narrow, gate_wide, gate_narrow, log_decay, gain_wide, gain_narrow, out_wide, out_narrow, gain_mix, gain_pre, gain_post, weight_gate, weight_lin, weight_down, taps_gate, taps_lin):
    wide = gate_heads(retain(wide_head_query, broad_attention_lookup_vectors, values_wide, log_decay[0], KW, VW), gain_wide, gate_wide)
    narrow = gate_heads(retain(query_narrow, keys_narrow, values_narrow, log_decay[1], KN, VN), gain_narrow, gate_narrow)
    share = HEADS // N_TP
    mixed = jnp.zeros((TOKENS, D), jnp.float32)
    for group in range(N_TP):
        lo_wide, hi_wide = (group * share * VW, (group + 1) * share * VW)
        lo_narrow, hi_narrow = (group * share * VN, (group + 1) * share * VN)
        partial_sum = jnp.dot(wide[:, lo_wide:hi_wide], out_wide[lo_wide:hi_wide], preferred_element_type=jnp.float32)
        partial_sum = partial_sum + jnp.dot(narrow[:, lo_narrow:hi_narrow], out_narrow[lo_narrow:hi_narrow], preferred_element_type=jnp.float32)
        mixed = mixed + lax.optimization_barrier(partial_sum.astype(jnp.bfloat16)).astype(jnp.float32)
    resid = lax.optimization_barrier((stream.astype(jnp.float32) + scale_rows(mixed, gain_mix)).astype(jnp.bfloat16))
    normed_in = scale_rows(resid.astype(jnp.float32), gain_pre).astype(jnp.bfloat16)
    up_gate = jnp.dot(normed_in, weight_gate, preferred_element_type=jnp.float32).astype(jnp.bfloat16)
    up_lin = jnp.dot(normed_in, weight_lin, preferred_element_type=jnp.float32).astype(jnp.bfloat16)
    smooth_gate = causal_taps(up_gate, taps_gate)
    smooth_lin = causal_taps(up_lin, taps_lin)
    hidden = (jax.nn.silu(smooth_gate) * smooth_lin).astype(jnp.bfloat16)
    units = FF // N_TP
    fed = jnp.zeros((TOKENS, D), jnp.float32)
    for group in range(N_TP):
        partial_sum = lax.dot_general(hidden[:, group * units:(group + 1) * units], weight_down[:, group * units:(group + 1) * units], (((1,), (1,)), ((), ())), preferred_element_type=jnp.float32)
        fed = fed + lax.optimization_barrier(partial_sum.astype(jnp.bfloat16)).astype(jnp.float32)
    return (resid.astype(jnp.float32) + scale_rows(fed, gain_post)).astype(jnp.bfloat16)
```

```python
import functools

import jax
import jax.numpy as jnp
import numpy as np
from jax import lax
from jax.experimental import pallas as pl
from jax.experimental.pallas import tpu as pltpu
from jax.sharding import PartitionSpec as P

KW = 128
VW = 256
KN = 64
VN = 128
BLOCK = 128


EPS = 1e-06
THETA = 10000.0
LANES = 128
PAD = 16
VMEM_BYTES = 60 * 2**20


def passed_along(value, axis, steps):
    count = lax.axis_size(axis)
    first, last = (max(0, -steps), min(count, count - steps))
    return lax.ppermute(value, axis, [(source, source + steps) for source in range(first, last)])


def rotate(block, positions):
    width = block.shape[-1]
    half = width // 2
    frequency = THETA ** (-(jnp.arange(half, dtype=jnp.float32) * 2.0 / width))
    angles = positions.astype(jnp.float32)[:, None] * frequency[None, :]
    cosine = jnp.cos(angles)[:, None, :]
    sine = jnp.sin(angles)[:, None, :]
    values = block.astype(jnp.float32)
    first = values[..., :half]
    second = values[..., half:]
    return jnp.concatenate(
        [first * cosine - second * sine, second * cosine + first * sine], axis=-1
    )


def block_step(state, inputs):
    query, keys, values, log_rate = inputs
    running = jnp.cumsum(log_rate, axis=1)
    length = running.shape[1]
    index = jnp.arange(length)
    lower = (index[:, None] >= index[None, :])[None]
    spread = jnp.where(
        lower, jnp.exp(jnp.where(lower, running[:, :, None] - running[:, None, :], 0.0)), 0.0
    )
    scores = (
        jnp.einsum("ihd,jhd->hij", query, keys, preferred_element_type=jnp.float32) * spread
    ).astype(jnp.bfloat16)
    inner = jnp.einsum("hij,jhe->ihe", scores, values, preferred_element_type=jnp.float32)
    lifted = query.astype(jnp.float32) * jnp.exp(running).T[:, :, None]
    cross = jnp.einsum("ihd,hde->ihe", lifted, state, precision=lax.Precision.HIGHEST)
    tail = running[:, -1:]
    scaled = (keys.astype(jnp.float32) * jnp.exp(tail - running).T[:, :, None]).astype(jnp.bfloat16)
    update = jnp.einsum("jhd,jhe->hde", scaled, values, preferred_element_type=jnp.float32)
    state = state * jnp.exp(tail)[:, :, None] + update
    return (state, inner + cross)


def kept_nearby_memory(query, keys, values, log_rate, head_dim, value_dim, offset):
    rows = query.shape[0]
    heads = query.shape[1] // head_dim
    positions = offset + jnp.arange(rows, dtype=jnp.int32)
    rotated_query = rotate(query.reshape(rows, heads, head_dim), positions).astype(jnp.bfloat16)
    rotated_keys = (
        rotate(keys.reshape(rows, heads, head_dim), positions) * head_dim ** (-0.5)
    ).astype(jnp.bfloat16)
    layer_groups_list = rows // BLOCK

    def split(array):
        return array.reshape(layer_groups_list, BLOCK, heads, array.shape[-1])

    rates = jnp.transpose(log_rate.reshape(heads, layer_groups_list, BLOCK), (1, 0, 2))
    start = jnp.zeros((heads, head_dim, value_dim), jnp.float32)
    inputs = (
        split(rotated_query),
        split(rotated_keys),
        split(values.reshape(rows, heads, value_dim)),
        rates,
    )
    state, outs = lax.scan(block_step, start, inputs)
    return (rotated_query, outs.reshape(rows, heads, value_dim), state)


def carried(rotated_query, log_rate, state_in):
    lifted = rotated_query.astype(jnp.float32) * jnp.exp(jnp.cumsum(log_rate, axis=1)).T[:, :, None]
    return jnp.einsum("ihd,hde->ihe", lifted, state_in, precision=lax.Precision.HIGHEST)


def gate_heads(retained, gain, gate):
    mean = jnp.mean(retained, axis=-1, keepdims=True)
    centred = retained - mean
    variance = jnp.mean(centred * centred, axis=-1, keepdims=True)
    normed = (centred * lax.rsqrt(variance + EPS)).reshape(retained.shape[0], -1)
    return (normed * gain.astype(jnp.float32) * jax.nn.silu(gate.astype(jnp.float32))).astype(
        jnp.bfloat16
    )


def scale_rows(rows, gain):
    return (
        rows
        * lax.rsqrt(jnp.mean(rows * rows, axis=-1, keepdims=True) + EPS)
        * gain.astype(jnp.float32)
    )


def causal_taps(upward, before, taps):
    width = taps.shape[0]
    total = upward.shape[0]
    padded_rows = jnp.concatenate([before, upward], axis=0).astype(jnp.float32)
    smooth = jnp.zeros((total, upward.shape[1]), jnp.float32)
    for tap_index in range(width):
        smooth = (
            smooth
            + taps[tap_index].astype(jnp.float32)[None, :]
            * padded_rows[tap_index : tap_index + total]
        )
    return smooth


def swap_blocks(blocks, axis):
    return lax.all_to_all(blocks, axis, 0, 0, tiled=False)


def share_rows(parts, axis):
    count = lax.axis_size(axis)
    place = lax.axis_index(axis)
    total = lax.dynamic_index_in_dim(parts, place, 0, False).astype(jnp.float32)
    for step in range(1, count):
        piece = lax.dynamic_index_in_dim(parts, (place + step) % count, 0, False)
        moved = lax.ppermute(piece, axis, [(i, (i + step) % count) for i in range(count)])
        total = total + moved.astype(jnp.float32)
    return total


def carried_in(states, totals, axis):
    count = lax.axis_size(axis)
    lanes = states[-1].shape[-1]
    flat = jnp.concatenate([s.reshape(-1, lanes) for s in states]).astype(jnp.bfloat16)
    rates = jnp.concatenate(
        [jnp.repeat(d, s.size // s.shape[0] // lanes) for s, d in zip(states, totals)]
    )
    share = flat.shape[0] // count
    rates = rates.reshape(count, share)
    rates = jnp.pad(rates, ((0, 0), (0, -share % lanes)))
    parts, left = [], rates
    for _ in range(3):
        parts.append(left.astype(jnp.bfloat16))
        left = left - parts[-1].astype(jnp.float32)
    parts = [part.reshape(count, -1, lanes) for part in parts]
    sent = jnp.concatenate([flat.reshape(count, share, lanes)] + parts, axis=1)
    got = swap_blocks(sent, axis).astype(jnp.float32)
    parts = jnp.split(got[:, share:], 3, axis=1)
    logs = (parts[0] + parts[1] + parts[2]).reshape(count, -1)[:, :share]
    own = got[:, :share]
    steps = jnp.arange(count)
    between = (steps[None, None] > steps[None, :, None]) & (
        steps[None, None] < steps[:, None, None]
    )
    span = jnp.sum(jnp.where(between[..., None], logs[None, None], 0.0), axis=2)
    factor = jnp.where((steps[None] < steps[:, None])[..., None], jnp.exp(span), 0.0)
    before = sum(factor[:, step, :, None] * own[step][None] for step in range(count))
    back = swap_blocks(before.astype(jnp.bfloat16), axis).reshape(-1, lanes).astype(jnp.float32)
    outs, at = [], 0
    for s in states:
        rows = s.size // lanes
        outs.append(back[at : at + rows].reshape(s.shape))
        at += rows
    return outs


def feed_by_weights(normed_in, weight_gate, weight_lin, weight_down, taps_gate, taps_lin):
    normed_all = lax.all_gather(normed_in, "tp", axis=0, tiled=True)
    rows = normed_all.shape[0]
    whole_gate, whole_lin = (
        lax.all_gather(weight_gate, "sp", axis=0, tiled=True),
        lax.all_gather(weight_lin, "sp", axis=0, tiled=True),
    )
    up_gate = jnp.dot(normed_all, whole_gate, preferred_element_type=jnp.float32).astype(
        jnp.bfloat16
    )
    up_lin = jnp.dot(normed_all, whole_lin, preferred_element_type=jnp.float32).astype(jnp.bfloat16)
    reach = taps_gate.shape[0] - 1
    before_gate, before_lin = passed_along(
        (up_gate[rows - reach :], up_lin[rows - reach :]), "sp", 1
    )
    smooth_gate = causal_taps(up_gate, before_gate, taps_gate)
    smooth_lin = causal_taps(up_lin, before_lin, taps_lin)
    hidden = (jax.nn.silu(smooth_gate) * smooth_lin).astype(jnp.bfloat16)
    terms = lax.dot_general(
        hidden,
        lax.all_gather(weight_down, "sp", axis=0, tiled=True),
        (((1,), (1,)), ((), ())),
        preferred_element_type=jnp.float32,
    )
    return lax.psum_scatter(
        terms.astype(jnp.bfloat16), "tp", scatter_dimension=0, tiled=True
    ).astype(jnp.float32)


def from_all(value, axis, dim):
    count = lax.axis_size(axis)
    found = [value]
    for step in range(1, count):
        found.append(lax.ppermute(value, axis, [(i, (i + step) % count) for i in range(count)]))
    return jnp.concatenate(found, axis=dim)


def unit_slices(weight_gate, weight_lin, weight_down, taps_gate, taps_lin):
    count = lax.axis_size("sp")
    place = lax.axis_index("sp")
    deep, units = weight_gate.shape
    share = units // count
    turned = jnp.stack([weight_gate.T, weight_lin.T, weight_down.T])
    blocks = turned.reshape(3, count, share, deep).transpose(1, 0, 2, 3)
    got = swap_blocks(blocks, "sp")
    mine = got.transpose(1, 2, 0, 3).reshape(3, share, count * deep)
    taps = jnp.stack([taps_gate, taps_lin])
    taps = lax.dynamic_slice_in_dim(taps, place * share, share, 2)
    return from_all(mine, "tp", 1), from_all(taps, "tp", 2)


def flip(value, axis, bit):
    return lax.ppermute(
        value, axis, [(i, i ^ (1 << bit)) for i in range(lax.axis_size(axis))]
    )


def bits_of(count, swapped):
    bits = list(range(count.bit_length() - 1))
    if swapped:
        bits[:2] = bits[:2][::-1]
    return bits


def gather_around(value, axis, swapped):
    bits = bits_of(lax.axis_size(axis), swapped)
    for bit in bits[::-1]:
        value = jnp.stack([value, flip(value, axis, bit)])
    order = [bits.index(bit) for bit in sorted(bits, reverse=True)]
    value = value.transpose(*order, *range(len(bits), value.ndim))
    return value.reshape(-1, *value.shape[len(bits) :])


def add_around(value, axis, swapped):
    bits = bits_of(lax.axis_size(axis), swapped)
    value = value.reshape(*[2] * len(bits), *value.shape[1:])
    dims = sorted(bits, reverse=True)
    for bit in bits:
        at = dims.index(bit)
        dims.remove(bit)
        kept = lax.index_in_dim(value, 0, at, False).astype(jnp.float32)
        sent = lax.index_in_dim(value, 1, at, False).astype(jnp.bfloat16)
        value = kept + flip(sent, axis, bit).astype(jnp.float32)
        if dims:
            value = value.astype(jnp.bfloat16)
    return value


def feed_by_tokens(normed_in, weights, taps):
    count = lax.axis_size("sp")
    n_tp = lax.axis_size("tp")
    rows, width = normed_in.shape
    place = lax.axis_index("sp")
    half = width // 2
    flat = weights[:2].reshape(-1, width)
    units = flat.shape[0] // 2
    ups = 0.0
    for part in range(2):
        cut = slice(part * half, (part + 1) * half)
        tokens = gather_around(normed_in[:, cut], "sp", part == 1)
        ups = ups + lax.dot_general(
            tokens.reshape(count * rows, half),
            flat[:, cut],
            (((1,), (1,)), ((), ())),
            preferred_element_type=jnp.float32,
        )
    ups = ups.astype(jnp.bfloat16).reshape(count, rows, 2 * units)
    reach = taps.shape[1] - 1
    tails = ups[:, rows - reach :]
    prior = lax.ppermute(tails, "tp", [(i, (i + 1) % n_tp) for i in range(n_tp)])
    prior = jnp.roll(prior.reshape(count, reach, 2, n_tp, -1), 1, axis=3).reshape(prior.shape)
    blocks = place ^ jnp.arange(count)
    follows = (blocks[:, None] == blocks[None, :] + 1).astype(jnp.bfloat16)
    shifted = jnp.dot(
        follows, prior.reshape(count, -1), preferred_element_type=jnp.float32
    ).astype(jnp.bfloat16).reshape(prior.shape)
    prior = jnp.where(lax.axis_index("tp") == 0, shifted, prior)
    padded = jnp.concatenate([prior, ups], axis=1).astype(jnp.float32)
    taps = jnp.concatenate([taps[0], taps[1]], axis=1).astype(jnp.float32)
    smooth = sum(taps[j] * padded[:, j : j + rows] for j in range(reach + 1))
    hidden = (jax.nn.silu(smooth[..., :units]) * smooth[..., units:]).astype(jnp.bfloat16)
    hidden = hidden.reshape(count * rows, units)
    sums = []
    for part in range(2):
        cut = slice(part * half, (part + 1) * half)
        terms = jnp.dot(hidden, weights[2][:, cut], preferred_element_type=jnp.float32)
        terms = terms.astype(jnp.bfloat16).reshape(count, rows, half)
        sums.append(add_around(terms, "sp", part == 1))
    return jnp.concatenate(sums, axis=1)


def tables_of(count, rows):
    def angles(positions, width):
        half = width // 2
        frequency = THETA ** (-(np.arange(half, dtype=np.float64) * 2.0 / width))
        return np.tile(positions[:, None] * frequency[None, :], (1, LANES // half))

    positions = np.concatenate([np.arange(rows), np.arange(count) * rows]).astype(np.float64)
    found = []
    for width in (KW, KN):
        turned = angles(positions, width)
        found += [np.cos(turned), np.sin(turned)]
    return np.stack(found).astype(np.float32)


def remote(source, target, sent, got, sp, tp):
    return pltpu.make_async_remote_copy(
        src_ref=source, dst_ref=target, send_sem=sent, recv_sem=got,
        device_id=(sp, tp), device_id_type=pl.DeviceIdType.MESH,
    )


def silu(value):
    return value / (1.0 + jnp.exp(-value))


def rms(value):
    return value * lax.rsqrt(jnp.mean(value * value, axis=-1, keepdims=True) + EPS)


def layer_kernel(
    dims,
    stream, q_wide, k_wide, v_wide, q_narrow, k_narrow, v_narrow, gate_wide, gate_narrow,
    decay, gain_wide, gain_narrow, gain_mix, gain_pre, gain_post, tables, taps_in,
    out_wide_hbm, out_narrow_hbm, turned_gate, turned_lin, turned_down,
    result,
    out_w, weights, tokens, terms, from_y, from_up, from_down, rotated, local, states, got,
    before, state_in, gated, logs_own, logs, taps_own, taps_got, mix_sent, mix_got, resid, tail_f, tail, halos, halo_f,
    padded, hidden,
    out_sem, own_sem, w_send, w_recv, xw_send, xw_recv, dw_send, dw_recv,
    log_send, log_recv, one_send, one_recv, two_send, two_recv, tap_sem, mix_sem,
    halo_send, halo_recv, up_send, dn_send, y_send, z_recv, y_recv,
    ry_send, ry_recv, ru_send, ru_recv, rd_send, rd_recv,
):
    count, n_tp = dims["count"], dims["n_tp"]
    rows, width = dims["rows"], dims["width"]
    half = rows // n_tp
    places = count // 2
    nz = count // 4
    share = dims["share"]
    units = n_tp * share
    piece = dims["piece"]
    parts = 2
    step_rows = half // parts
    pad = PAD
    me = lax.axis_index("sp")
    core = lax.axis_index("tp")
    other = 1 - core
    x = me % 2
    y = (me // 2) % 2
    z = me // 4
    place = me // 2
    x_mate = me + 1 - 2 * x
    y_mate = me + 2 - 4 * y
    mine = pl.multiple_of(me * LANES, LANES)

    def in_plane(k):
        at = (place + k) % places
        return at, 2 * at + x

    barrier = pltpu.get_barrier_semaphore()

    def greet(k, carry):
        to = (me * n_tp + core + k) % (count * n_tp)
        pl.semaphore_signal(
            barrier, inc=1, device_id=(to // n_tp, to % n_tp),
            device_id_type=pl.DeviceIdType.MESH,
        )
        return carry

    lax.fori_loop(1, count * n_tp, greet, 0)

    wide_rows = out_wide_hbm.shape[0]
    narrow_rows = out_narrow_hbm.shape[0]
    out_copies = [
        pltpu.make_async_copy(out_wide_hbm, out_w.at[pl.ds(0, wide_rows)], out_sem.at[0]),
        pltpu.make_async_copy(out_narrow_hbm, out_w.at[pl.ds(wide_rows, narrow_rows)], out_sem.at[1]),
    ]
    for copy in out_copies:
        copy.start()

    def own_rows(at):
        return pl.ds(pl.multiple_of(at * share, 16), share)

    turned = (turned_gate, turned_lin, turned_down)
    core_rows = pl.ds(pl.multiple_of(core * share, 16), share)

    def weight_copy(which, k):
        at, to = in_plane(k)
        return remote(
            turned[which].at[own_rows(at)], weights.at[which, core_rows, pl.ds(mine, LANES)],
            w_send.at[which, k], w_recv.at[which, k], to, core,
        )

    def weight_wait(which, k):
        from_at = (place + places - k) % places
        columns = pl.ds(pl.multiple_of((2 * from_at + x) * LANES, LANES), LANES)
        spot = weights.at[which, core_rows, columns]
        remote(spot, spot, w_send.at[which, k], w_recv.at[which, k], x_mate, core).wait_recv()

    def over_x(which, k):
        from_at = (place + places - k) % places
        columns = pl.ds(pl.multiple_of((2 * from_at + x) * LANES, LANES), LANES)
        spot = weights.at[which, core_rows, columns]
        return remote(spot, spot, xw_send.at[which, k], xw_recv.at[which, k], x_mate, core)

    def over_x_wait(which, k):
        from_at = (place + places - k) % places
        columns = pl.ds(pl.multiple_of((2 * from_at + 1 - x) * LANES, LANES), LANES)
        spot = weights.at[which, core_rows, columns]
        remote(spot, spot, xw_send.at[which, k], xw_recv.at[which, k], x_mate, core).wait_recv()

    def across(which):
        spot = weights.at[which, core_rows]
        return remote(spot, spot, dw_send.at[which], dw_recv.at[which], me, other)

    def across_wait(which):
        spot = weights.at[which, pl.ds(pl.multiple_of(other * share, 16), share)]
        remote(spot, spot, dw_send.at[which], dw_recv.at[which], me, other).wait_recv()

    def send_weights(which):
        def go(k, carry):
            weight_copy(which, k).start()
            return carry
        lax.fori_loop(1, places, go, 0)

    def own_copy(which):
        return pltpu.make_async_copy(
            turned[which].at[own_rows(place)], weights.at[which, core_rows, pl.ds(mine, LANES)],
            own_sem.at[which],
        )

    def forward_weights(which):
        own_copy(which).wait()
        over_x(which, 0).start()

        def go(k, carry):
            weight_wait(which, k)
            over_x(which, k).start()
            return carry
        lax.fori_loop(1, places, go, 0)

    def pass_weights(which):
        def go(k, carry):
            over_x_wait(which, k)
            return carry
        lax.fori_loop(0, places, go, 0)
        across(which).start()

    for which in range(3):
        own_copy(which).start()
    pl.semaphore_wait(barrier, count * n_tp - 1)
    send_weights(0)
    taps_copy = remote(taps_own, taps_got, tap_sem.at[0], tap_sem.at[1], me, other)
    taps_own[...] = taps_in[place]

    i_at = lax.broadcasted_iota(jnp.int32, (rows, rows), 0)
    j_at = lax.broadcasted_iota(jnp.int32, (rows, rows), 1)
    lower = i_at >= j_at
    lower_f = lower.astype(jnp.float32)
    upper_f = (i_at <= j_at).astype(jnp.float32)
    rates = decay[...]
    run_rows = lax.dot_general(
        rates, upper_f, (((1,), (0,)), ((), ())), precision=lax.Precision.HIGHEST,
        preferred_element_type=jnp.float32,
    )
    run_cols = lax.dot_general(
        lower_f, rates, (((1,), (1,)), ((), ())), precision=lax.Precision.HIGHEST,
        preferred_element_type=jnp.float32,
    )
    totals = run_rows[:, rows - 1 : rows]
    logs_own[...] = jnp.broadcast_to(totals, logs_own.shape)
    logs[me] = jnp.broadcast_to(totals, logs_own.shape)
    taps_copy.start()

    def peer(k):
        return (me + k) % count

    def log_copy(k):
        return remote(logs_own, logs.at[me], log_send.at[k], log_recv.at[k], peer(k), core)

    def send_logs(k, carry):
        log_copy(k).start()
        return carry

    heads = wide_rows // VW
    lane = lax.broadcasted_iota(jnp.int32, (rows, LANES), 1)

    def angle_table(first, half_width):
        cos_i, sin_i = tables[first, 0:rows, :], tables[first + 1, 0:rows, :]
        cos_o = tables[first, pl.ds(rows + me, 1), :]
        sin_o = tables[first + 1, pl.ds(rows + me, 1), :]
        cosine = cos_o * cos_i - sin_o * sin_i
        sine = sin_o * cos_i + cos_o * sin_i
        early = lane % (2 * half_width) < half_width
        return cosine, jnp.where(early, -sine, sine), early

    cos_w, sin_w, _ = angle_table(0, KW // 2)

    def dot(a, b, dims_):
        return lax.dot_general(a, b, (dims_, ((), ())), preferred_element_type=jnp.float32)

    def spread_of(column, row):
        return jnp.where(lower, jnp.exp(jnp.where(lower, column - row, 0.0)), 0.0)

    for h in range(heads):
        cut = slice(h * KW, (h + 1) * KW)
        query = q_wide[:, cut].astype(jnp.float32)
        query = (query * cos_w + pltpu.roll(query, KW // 2, 1) * sin_w).astype(jnp.bfloat16)
        keys = k_wide[:, cut].astype(jnp.float32)
        keys = ((keys * cos_w + pltpu.roll(keys, KW // 2, 1) * sin_w) * KW ** (-0.5)).astype(jnp.bfloat16)
        column, row = run_cols[:, h : h + 1], run_rows[h : h + 1, :]
        scores = (dot(query, keys, ((1,), (1,))) * spread_of(column, row)).astype(jnp.bfloat16)
        values = v_wide[:, h * VW : (h + 1) * VW]
        local[:, h * VW : (h + 1) * VW] = dot(scores, values, ((1,), (0,)))
        last = totals[h : h + 1, :]
        scaled = (keys.astype(jnp.float32) * jnp.exp(last - column)).astype(jnp.bfloat16)
        state = dot(scaled, values, ((0,), (0,))).astype(jnp.bfloat16)
        for e in range(VW // LANES):
            at = (h * (VW // LANES) + e) * KW
            states[at : at + KW, :] = state[:, e * LANES : (e + 1) * LANES]
        rotated[:, cut] = (query.astype(jnp.float32) * jnp.exp(column)).astype(jnp.bfloat16)

    cos_n, sin_n, early_n = angle_table(2, KN // 2)

    def swap_narrow(value):
        return jnp.where(
            early_n, pltpu.roll(value, LANES - KN // 2, 1), pltpu.roll(value, KN // 2, 1)
        )

    base_wide = wide_rows // LANES * KW
    first_head = lane < KN
    for g in range(heads // 2):
        cut = slice(g * LANES, (g + 1) * LANES)
        query = q_narrow[:, cut].astype(jnp.float32)
        query = (query * cos_n + swap_narrow(query) * sin_n).astype(jnp.bfloat16)
        keys = k_narrow[:, cut].astype(jnp.float32)
        keys = ((keys * cos_n + swap_narrow(keys) * sin_n) * KN ** (-0.5)).astype(jnp.bfloat16)
        spot = heads + 2 * g
        columns = [run_cols[:, spot + e : spot + e + 1] for e in range(2)]
        lasts = [totals[spot + e : spot + e + 1, :] for e in range(2)]
        falls = jnp.where(
            first_head, jnp.exp(lasts[0] - columns[0]), jnp.exp(lasts[1] - columns[1])
        )
        scaled = (keys.astype(jnp.float32) * falls).astype(jnp.bfloat16)
        rises = jnp.where(first_head, jnp.exp(columns[0]), jnp.exp(columns[1]))
        query_f = query.astype(jnp.float32)
        rotated[:, heads * KW + g * LANES : heads * KW + (g + 1) * LANES] = (
            query_f * rises
        ).astype(jnp.bfloat16)
        for e in range(2):
            h = 2 * g + e
            own = first_head if e == 0 else jnp.logical_not(first_head)
            masked = jnp.where(own, query_f, 0.0).astype(jnp.bfloat16)
            scores = (
                dot(masked, keys, ((1,), (1,)))
                * spread_of(columns[e], run_rows[spot + e : spot + e + 1, :])
            ).astype(jnp.bfloat16)
            values = v_narrow[:, h * VN : (h + 1) * VN]
            local[:, wide_rows + h * VN : wide_rows + (h + 1) * VN] = dot(scores, values, ((1,), (0,)))
            state = dot(scaled, values, ((0,), (0,))).astype(jnp.bfloat16)
            at = base_wide + h * KN
            states[at : at + KN, :] = state[e * KN : (e + 1) * KN, :]

    lax.fori_loop(1, count, send_logs, 0)

    def piece_rows(at):
        return pl.ds(pl.multiple_of(at * piece, 16), piece)

    def one_copy(k):
        return remote(
            states.at[piece_rows(peer(k))], got.at[me], one_send.at[k], one_recv.at[k],
            peer(k), core,
        )

    def send_one(k, carry):
        one_copy(k).start()
        return carry

    lax.fori_loop(1, count, send_one, 0)
    got[me] = states[piece_rows(me), :]
    forward_weights(0)

    def source(k):
        return (me + count - k) % count

    def wait_one(k, carry):
        at = source(k)
        remote(logs.at[at], logs.at[at], log_send.at[k], log_recv.at[k], at, core).wait_recv()
        remote(got.at[at], got.at[at], one_send.at[k], one_recv.at[k], at, core).wait_recv()
        return carry

    lax.fori_loop(1, count, wait_one, 0)
    groups_wide = VW // LANES * KW // 16
    groups_narrow = KN // 16
    for i in range(piece // 16):
        g = me * (piece // 16) + i
        head = jnp.where(
            g < heads * groups_wide, g // groups_wide,
            heads + (g - heads * groups_wide) // groups_narrow,
        )
        head = jnp.minimum(head, 2 * heads - 1)
        total = jnp.zeros((16, LANES), jnp.float32)
        for t in range(count):
            before[t, i * 16 : (i + 1) * 16, :] = total.astype(jnp.bfloat16)
            total = total * jnp.exp(logs[t, pl.ds(head, 1), :]) + got[
                t, i * 16 : (i + 1) * 16, :
            ].astype(jnp.float32)

    def two_copy(k):
        return remote(
            before.at[peer(k)], state_in.at[piece_rows(me)], two_send.at[k], two_recv.at[k],
            peer(k), core,
        )

    def send_two(k, carry):
        two_copy(k).start()
        return carry

    lax.fori_loop(1, count, send_two, 0)
    state_in[piece_rows(me), :] = before[me]
    send_weights(1)
    for copy in out_copies:
        copy.wait()

    def wait_two(k, carry):
        at = source(k)
        spot = state_in.at[piece_rows(at)]
        remote(spot, spot, two_send.at[k], two_recv.at[k], at, core).wait_recv()
        return carry

    lax.fori_loop(1, count, wait_two, 0)

    def gate_head(retained, gain, gate):
        centred = retained - jnp.mean(retained, axis=-1, keepdims=True)
        variance = jnp.mean(centred * centred, axis=-1, keepdims=True)
        normed = centred * lax.rsqrt(variance + EPS)
        return (normed * gain.astype(jnp.float32) * silu(gate.astype(jnp.float32))).astype(jnp.bfloat16)

    for h in range(heads):
        lifted = rotated[:, h * KW : (h + 1) * KW]
        crosses = []
        for e in range(VW // LANES):
            at = (h * (VW // LANES) + e) * KW
            crosses.append(dot(lifted, state_in[at : at + KW, :], ((1,), (0,))))
        cut = slice(h * VW, (h + 1) * VW)
        gated[:, cut] = gate_head(
            local[:, cut] + jnp.concatenate(crosses, axis=1), gain_wide[:, cut], gate_wide[:, cut]
        )
    for h in range(heads):
        g, e = h // 2, h % 2
        own = first_head if e == 0 else jnp.logical_not(first_head)
        lifted = rotated[:, heads * KW + g * LANES : heads * KW + (g + 1) * LANES]
        lifted = jnp.where(own, lifted.astype(jnp.float32), 0.0).astype(jnp.bfloat16)
        at = base_wide + g * LANES
        cross = dot(lifted, state_in[at : at + LANES, :], ((1,), (0,)))
        cut = slice(h * VN, (h + 1) * VN)
        spot = slice(wide_rows + h * VN, wide_rows + (h + 1) * VN)
        gated[:, spot] = gate_head(local[:, spot] + cross, gain_narrow[:, cut], gate_narrow[:, cut])

    mine_f = []
    chunk = dims["chunk"]
    for n in range(width // chunk):
        cut = slice(n * chunk, (n + 1) * chunk)
        product = dot(gated[...], out_w[:, cut], ((1,), (0,))).astype(jnp.bfloat16)
        low, high = product[:half], product[half:]
        first = core == 0
        mix_sent[:, cut] = jnp.where(first, high.astype(jnp.float32), low.astype(jnp.float32)).astype(jnp.bfloat16)
        resid[:, cut] = jnp.where(first, low.astype(jnp.float32), high.astype(jnp.float32))
    mix_copy = remote(mix_sent, mix_got, mix_sem.at[0], mix_sem.at[1], me, other)
    mix_copy.start()
    mix_copy.wait_recv()
    mixed = resid[...] + mix_got[...].astype(jnp.float32)
    stay = (
        stream[...].astype(jnp.float32) + rms(mixed) * gain_mix[...].astype(jnp.float32)
    ).astype(jnp.bfloat16).astype(jnp.float32)
    resid[...] = stay
    normed = rms(stay) * gain_pre[...].astype(jnp.float32)
    tokens[0, pl.ds(pl.multiple_of(pad + z * half, 16), half), :] = normed.astype(jnp.bfloat16)
    reach = dims["reach"]
    span = reach * width // 16
    for r in range(reach):
        for j in range(16 // reach):
            at = r * (16 // reach) + j
            tail_f[at : at + 1, :] = normed[half - reach + r : half - reach + r + 1, j * span : (j + 1) * span]
    tail[...] = tail_f[...].astype(jnp.bfloat16)

    def block(side, at, q):
        return tokens.at[side, pl.ds(pl.multiple_of(pad + at * half + q * step_rows, 16), step_rows)]

    def flow(at, q, sems, to):
        return remote(block(0, at, q), block(0, at, q), sems.at[at, q], z_recv.at[at, q], to, core)

    def over_y(at, q):
        return remote(block(0, at, q), block(1, at, q), y_send.at[at, q], y_recv.at[at, q], y_mate, core)

    def z_wait(at, q):
        remote(block(0, at, q), block(0, at, q), up_send.at[at, q], z_recv.at[at, q], y_mate, core).wait_recv()

    def pass_on(at, q, up, down):
        if up:
            @pl.when(z < nz - 1)
            def _():
                flow(at, q, up_send, me + 4).start()
        if down:
            @pl.when(z > 0)
            def _():
                flow(at, q, dn_send, me - 4).start()
        over_y(at, q).start()

    for q in range(parts):
        pass_on(z, q, True, True)

    next_chip = jnp.where(core == 0, me, (me + 1) % count)

    def halo_copy(k):
        at = (place + k) % places
        return remote(
            tail, halos.at[next_chip // 2], halo_send.at[k], halo_recv.at[next_chip // 2],
            2 * at + next_chip % 2, other,
        )

    def send_halo(k, carry):
        halo_copy(k).start()
        return carry

    lax.fori_loop(0, places, send_halo, 0)
    send_weights(2)
    pass_weights(0)
    forward_weights(1)

    for h in range(1, nz):
        for q in range(parts):
            @pl.when(z - h >= 0)
            def _():
                z_wait(z - h, q)
                pass_on(z - h, q, True, False)

            @pl.when(z + h < nz)
            def _():
                z_wait(z + h, q)
                pass_on(z + h, q, False, True)

    def wait_halo(at, carry):
        remote(halos.at[at], halos.at[at], halo_send.at[at], halo_recv.at[at], me, other).wait_recv()
        return carry

    lax.fori_loop(0, places, wait_halo, 0)
    for side in range(2):
        for at in range(nz):
            p = at * 2 + jnp.where(side == 0, y, 1 - y)
            start = jnp.logical_and(jnp.logical_and(p == 0, x == 0), core == 0)
            block_tail = halos[p].astype(jnp.float32)
            block_tail = jnp.where(start, 0.0, block_tail)
            for r in range(reach):
                for j in range(16 // reach):
                    spot = r * (16 // reach) + j
                    halo_f[side, at * reach + r : at * reach + r + 1, j * span : (j + 1) * span] = (
                        block_tail[spot : spot + 1, :]
                    )
        tokens[side, 0:pad, :] = halo_f[side].astype(jnp.bfloat16)
    pass_weights(1)
    taps_copy.wait()
    forward_weights(2)
    across_wait(0)
    across_wait(1)

    def feed(side):
        rows_in = tokens[side]
        ups = []
        for which in range(2):
            ups.append(
                dot(rows_in, weights[which], ((1,), (1,))).astype(jnp.bfloat16).astype(jnp.float32)
            )
        padded[0] = ups[0]
        padded[1] = ups[1]
        taps = taps_own[...] + taps_got[...]
        for at in range(nz):
            for u in range(units // LANES):
                cut = slice(u * LANES, (u + 1) * LANES)
                smooth = []
                for which in range(2):
                    rows_u = padded[which, pad + at * half : pad + (at + 1) * half, cut]
                    place_u = lax.broadcasted_iota(jnp.int32, (half, LANES), 0)
                    total = 0.0
                    for j in range(reach + 1):
                        back = reach - j
                        shifted = rows_u
                        if back:
                            shifted = pltpu.roll(rows_u, back, 0)
                            for r in range(back):
                                spot = at * reach + reach - back + r
                                shifted = jnp.where(
                                    place_u == r, padded[which, spot : spot + 1, cut], shifted
                                )
                        tap = which * (reach + 1) + j
                        total = total + taps[tap : tap + 1, cut] * shifted
                    smooth.append(total)
                hidden[side, at * half : (at + 1) * half, cut] = (silu(smooth[0]) * smooth[1]).astype(jnp.bfloat16)

    def lower_rows(side, at):
        spot = slice(at * half, (at + 1) * half)
        for n in range(width // chunk):
            cut = slice(n * chunk, (n + 1) * chunk)
            terms[side, spot, cut] = dot(
                hidden[side, spot, :], weights[2, :, cut], ((1,), (0,))
            ).astype(jnp.bfloat16)

    def down(side):
        for n in range(width // chunk):
            cut = slice(n * chunk, (n + 1) * chunk)
            terms[side, :, cut] = dot(
                hidden[side], weights[2, :, cut], ((1,), (0,))
            ).astype(jnp.bfloat16)

    for at in range(nz):
        for q in range(parts):
            remote(block(1, at, q), block(1, at, q), y_send.at[at, q], y_recv.at[at, q], y_mate, core).wait_recv()
    feed(1)
    pass_weights(2)
    across_wait(2)
    down(1)

    def part_of(ref, lead, at, q):
        return ref.at[lead, pl.ds(pl.multiple_of(at * half + q * step_rows, 16), step_rows)]

    def sum_y(at, q):
        return remote(
            part_of(terms, 1, at, q), from_y.at[at, q], ry_send.at[at, q], ry_recv.at[at, q],
            y_mate, core,
        )

    def sum_z(at, q, upward):
        if upward:
            return remote(
                part_of(terms, 0, at, q), from_up.at[at, q], ru_send.at[at, q], ru_recv.at[at, q],
                me + 4, core,
            )
        return remote(
            part_of(terms, 0, at, q), from_down.at[at, q], rd_send.at[at, q], rd_recv.at[at, q],
            me - 4, core,
        )

    for h in list(range(nz - 1, 0, -1)):
        for q in range(parts):
            @pl.when(z + h < nz)
            def _():
                sum_y(z + h, q).start()

            @pl.when(z - h >= 0)
            def _():
                sum_y(z - h, q).start()
    for q in range(parts):
        sum_y(z, q).start()
    feed(0)
    down(0)

    def rows_at(at, q):
        return pl.ds(pl.multiple_of(at * half + q * step_rows, 16), step_rows)

    def add_y(at, q):
        sum_y(at, q).wait_recv()
        terms[0, rows_at(at, q), :] = (
            terms[0, rows_at(at, q), :].astype(jnp.float32) + from_y[at, q].astype(jnp.float32)
        ).astype(jnp.bfloat16)

    def add_from(at, q, ref, sem):
        remote(ref.at[at, q], ref.at[at, q], ru_send.at[at, q], sem.at[at, q], y_mate, core).wait_recv()
        terms[0, rows_at(at, q), :] = (
            terms[0, rows_at(at, q), :].astype(jnp.float32) + ref[at, q].astype(jnp.float32)
        ).astype(jnp.bfloat16)

    for h in list(range(nz - 1, 0, -1)):
        for q in range(parts):
            @pl.when(z + h < nz)
            def _():
                add_y(z + h, q)

                @pl.when(z > 0)
                def _():
                    add_from(z + h, q, from_up, ru_recv)
                sum_z(z + h, q, True).start()

            @pl.when(z - h >= 0)
            def _():
                add_y(z - h, q)

                @pl.when(z < nz - 1)
                def _():
                    add_from(z - h, q, from_down, rd_recv)
                sum_z(z - h, q, False).start()
    for q in range(parts):
        add_y(z, q)

        @pl.when(z > 0)
        def _():
            add_from(z, q, from_up, ru_recv)

        @pl.when(z < nz - 1)
        def _():
            add_from(z, q, from_down, rd_recv)
    fed = terms[0, pl.ds(pl.multiple_of(z * half, 16), half), :].astype(jnp.float32)
    result[...] = (resid[...] + rms(fed) * gain_post[...].astype(jnp.float32)).astype(jnp.bfloat16)

    def drain(k, carry):
        log_copy(k).wait_send()
        one_copy(k).wait_send()
        two_copy(k).wait_send()
        return carry

    lax.fori_loop(1, count, drain, 0)

    def drain_weights(k, carry):
        for which in range(3):
            weight_copy(which, k).wait_send()
        return carry

    lax.fori_loop(1, places, drain_weights, 0)

    def drain_over(k, carry):
        for which in range(3):
            over_x(which, k).wait_send()
        halo_copy(k).wait_send()
        return carry

    lax.fori_loop(0, places, drain_over, 0)
    for which in range(3):
        across(which).wait_send()
    mix_copy.wait_send()

    def drain_blocks(at, carry):
        for q in range(parts):
            over_y(at, q).wait_send()
            sum_y(at, q).wait_send()

            @pl.when(jnp.logical_and(z < nz - 1, at <= z))
            def _():
                flow(at, q, up_send, me + 4).wait_send()

            @pl.when(jnp.logical_and(z > 0, at >= z))
            def _():
                flow(at, q, dn_send, me - 4).wait_send()

            @pl.when(at > z)
            def _():
                sum_z(at, q, True).wait_send()

            @pl.when(at < z)
            def _():
                sum_z(at, q, False).wait_send()
        return carry

    lax.fori_loop(0, nz, drain_blocks, 0)


def fused_layer(
    stream, q_wide, k_wide, v_wide, q_narrow, k_narrow, v_narrow, gate_wide, gate_narrow, log_decay,
    gain_wide, gain_narrow, out_wide, out_narrow, gain_mix, gain_pre, gain_post,
    weight_gate, weight_lin, weight_down, taps_gate, taps_lin,
):
    count, n_tp = lax.axis_size("sp"), lax.axis_size("tp")
    rows, width = q_wide.shape[0], stream.shape[1]
    places, nz = count // 2, count // 4
    heads = q_wide.shape[1] // KW
    columns = weight_gate.shape[1]
    share = columns // places
    units = share * n_tp
    reach = taps_gate.shape[0] - 1
    state_rows = heads * (KW * VW + KN * VN) // LANES
    piece = state_rows // count
    half = rows // n_tp
    parts = 2
    values = out_wide.shape[0] + out_narrow.shape[0]
    dims = dict(
        count=count, n_tp=n_tp, rows=rows, width=width, share=share, piece=piece, reach=reach,
        chunk=512,
    )
    taps = jnp.concatenate([taps_gate, taps_lin], axis=0).astype(jnp.float32)
    taps = taps.reshape(2 * (reach + 1), places, share).transpose(1, 0, 2)
    core = lax.axis_index("tp")
    zero = jnp.zeros_like(taps)
    taps = jnp.concatenate(
        [jnp.where(core == 0, taps, zero), jnp.where(core == 1, taps, zero)], axis=2
    )
    taps = jnp.pad(taps, ((0, 0), (0, -taps.shape[1] % 8), (0, 0)))
    vmem = pl.BlockSpec(memory_space=pltpu.VMEM)
    anywhere = pl.BlockSpec(memory_space=pl.ANY)
    bf, f32 = jnp.bfloat16, jnp.float32
    dma = pltpu.SemaphoreType.DMA
    scratch = [
        pltpu.VMEM((values, width), bf),
        pltpu.VMEM((3, units, width), bf),
        pltpu.VMEM((2, PAD + nz * half, width), bf),
        pltpu.VMEM((2, nz * half, width), bf),
        pltpu.VMEM((nz, parts, half // parts, width), bf),
        pltpu.VMEM((nz, parts, half // parts, width), bf),
        pltpu.VMEM((nz, parts, half // parts, width), bf),
        pltpu.VMEM((rows, heads * (KW + KN)), bf),
        pltpu.VMEM((rows, values), f32),
        pltpu.VMEM((state_rows, LANES), bf),
        pltpu.VMEM((count, piece, LANES), bf),
        pltpu.VMEM((count, piece, LANES), bf),
        pltpu.VMEM((state_rows, LANES), bf),
        pltpu.VMEM((rows, values), bf),
        pltpu.VMEM((2 * heads, LANES), f32),
        pltpu.VMEM((count, 2 * heads, LANES), f32),
        pltpu.VMEM(taps.shape[1:], f32),
        pltpu.VMEM(taps.shape[1:], f32),
        pltpu.VMEM((half, width), bf),
        pltpu.VMEM((half, width), bf),
        pltpu.VMEM((half, width), f32),
        pltpu.VMEM((16, reach * width // 16), f32),
        pltpu.VMEM((16, reach * width // 16), bf),
        pltpu.VMEM((places, 16, reach * width // 16), bf),
        pltpu.VMEM((2, PAD, width), f32),
        pltpu.VMEM((2, PAD + nz * half, units), f32),
        pltpu.VMEM((2, nz * half, units), bf),
        dma((2,)), dma((3,)), dma((3, places)), dma((3, places)), dma((3, places)),
        dma((3, places)), dma((3,)), dma((3,)),
        dma((count,)), dma((count,)), dma((count,)), dma((count,)), dma((count,)), dma((count,)),
        dma((2,)), dma((2,)), dma((places,)), dma((places,)),
    ] + [dma((nz, parts)) for _ in range(11)]
    kernel = pl.pallas_call(
        functools.partial(layer_kernel, dims),
        out_shape=jax.ShapeDtypeStruct(stream.shape, bf),
        in_specs=[vmem] * 17 + [anywhere] * 5,
        out_specs=vmem,
        scratch_shapes=scratch,
        compiler_params=pltpu.CompilerParams(
            collective_id=0, has_side_effects=True, vmem_limit_bytes=VMEM_BYTES
        ),
    )
    return kernel(
        stream, q_wide, k_wide, v_wide, q_narrow, k_narrow, v_narrow, gate_wide, gate_narrow,
        log_decay.reshape(-1, rows), gain_wide[None], gain_narrow[None], gain_mix[None],
        gain_pre[None], gain_post[None], jnp.asarray(tables_of(count, rows)), taps,
        out_wide, out_narrow, weight_gate.T, weight_lin.T, weight_down.T,
    )


def fits(stream, q_wide, log_decay, weight_gate, taps_gate):
    count, n_tp = lax.axis_size("sp"), lax.axis_size("tp")
    rows, width = q_wide.shape[0], stream.shape[1]
    if n_tp != 2 or count % 4 or count < 8 or rows != BLOCK or q_wide.shape[1] % (2 * KW):
        return False
    heads = q_wide.shape[1] // KW
    units = weight_gate.shape[1]
    state_rows = heads * (KW * VW + KN * VN) // LANES
    reach = taps_gate.shape[0] - 1
    held = units // (count // 2)
    return (
        2 * heads == 8
        and weight_gate.shape[0] == LANES
        and units % (count // 2 * 16) == 0
        and (n_tp * held) % LANES == 0
        and state_rows % (count * 16) == 0
        and reach == 2
        and (count // 4) * reach <= PAD
        and width % 512 == 0
        and 3 * n_tp * held * width <= 5 * 2 ** 20
    )


def body(
    stream,
    wide_head_query,
    broad_attention_lookup_vectors,
    values_wide,
    query_narrow,
    keys_narrow,
    values_narrow,
    gate_wide,
    gate_narrow,
    log_decay,
    gain_wide,
    gain_narrow,
    out_wide,
    out_narrow,
    gain_mix,
    gain_pre,
    gain_post,
    weight_gate,
    weight_lin,
    weight_down,
    taps_gate,
    taps_lin,
):
    if fits(stream, wide_head_query, log_decay, weight_gate, taps_gate):
        return fused_layer(
            stream, wide_head_query, broad_attention_lookup_vectors, values_wide, query_narrow,
            keys_narrow, values_narrow, gate_wide, gate_narrow, log_decay, gain_wide, gain_narrow,
            out_wide, out_narrow, gain_mix, gain_pre, gain_post, weight_gate, weight_lin,
            weight_down, taps_gate, taps_lin,
        )
    rows = wide_head_query.shape[0]
    count = lax.axis_size("sp")
    n_tp = lax.axis_size("tp")
    width = stream.shape[1]
    units = weight_gate.shape[1]
    by_tokens = 2 * count * rows < 3 * units and units % (count * 16) == 0
    by_tokens = by_tokens and count & (count - 1) == 0
    if by_tokens:
        weights, taps = unit_slices(weight_gate, weight_lin, weight_down, taps_gate, taps_lin)
    offset = lax.axis_index("sp") * rows
    rates_wide = log_decay[0]
    rates_narrow = log_decay[1]
    rot_wide, local_wide, state_wide = kept_nearby_memory(
        wide_head_query, broad_attention_lookup_vectors, values_wide, rates_wide, KW, VW, offset
    )
    rot_narrow, local_narrow, state_narrow = kept_nearby_memory(
        query_narrow, keys_narrow, values_narrow, rates_narrow, KN, VN, offset
    )
    incoming = carried_in(
        (state_wide, state_narrow),
        (jnp.sum(rates_wide, axis=1), jnp.sum(rates_narrow, axis=1)),
        "sp",
    )
    gated_wide = gate_heads(
        local_wide + carried(rot_wide, rates_wide, incoming[0]), gain_wide, gate_wide
    )
    gated_narrow = gate_heads(
        local_narrow + carried(rot_narrow, rates_narrow, incoming[1]), gain_narrow, gate_narrow
    )
    part_wide = jnp.dot(gated_wide, out_wide, preferred_element_type=jnp.float32)
    part_narrow = jnp.dot(gated_narrow, out_narrow, preferred_element_type=jnp.float32)
    mixed = share_rows(
        (part_wide + part_narrow).astype(jnp.bfloat16).reshape(n_tp, rows // n_tp, width), "tp"
    )
    resid = (stream.astype(jnp.float32) + scale_rows(mixed, gain_mix)).astype(jnp.bfloat16)
    normed_in = scale_rows(resid.astype(jnp.float32), gain_pre).astype(jnp.bfloat16)
    if by_tokens:
        fed = feed_by_tokens(normed_in, weights, taps)
    else:
        fed = feed_by_weights(normed_in, weight_gate, weight_lin, weight_down, taps_gate, taps_lin)
    return (resid.astype(jnp.float32) + scale_rows(fed, gain_post)).astype(jnp.bfloat16)


def solution(mesh):
    in_specs = (
        P(("sp", "tp"), None),
        P("sp", "tp"),
        P("sp", "tp"),
        P("sp", "tp"),
        P("sp", "tp"),
        P("sp", "tp"),
        P("sp", "tp"),
        P("sp", "tp"),
        P("sp", "tp"),
        P(None, "tp", "sp"),
        P("tp"),
        P("tp"),
        P("tp", None),
        P("tp", None),
        P(),
        P(),
        P(),
        P("sp", "tp"),
        P("sp", "tp"),
        P("sp", "tp"),
        P(None, "tp"),
        P(None, "tp"),
    )
    out_specs = P(("sp", "tp"), None)
    return jax.shard_map(body, mesh=mesh, in_specs=in_specs, out_specs=out_specs, check_vma=False)
```

```python
import functools

import jax
import jax.numpy as jnp
import numpy as np
from jax import lax
from jax.experimental import pallas as pl
from jax.experimental.pallas import tpu as pltpu
from jax.sharding import PartitionSpec as P

KW = 128
VW = 256
KN = 64
VN = 128
BLOCK = 128


EPS = 1e-06
THETA = 10000.0
LANES = 128
PAD = 16
VMEM_BYTES = 60 * 2**20


def passed_along(value, axis, steps):
    count = lax.axis_size(axis)
    first, last = (max(0, -steps), min(count, count - steps))
    return lax.ppermute(value, axis, [(source, source + steps) for source in range(first, last)])


def rotate(block, positions):
    width = block.shape[-1]
    half = width // 2
    frequency = THETA ** (-(jnp.arange(half, dtype=jnp.float32) * 2.0 / width))
    angles = positions.astype(jnp.float32)[:, None] * frequency[None, :]
    cosine = jnp.cos(angles)[:, None, :]
    sine = jnp.sin(angles)[:, None, :]
    values = block.astype(jnp.float32)
    first = values[..., :half]
    second = values[..., half:]
    return jnp.concatenate(
        [first * cosine - second * sine, second * cosine + first * sine], axis=-1
    )


def block_step(state, inputs):
    query, keys, values, log_rate = inputs
    running = jnp.cumsum(log_rate, axis=1)
    length = running.shape[1]
    index = jnp.arange(length)
    lower = (index[:, None] >= index[None, :])[None]
    spread = jnp.where(
        lower, jnp.exp(jnp.where(lower, running[:, :, None] - running[:, None, :], 0.0)), 0.0
    )
    scores = (
        jnp.einsum("ihd,jhd->hij", query, keys, preferred_element_type=jnp.float32) * spread
    ).astype(jnp.bfloat16)
    inner = jnp.einsum("hij,jhe->ihe", scores, values, preferred_element_type=jnp.float32)
    lifted = query.astype(jnp.float32) * jnp.exp(running).T[:, :, None]
    cross = jnp.einsum("ihd,hde->ihe", lifted, state, precision=lax.Precision.HIGHEST)
    tail = running[:, -1:]
    scaled = (keys.astype(jnp.float32) * jnp.exp(tail - running).T[:, :, None]).astype(jnp.bfloat16)
    update = jnp.einsum("jhd,jhe->hde", scaled, values, preferred_element_type=jnp.float32)
    state = state * jnp.exp(tail)[:, :, None] + update
    return (state, inner + cross)


def kept_nearby_memory(query, keys, values, log_rate, head_dim, value_dim, offset):
    rows = query.shape[0]
    heads = query.shape[1] // head_dim
    positions = offset + jnp.arange(rows, dtype=jnp.int32)
    rotated_query = rotate(query.reshape(rows, heads, head_dim), positions).astype(jnp.bfloat16)
    rotated_keys = (
        rotate(keys.reshape(rows, heads, head_dim), positions) * head_dim ** (-0.5)
    ).astype(jnp.bfloat16)
    layer_groups_list = rows // BLOCK

    def split(array):
        return array.reshape(layer_groups_list, BLOCK, heads, array.shape[-1])

    rates = jnp.transpose(log_rate.reshape(heads, layer_groups_list, BLOCK), (1, 0, 2))
    start = jnp.zeros((heads, head_dim, value_dim), jnp.float32)
    inputs = (
        split(rotated_query),
        split(rotated_keys),
        split(values.reshape(rows, heads, value_dim)),
        rates,
    )
    state, outs = lax.scan(block_step, start, inputs)
    return (rotated_query, outs.reshape(rows, heads, value_dim), state)


def carried(rotated_query, log_rate, state_in):
    lifted = rotated_query.astype(jnp.float32) * jnp.exp(jnp.cumsum(log_rate, axis=1)).T[:, :, None]
    return jnp.einsum("ihd,hde->ihe", lifted, state_in, precision=lax.Precision.HIGHEST)


def gate_heads(retained, gain, gate):
    mean = jnp.mean(retained, axis=-1, keepdims=True)
    centred = retained - mean
    variance = jnp.mean(centred * centred, axis=-1, keepdims=True)
    normed = (centred * lax.rsqrt(variance + EPS)).reshape(retained.shape[0], -1)
    return (normed * gain.astype(jnp.float32) * jax.nn.silu(gate.astype(jnp.float32))).astype(
        jnp.bfloat16
    )


def scale_rows(rows, gain):
    return (
        rows
        * lax.rsqrt(jnp.mean(rows * rows, axis=-1, keepdims=True) + EPS)
        * gain.astype(jnp.float32)
    )


def causal_taps(upward, before, taps):
    width = taps.shape[0]
    total = upward.shape[0]
    padded_rows = jnp.concatenate([before, upward], axis=0).astype(jnp.float32)
    smooth = jnp.zeros((total, upward.shape[1]), jnp.float32)
    for tap_index in range(width):
        smooth = (
            smooth
            + taps[tap_index].astype(jnp.float32)[None, :]
            * padded_rows[tap_index : tap_index + total]
        )
    return smooth


def swap_blocks(blocks, axis):
    return lax.all_to_all(blocks, axis, 0, 0, tiled=False)


def share_rows(parts, axis):
    count = lax.axis_size(axis)
    place = lax.axis_index(axis)
    total = lax.dynamic_index_in_dim(parts, place, 0, False).astype(jnp.float32)
    for step in range(1, count):
        piece = lax.dynamic_index_in_dim(parts, (place + step) % count, 0, False)
        moved = lax.ppermute(piece, axis, [(i, (i + step) % count) for i in range(count)])
        total = total + moved.astype(jnp.float32)
    return total


def carried_in(states, totals, axis):
    count = lax.axis_size(axis)
    lanes = states[-1].shape[-1]
    flat = jnp.concatenate([s.reshape(-1, lanes) for s in states]).astype(jnp.bfloat16)
    rates = jnp.concatenate(
        [jnp.repeat(d, s.size // s.shape[0] // lanes) for s, d in zip(states, totals)]
    )
    share = flat.shape[0] // count
    rates = rates.reshape(count, share)
    rates = jnp.pad(rates, ((0, 0), (0, -share % lanes)))
    parts, left = [], rates
    for _ in range(3):
        parts.append(left.astype(jnp.bfloat16))
        left = left - parts[-1].astype(jnp.float32)
    parts = [part.reshape(count, -1, lanes) for part in parts]
    sent = jnp.concatenate([flat.reshape(count, share, lanes)] + parts, axis=1)
    got = swap_blocks(sent, axis).astype(jnp.float32)
    parts = jnp.split(got[:, share:], 3, axis=1)
    logs = (parts[0] + parts[1] + parts[2]).reshape(count, -1)[:, :share]
    own = got[:, :share]
    steps = jnp.arange(count)
    between = (steps[None, None] > steps[None, :, None]) & (
        steps[None, None] < steps[:, None, None]
    )
    span = jnp.sum(jnp.where(between[..., None], logs[None, None], 0.0), axis=2)
    factor = jnp.where((steps[None] < steps[:, None])[..., None], jnp.exp(span), 0.0)
    before = sum(factor[:, step, :, None] * own[step][None] for step in range(count))
    back = swap_blocks(before.astype(jnp.bfloat16), axis).reshape(-1, lanes).astype(jnp.float32)
    outs, at = [], 0
    for s in states:
        rows = s.size // lanes
        outs.append(back[at : at + rows].reshape(s.shape))
        at += rows
    return outs


def feed_by_weights(normed_in, weight_gate, weight_lin, weight_down, taps_gate, taps_lin):
    normed_all = lax.all_gather(normed_in, "tp", axis=0, tiled=True)
    rows = normed_all.shape[0]
    whole_gate, whole_lin = (
        lax.all_gather(weight_gate, "sp", axis=0, tiled=True),
        lax.all_gather(weight_lin, "sp", axis=0, tiled=True),
    )
    up_gate = jnp.dot(normed_all, whole_gate, preferred_element_type=jnp.float32).astype(
        jnp.bfloat16
    )
    up_lin = jnp.dot(normed_all, whole_lin, preferred_element_type=jnp.float32).astype(jnp.bfloat16)
    reach = taps_gate.shape[0] - 1
    before_gate, before_lin = passed_along(
        (up_gate[rows - reach :], up_lin[rows - reach :]), "sp", 1
    )
    smooth_gate = causal_taps(up_gate, before_gate, taps_gate)
    smooth_lin = causal_taps(up_lin, before_lin, taps_lin)
    hidden = (jax.nn.silu(smooth_gate) * smooth_lin).astype(jnp.bfloat16)
    terms = lax.dot_general(
        hidden,
        lax.all_gather(weight_down, "sp", axis=0, tiled=True),
        (((1,), (1,)), ((), ())),
        preferred_element_type=jnp.float32,
    )
    return lax.psum_scatter(
        terms.astype(jnp.bfloat16), "tp", scatter_dimension=0, tiled=True
    ).astype(jnp.float32)


def from_all(value, axis, dim):
    count = lax.axis_size(axis)
    found = [value]
    for step in range(1, count):
        found.append(lax.ppermute(value, axis, [(i, (i + step) % count) for i in range(count)]))
    return jnp.concatenate(found, axis=dim)


def unit_slices(weight_gate, weight_lin, weight_down, taps_gate, taps_lin):
    count = lax.axis_size("sp")
    place = lax.axis_index("sp")
    deep, units = weight_gate.shape
    share = units // count
    turned = jnp.stack([weight_gate.T, weight_lin.T, weight_down.T])
    blocks = turned.reshape(3, count, share, deep).transpose(1, 0, 2, 3)
    got = swap_blocks(blocks, "sp")
    mine = got.transpose(1, 2, 0, 3).reshape(3, share, count * deep)
    taps = jnp.stack([taps_gate, taps_lin])
    taps = lax.dynamic_slice_in_dim(taps, place * share, share, 2)
    return from_all(mine, "tp", 1), from_all(taps, "tp", 2)


def flip(value, axis, bit):
    return lax.ppermute(
        value, axis, [(i, i ^ (1 << bit)) for i in range(lax.axis_size(axis))]
    )


def bits_of(count, swapped):
    bits = list(range(count.bit_length() - 1))
    if swapped:
        bits[:2] = bits[:2][::-1]
    return bits


def gather_around(value, axis, swapped):
    bits = bits_of(lax.axis_size(axis), swapped)
    for bit in bits[::-1]:
        value = jnp.stack([value, flip(value, axis, bit)])
    order = [bits.index(bit) for bit in sorted(bits, reverse=True)]
    value = value.transpose(*order, *range(len(bits), value.ndim))
    return value.reshape(-1, *value.shape[len(bits) :])


def add_around(value, axis, swapped):
    bits = bits_of(lax.axis_size(axis), swapped)
    value = value.reshape(*[2] * len(bits), *value.shape[1:])
    dims = sorted(bits, reverse=True)
    for bit in bits:
        at = dims.index(bit)
        dims.remove(bit)
        kept = lax.index_in_dim(value, 0, at, False).astype(jnp.float32)
        sent = lax.index_in_dim(value, 1, at, False).astype(jnp.bfloat16)
        value = kept + flip(sent, axis, bit).astype(jnp.float32)
        if dims:
            value = value.astype(jnp.bfloat16)
    return value


def feed_by_tokens(normed_in, weights, taps):
    count = lax.axis_size("sp")
    n_tp = lax.axis_size("tp")
    rows, width = normed_in.shape
    place = lax.axis_index("sp")
    half = width // 2
    flat = weights[:2].reshape(-1, width)
    units = flat.shape[0] // 2
    ups = 0.0
    for part in range(2):
        cut = slice(part * half, (part + 1) * half)
        tokens = gather_around(normed_in[:, cut], "sp", part == 1)
        ups = ups + lax.dot_general(
            tokens.reshape(count * rows, half),
            flat[:, cut],
            (((1,), (1,)), ((), ())),
            preferred_element_type=jnp.float32,
        )
    ups = ups.astype(jnp.bfloat16).reshape(count, rows, 2 * units)
    reach = taps.shape[1] - 1
    tails = ups[:, rows - reach :]
    prior = lax.ppermute(tails, "tp", [(i, (i + 1) % n_tp) for i in range(n_tp)])
    prior = jnp.roll(prior.reshape(count, reach, 2, n_tp, -1), 1, axis=3).reshape(prior.shape)
    blocks = place ^ jnp.arange(count)
    follows = (blocks[:, None] == blocks[None, :] + 1).astype(jnp.bfloat16)
    shifted = jnp.dot(
        follows, prior.reshape(count, -1), preferred_element_type=jnp.float32
    ).astype(jnp.bfloat16).reshape(prior.shape)
    prior = jnp.where(lax.axis_index("tp") == 0, shifted, prior)
    padded = jnp.concatenate([prior, ups], axis=1).astype(jnp.float32)
    taps = jnp.concatenate([taps[0], taps[1]], axis=1).astype(jnp.float32)
    smooth = sum(taps[j] * padded[:, j : j + rows] for j in range(reach + 1))
    hidden = (jax.nn.silu(smooth[..., :units]) * smooth[..., units:]).astype(jnp.bfloat16)
    hidden = hidden.reshape(count * rows, units)
    sums = []
    for part in range(2):
        cut = slice(part * half, (part + 1) * half)
        terms = jnp.dot(hidden, weights[2][:, cut], preferred_element_type=jnp.float32)
        terms = terms.astype(jnp.bfloat16).reshape(count, rows, half)
        sums.append(add_around(terms, "sp", part == 1))
    return jnp.concatenate(sums, axis=1)


def tables_of(count, rows):
    def angles(positions, width):
        half = width // 2
        frequency = THETA ** (-(np.arange(half, dtype=np.float64) * 2.0 / width))
        return np.tile(positions[:, None] * frequency[None, :], (1, LANES // half))

    positions = np.concatenate([np.arange(rows), np.arange(count) * rows]).astype(np.float64)
    found = []
    for width in (KW, KN):
        turned = angles(positions, width)
        found += [np.cos(turned), np.sin(turned)]
    return np.stack(found).astype(np.float32)


def remote(source, target, sent, got, sp, tp):
    return pltpu.make_async_remote_copy(
        src_ref=source, dst_ref=target, send_sem=sent, recv_sem=got,
        device_id=(sp, tp), device_id_type=pl.DeviceIdType.MESH,
    )


def silu(value):
    return value / (1.0 + jnp.exp(-value))


def rms(value):
    return value * lax.rsqrt(jnp.mean(value * value, axis=-1, keepdims=True) + EPS)


def layer_kernel(
    dims,
    stream, q_wide, k_wide, v_wide, q_narrow, k_narrow, v_narrow, gate_wide, gate_narrow,
    decay, gain_wide, gain_narrow, gain_mix, gain_pre, gain_post, tables, taps_gate, taps_lin,
    out_wide_hbm, out_narrow_hbm, weight_gate, weight_lin, weight_down,
    result,
    raw, turned, out_w, weights, tokens, terms, from_y, from_up, from_down, rotated, local, states,
    got, plane_sum, planes, carry, before, state_in, gated, fades, taps_all, logs_own, logs, taps_own, taps_got, mix_sent, mix_got, resid, tail_f, tail, halos, halo_f,
    padded, hidden,
    raw_sem, out_sem, own_sem, w_send, w_recv, xw_send, xw_recv, dw_send, dw_recv,
    log_send, log_recv, one_send, one_recv, z_sum_send, z_sum_recv, two_send, two_recv, tap_sem, mix_sem,
    halo_send, halo_recv, up_send, dn_send, y_send, z_recv, y_recv,
    ry_send, ry_recv, ru_send, ru_recv, rd_send, rd_recv,
):
    count, n_tp = dims["count"], dims["n_tp"]
    rows, width = dims["rows"], dims["width"]
    half = rows // n_tp
    places = count // 2
    nz = count // 4
    share = dims["share"]
    n_tiles = share * places // LANES
    units = n_tp * share
    piece = dims["piece"]
    reach = dims["reach"]
    parts = 2
    step_rows = half // parts
    pad = PAD
    me = lax.axis_index("sp")
    core = lax.axis_index("tp")
    other = 1 - core
    x = me % 2
    y = (me // 2) % 2
    z = me // 4
    place = me // 2
    x_mate = me + 1 - 2 * x
    y_mate = me + 2 - 4 * y
    mine = pl.multiple_of(me * LANES, LANES)

    def in_plane(k):
        at = (place + k) % places
        return at, 2 * at + x

    barrier = pltpu.get_barrier_semaphore()

    def greet(k, carry):
        to = (me * n_tp + core + k) % (count * n_tp)
        pl.semaphore_signal(
            barrier, inc=1, device_id=(to // n_tp, to % n_tp),
            device_id_type=pl.DeviceIdType.MESH,
        )
        return carry

    lax.fori_loop(1, count * n_tp, greet, 0)

    wide_rows = out_wide_hbm.shape[0]
    narrow_rows = out_narrow_hbm.shape[0]
    out_copies = [
        pltpu.make_async_copy(out_wide_hbm, out_w.at[pl.ds(0, wide_rows)], out_sem.at[0]),
        pltpu.make_async_copy(out_narrow_hbm, out_w.at[pl.ds(wide_rows, narrow_rows)], out_sem.at[1]),
    ]
    raw_copies = [
        pltpu.make_async_copy(source, raw.at[which], raw_sem.at[which])
        for which, source in enumerate((weight_gate, weight_lin, weight_down))
    ]
    for copy in raw_copies + out_copies:
        copy.start()

    def own_rows(at):
        return pl.ds(pl.multiple_of(at * share, 16), share)

    core_rows = pl.ds(pl.multiple_of(core * share, 16), share)

    def weight_copy(which, k):
        at, to = in_plane(k)
        return remote(
            turned.at[which, own_rows(at)], weights.at[which, core_rows, pl.ds(mine, LANES)],
            w_send.at[which, k], w_recv.at[which, k], to, core,
        )

    def weight_wait(which, k):
        from_at = (place + places - k) % places
        columns = pl.ds(pl.multiple_of((2 * from_at + x) * LANES, LANES), LANES)
        spot = weights.at[which, core_rows, columns]
        remote(spot, spot, w_send.at[which, k], w_recv.at[which, k], x_mate, core).wait_recv()

    def over_x(which, k):
        from_at = (place + places - k) % places
        columns = pl.ds(pl.multiple_of((2 * from_at + x) * LANES, LANES), LANES)
        spot = weights.at[which, core_rows, columns]
        return remote(spot, spot, xw_send.at[which, k], xw_recv.at[which, k], x_mate, core)

    def over_x_wait(which, k):
        from_at = (place + places - k) % places
        columns = pl.ds(pl.multiple_of((2 * from_at + 1 - x) * LANES, LANES), LANES)
        spot = weights.at[which, core_rows, columns]
        remote(spot, spot, xw_send.at[which, k], xw_recv.at[which, k], x_mate, core).wait_recv()

    def across(which):
        spot = weights.at[which, core_rows]
        return remote(spot, spot, dw_send.at[which], dw_recv.at[which], me, other)

    def across_wait(which):
        spot = weights.at[which, pl.ds(pl.multiple_of(other * share, 16), share)]
        remote(spot, spot, dw_send.at[which], dw_recv.at[which], me, other).wait_recv()

    def send_weights(which):
        def go(k, carry):
            weight_copy(which, k).start()
            return carry
        lax.fori_loop(1, places, go, 0)

    def own_copy(which):
        return pltpu.make_async_copy(
            turned.at[which, own_rows(place)], weights.at[which, core_rows, pl.ds(mine, LANES)],
            own_sem.at[which],
        )

    def forward_weights(which, first=0, last=places):
        if first == 0:
            own_copy(which).wait()
            over_x(which, 0).start()

        def go(k, carry):
            weight_wait(which, k)
            over_x(which, k).start()
            return carry
        lax.fori_loop(max(first, 1), last, go, 0)

    def pass_weights(which):
        def go(k, carry):
            over_x_wait(which, k)
            return carry
        lax.fori_loop(0, places, go, 0)
        across(which).start()

    def turn(which):
        raw_copies[which].wait()
        for at in range(n_tiles):
            cut = slice(at * LANES, (at + 1) * LANES)
            turned[which, cut, :] = raw[which, :, cut].T
        own_copy(which).start()

    i_at = lax.broadcasted_iota(jnp.int32, (rows, rows), 0)
    j_at = lax.broadcasted_iota(jnp.int32, (rows, rows), 1)
    lower = i_at >= j_at
    lower_f = lower.astype(jnp.float32)
    upper_f = (i_at <= j_at).astype(jnp.float32)
    rates = decay[...].reshape(-1, rows)
    run_rows = lax.dot_general(
        rates, upper_f, (((1,), (0,)), ((), ())), precision=lax.Precision.HIGHEST,
        preferred_element_type=jnp.float32,
    )
    run_cols = lax.dot_general(
        lower_f, rates, (((1,), (1,)), ((), ())), precision=lax.Precision.HIGHEST,
        preferred_element_type=jnp.float32,
    )
    totals = run_rows[:, rows - 1 : rows]
    logs_own[...] = jnp.broadcast_to(totals, logs_own.shape)
    logs[me] = jnp.broadcast_to(totals, logs_own.shape)

    def peer(k):
        return (me + k) % count

    def log_copy(k):
        return remote(logs_own, logs.at[me], log_send.at[k], log_recv.at[k], peer(k), core)

    def send_logs(k, carry):
        log_copy(k).start()
        return carry

    heads = wide_rows // VW
    lane = lax.broadcasted_iota(jnp.int32, (rows, LANES), 1)

    def angle_table(first, half_width):
        cos_i, sin_i = tables[first, 0:rows, :], tables[first + 1, 0:rows, :]
        cos_o = tables[first, pl.ds(rows + me, 1), :]
        sin_o = tables[first + 1, pl.ds(rows + me, 1), :]
        cosine = cos_o * cos_i - sin_o * sin_i
        sine = sin_o * cos_i + cos_o * sin_i
        early = lane % (2 * half_width) < half_width
        return cosine, jnp.where(early, -sine, sine), early

    cos_w, sin_w, _ = angle_table(0, KW // 2)

    def dot(a, b, dims_):
        return lax.dot_general(a, b, (dims_, ((), ())), preferred_element_type=jnp.float32)

    def spread_of(column, row):
        return jnp.where(lower, jnp.exp(jnp.where(lower, column - row, 0.0)), 0.0)

    for h in range(heads):
        cut = slice(h * KW, (h + 1) * KW)
        query = q_wide[:, cut].astype(jnp.float32)
        query = (query * cos_w + pltpu.roll(query, KW // 2, 1) * sin_w).astype(jnp.bfloat16)
        keys = k_wide[:, cut].astype(jnp.float32)
        keys = ((keys * cos_w + pltpu.roll(keys, KW // 2, 1) * sin_w) * KW ** (-0.5)).astype(jnp.bfloat16)
        column, row = run_cols[:, h : h + 1], run_rows[h : h + 1, :]
        scores = (dot(query, keys, ((1,), (1,))) * spread_of(column, row)).astype(jnp.bfloat16)
        values = v_wide[:, h * VW : (h + 1) * VW]
        local[:, h * VW : (h + 1) * VW] = dot(scores, values, ((1,), (0,)))
        last = totals[h : h + 1, :]
        scaled = (keys.astype(jnp.float32) * jnp.exp(last - column)).astype(jnp.bfloat16)
        state = dot(scaled, values, ((0,), (0,))).astype(jnp.bfloat16)
        for e in range(VW // LANES):
            at = (h * (VW // LANES) + e) * KW
            states[at : at + KW, :] = state[:, e * LANES : (e + 1) * LANES]
        rotated[:, cut] = (query.astype(jnp.float32) * jnp.exp(column)).astype(jnp.bfloat16)

    cos_n, sin_n, early_n = angle_table(2, KN // 2)

    def swap_narrow(value):
        return jnp.where(
            early_n, pltpu.roll(value, LANES - KN // 2, 1), pltpu.roll(value, KN // 2, 1)
        )

    base_wide = wide_rows // LANES * KW
    first_head = lane < KN
    for g in range(heads // 2):
        cut = slice(g * LANES, (g + 1) * LANES)
        query = q_narrow[:, cut].astype(jnp.float32)
        query = (query * cos_n + swap_narrow(query) * sin_n).astype(jnp.bfloat16)
        keys = k_narrow[:, cut].astype(jnp.float32)
        keys = ((keys * cos_n + swap_narrow(keys) * sin_n) * KN ** (-0.5)).astype(jnp.bfloat16)
        spot = heads + 2 * g
        columns = [run_cols[:, spot + e : spot + e + 1] for e in range(2)]
        lasts = [totals[spot + e : spot + e + 1, :] for e in range(2)]
        falls = jnp.where(
            first_head, jnp.exp(lasts[0] - columns[0]), jnp.exp(lasts[1] - columns[1])
        )
        scaled = (keys.astype(jnp.float32) * falls).astype(jnp.bfloat16)
        rises = jnp.where(first_head, jnp.exp(columns[0]), jnp.exp(columns[1]))
        query_f = query.astype(jnp.float32)
        rotated[:, heads * KW + g * LANES : heads * KW + (g + 1) * LANES] = (
            query_f * rises
        ).astype(jnp.bfloat16)
        for e in range(2):
            h = 2 * g + e
            own = first_head if e == 0 else jnp.logical_not(first_head)
            masked = jnp.where(own, query_f, 0.0).astype(jnp.bfloat16)
            scores = (
                dot(masked, keys, ((1,), (1,)))
                * spread_of(columns[e], run_rows[spot + e : spot + e + 1, :])
            ).astype(jnp.bfloat16)
            values = v_narrow[:, h * VN : (h + 1) * VN]
            local[:, wide_rows + h * VN : wide_rows + (h + 1) * VN] = dot(scores, values, ((1,), (0,)))
            state = dot(scaled, values, ((0,), (0,))).astype(jnp.bfloat16)
            at = base_wide + h * KN
            states[at : at + KN, :] = state[e * KN : (e + 1) * KN, :]

    pl.semaphore_wait(barrier, count * n_tp - 1)
    spot_in = me % 4
    plane_at = z * 4

    def piece_rows(at):
        return pl.ds(pl.multiple_of(at * piece, 16), piece)

    def mate(k):
        return (spot_in + k) % 4

    def one_copy(k):
        return remote(
            states.at[piece_rows(mate(k))], got.at[spot_in], one_send.at[k], one_recv.at[k],
            plane_at + mate(k), core,
        )

    for k in range(1, 4):
        one_copy(k).start()
    lax.fori_loop(1, count, send_logs, 0)
    got[spot_in] = states[piece_rows(spot_in), :]
    turn(0)
    send_weights(0)
    taps_all[...] = jnp.zeros_like(taps_all)
    taps_all[0 : reach + 1, :] = taps_gate[...].astype(jnp.float32)
    taps_all[reach + 1 : 2 * (reach + 1), :] = taps_lin[...].astype(jnp.float32)
    taps_mine = pltpu.roll(taps_all[...], (share * places - place * share) % (share * places), 1)[:, :units]
    taps_lane = lax.broadcasted_iota(jnp.int32, taps_own.shape, 1)
    taps_mine = jnp.where(taps_lane < share, taps_mine, 0.0)
    taps_own[...] = jnp.where(core == 0, taps_mine, pltpu.roll(taps_mine, share, 1))
    turn(1)
    taps_copy = remote(taps_own, taps_got, tap_sem.at[0], tap_sem.at[1], me, other)
    taps_copy.start()

    def source(k):
        return (me + count - k) % count

    def wait_logs(k, carried_):
        at = source(k)
        remote(logs.at[at], logs.at[at], log_send.at[k], log_recv.at[k], at, core).wait_recv()
        return carried_

    for k in range(1, 4):
        at = (spot_in + 4 - k) % 4
        remote(got.at[at], got.at[at], one_send.at[k], one_recv.at[k], plane_at + at, core).wait_recv()
    lax.fori_loop(1, count, wait_logs, 0)
    fades[...] = jnp.exp(logs[...])
    groups_wide = VW // LANES * KW // 16
    groups_narrow = KN // 16

    def head_of(i):
        g = spot_in * (piece // 16) + i
        head = jnp.where(
            g < heads * groups_wide, g // groups_wide,
            heads + (g - heads * groups_wide) // groups_narrow,
        )
        return jnp.minimum(head, 2 * heads - 1)

    def fade_of(chip, i):
        return fades[chip, pl.ds(head_of(i), 1), :]

    for i in range(piece // 16):
        cut = slice(i * 16, (i + 1) * 16)
        total = got[0, cut, :].astype(jnp.float32)
        for t in range(1, 4):
            total = total * fade_of(plane_at + t, i) + got[t, cut, :].astype(jnp.float32)
        plane_sum[cut, :] = total.astype(jnp.bfloat16)

    def plane_copy(k):
        return remote(plane_sum, planes.at[z], z_sum_send.at[k], z_sum_recv.at[k], me + 4 * k, core)

    for k in range(1, nz):
        @pl.when(z + k < nz)
        def _():
            plane_copy(k).start()
    carry[...] = jnp.zeros_like(carry)
    turn(2)

    def add_plane(at, carried_):
        k = z - at
        remote(planes.at[at], planes.at[at], z_sum_send.at[k], z_sum_recv.at[k], me - 4 * k, core).wait_recv()
        for i in range(piece // 16):
            cut = slice(i * 16, (i + 1) * 16)
            fade = fade_of(at * 4, i)
            for t in range(1, 4):
                fade = fade * fade_of(at * 4 + t, i)
            carry[cut, :] = carry[cut, :] * fade + planes[at, cut, :].astype(jnp.float32)
        return carried_

    lax.fori_loop(0, z, add_plane, 0)
    for i in range(piece // 16):
        cut = slice(i * 16, (i + 1) * 16)
        total = carry[cut, :]
        for t in range(4):
            before[t, cut, :] = total.astype(jnp.bfloat16)
            if t < 3:
                total = total * fade_of(plane_at + t, i) + got[t, cut, :].astype(jnp.float32)

    def two_copy(k):
        return remote(
            before.at[mate(k)], state_in.at[piece_rows(spot_in)], two_send.at[k], two_recv.at[k],
            plane_at + mate(k), core,
        )

    for k in range(1, 4):
        two_copy(k).start()
    state_in[piece_rows(spot_in), :] = before[spot_in]
    send_weights(1)
    forward_weights(0)
    for copy in out_copies:
        copy.wait()

    for k in range(1, 4):
        at = (spot_in + 4 - k) % 4
        spot = state_in.at[piece_rows(at)]
        remote(spot, spot, two_send.at[k], two_recv.at[k], plane_at + at, core).wait_recv()

    def gate_head(retained, gain, gate):
        centred = retained - jnp.mean(retained, axis=-1, keepdims=True)
        variance = jnp.mean(centred * centred, axis=-1, keepdims=True)
        normed = centred * lax.rsqrt(variance + EPS)
        return (normed * gain * silu(gate.astype(jnp.float32))).astype(jnp.bfloat16)

    for h in range(heads):
        lifted = rotated[:, h * KW : (h + 1) * KW]
        crosses = []
        for e in range(VW // LANES):
            at = (h * (VW // LANES) + e) * KW
            crosses.append(dot(lifted, state_in[at : at + KW, :], ((1,), (0,))))
        cut = slice(h * VW, (h + 1) * VW)
        gated[:, cut] = gate_head(
            local[:, cut] + jnp.concatenate(crosses, axis=1), gain_wide[cut].astype(jnp.float32).reshape(1, -1), gate_wide[:, cut]
        )
    for h in range(heads):
        g, e = h // 2, h % 2
        own = first_head if e == 0 else jnp.logical_not(first_head)
        lifted = rotated[:, heads * KW + g * LANES : heads * KW + (g + 1) * LANES]
        lifted = jnp.where(own, lifted.astype(jnp.float32), 0.0).astype(jnp.bfloat16)
        at = base_wide + g * LANES
        cross = dot(lifted, state_in[at : at + LANES, :], ((1,), (0,)))
        cut = slice(h * VN, (h + 1) * VN)
        spot = slice(wide_rows + h * VN, wide_rows + (h + 1) * VN)
        gated[:, spot] = gate_head(local[:, spot] + cross, gain_narrow[cut].astype(jnp.float32).reshape(1, -1), gate_narrow[:, cut])

    mine_f = []
    chunk = dims["chunk"]
    for n in range(width // chunk):
        cut = slice(n * chunk, (n + 1) * chunk)
        product = dot(gated[...], out_w[:, cut], ((1,), (0,))).astype(jnp.bfloat16)
        low, high = product[:half], product[half:]
        first = core == 0
        mix_sent[:, cut] = jnp.where(first, high.astype(jnp.float32), low.astype(jnp.float32)).astype(jnp.bfloat16)
        resid[:, cut] = jnp.where(first, low.astype(jnp.float32), high.astype(jnp.float32))
    mix_copy = remote(mix_sent, mix_got, mix_sem.at[0], mix_sem.at[1], me, other)
    mix_copy.start()
    mix_copy.wait_recv()
    mixed = resid[...] + mix_got[...].astype(jnp.float32)
    stay = (
        stream[...].astype(jnp.float32) + rms(mixed) * gain_mix[...].astype(jnp.float32).reshape(1, -1)
    ).astype(jnp.bfloat16).astype(jnp.float32)
    resid[...] = stay
    normed = rms(stay) * gain_pre[...].astype(jnp.float32).reshape(1, -1)
    tokens[0, pl.ds(pl.multiple_of(pad + z * half, 16), half), :] = normed.astype(jnp.bfloat16)
    span = reach * width // 16
    for r in range(reach):
        for j in range(16 // reach):
            at = r * (16 // reach) + j
            tail_f[at : at + 1, :] = normed[half - reach + r : half - reach + r + 1, j * span : (j + 1) * span]
    tail[...] = tail_f[...].astype(jnp.bfloat16)

    def block(side, at, q):
        return tokens.at[side, pl.ds(pl.multiple_of(pad + at * half + q * step_rows, 16), step_rows)]

    def flow(at, q, sems, to):
        return remote(block(0, at, q), block(0, at, q), sems.at[at, q], z_recv.at[at, q], to, core)

    def over_y(at, q):
        return remote(block(0, at, q), block(1, at, q), y_send.at[at, q], y_recv.at[at, q], y_mate, core)

    def z_wait(at, q):
        remote(block(0, at, q), block(0, at, q), up_send.at[at, q], z_recv.at[at, q], y_mate, core).wait_recv()

    def pass_on(at, q, up, down):
        if up:
            @pl.when(z < nz - 1)
            def _():
                flow(at, q, up_send, me + 4).start()
        if down:
            @pl.when(z > 0)
            def _():
                flow(at, q, dn_send, me - 4).start()
        over_y(at, q).start()

    for q in range(parts):
        pass_on(z, q, True, True)

    next_chip = jnp.where(core == 0, me, (me + 1) % count)

    def halo_copy(k):
        at = (place + k) % places
        return remote(
            tail, halos.at[next_chip // 2], halo_send.at[k], halo_recv.at[next_chip // 2],
            2 * at + next_chip % 2, other,
        )

    def send_halo(k, carry):
        halo_copy(k).start()
        return carry

    lax.fori_loop(0, places, send_halo, 0)
    pass_weights(0)
    forward_weights(1)

    for h in range(1, nz):
        for q in range(parts):
            @pl.when(z - h >= 0)
            def _():
                z_wait(z - h, q)
                pass_on(z - h, q, True, False)

            @pl.when(z + h < nz)
            def _():
                z_wait(z + h, q)
                pass_on(z + h, q, False, True)

        if h == 1:
            send_weights(2)

    def wait_halo(at, carry):
        remote(halos.at[at], halos.at[at], halo_send.at[at], halo_recv.at[at], me, other).wait_recv()
        return carry

    lax.fori_loop(0, places, wait_halo, 0)
    for side in range(2):
        for at in range(nz):
            p = at * 2 + jnp.where(side == 0, y, 1 - y)
            start = jnp.logical_and(jnp.logical_and(p == 0, x == 0), core == 0)
            block_tail = halos[p].astype(jnp.float32)
            block_tail = jnp.where(start, 0.0, block_tail)
            for r in range(reach):
                for j in range(16 // reach):
                    spot = r * (16 // reach) + j
                    halo_f[side, at * reach + r : at * reach + r + 1, j * span : (j + 1) * span] = (
                        block_tail[spot : spot + 1, :]
                    )
        tokens[side, 0:pad, :] = halo_f[side].astype(jnp.bfloat16)
    pass_weights(1)
    taps_copy.wait()
    forward_weights(2, 0, places // 2)
    across_wait(0)
    across_wait(1)

    def feed(side):
        rows_in = tokens[side]
        ups = []
        for which in range(2):
            ups.append(
                dot(rows_in, weights[which], ((1,), (1,))).astype(jnp.bfloat16).astype(jnp.float32)
            )
        padded[0] = ups[0]
        padded[1] = ups[1]
        taps = taps_own[...] + taps_got[...]
        for at in range(nz):
            for u in range(units // LANES):
                cut = slice(u * LANES, (u + 1) * LANES)
                smooth = []
                for which in range(2):
                    rows_u = padded[which, pad + at * half : pad + (at + 1) * half, cut]
                    place_u = lax.broadcasted_iota(jnp.int32, (half, LANES), 0)
                    total = 0.0
                    for j in range(reach + 1):
                        back = reach - j
                        shifted = rows_u
                        if back:
                            shifted = pltpu.roll(rows_u, back, 0)
                            for r in range(back):
                                spot = at * reach + reach - back + r
                                shifted = jnp.where(
                                    place_u == r, padded[which, spot : spot + 1, cut], shifted
                                )
                        tap = which * (reach + 1) + j
                        total = total + taps[tap : tap + 1, cut] * shifted
                    smooth.append(total)
                hidden[side, at * half : (at + 1) * half, cut] = (silu(smooth[0]) * smooth[1]).astype(jnp.bfloat16)

    def lower_rows(side, at):
        spot = slice(at * half, (at + 1) * half)
        for n in range(width // chunk):
            cut = slice(n * chunk, (n + 1) * chunk)
            terms[side, spot, cut] = dot(
                hidden[side, spot, :], weights[2, :, cut], ((1,), (0,))
            ).astype(jnp.bfloat16)

    def down(side):
        for n in range(width // chunk):
            cut = slice(n * chunk, (n + 1) * chunk)
            terms[side, :, cut] = dot(
                hidden[side], weights[2, :, cut], ((1,), (0,))
            ).astype(jnp.bfloat16)

    feed(0)
    forward_weights(2, places // 2, places)
    for at in range(nz):
        for q in range(parts):
            remote(block(1, at, q), block(1, at, q), y_send.at[at, q], y_recv.at[at, q], y_mate, core).wait_recv()
    feed(1)
    pass_weights(2)
    across_wait(2)
    down(1)

    def part_of(ref, lead, at, q):
        return ref.at[lead, pl.ds(pl.multiple_of(at * half + q * step_rows, 16), step_rows)]

    def sum_y(at, q):
        return remote(
            part_of(terms, 1, at, q), from_y.at[at, q], ry_send.at[at, q], ry_recv.at[at, q],
            y_mate, core,
        )

    def sum_z(at, q, upward):
        if upward:
            return remote(
                part_of(terms, 0, at, q), from_up.at[at, q], ru_send.at[at, q], ru_recv.at[at, q],
                me + 4, core,
            )
        return remote(
            part_of(terms, 0, at, q), from_down.at[at, q], rd_send.at[at, q], rd_recv.at[at, q],
            me - 4, core,
        )

    for h in list(range(nz - 1, 0, -1)):
        for q in range(parts):
            @pl.when(z + h < nz)
            def _():
                sum_y(z + h, q).start()

            @pl.when(z - h >= 0)
            def _():
                sum_y(z - h, q).start()
    for q in range(parts):
        sum_y(z, q).start()
    down(0)

    def rows_at(at, q):
        return pl.ds(pl.multiple_of(at * half + q * step_rows, 16), step_rows)

    def add_y(at, q):
        sum_y(at, q).wait_recv()
        terms[0, rows_at(at, q), :] = (
            terms[0, rows_at(at, q), :].astype(jnp.float32) + from_y[at, q].astype(jnp.float32)
        ).astype(jnp.bfloat16)

    def add_from(at, q, ref, sem):
        remote(ref.at[at, q], ref.at[at, q], ru_send.at[at, q], sem.at[at, q], y_mate, core).wait_recv()
        terms[0, rows_at(at, q), :] = (
            terms[0, rows_at(at, q), :].astype(jnp.float32) + ref[at, q].astype(jnp.float32)
        ).astype(jnp.bfloat16)

    for h in list(range(nz - 1, 0, -1)):
        for q in range(parts):
            @pl.when(z + h < nz)
            def _():
                add_y(z + h, q)

                @pl.when(z > 0)
                def _():
                    add_from(z + h, q, from_up, ru_recv)
                sum_z(z + h, q, True).start()

            @pl.when(z - h >= 0)
            def _():
                add_y(z - h, q)

                @pl.when(z < nz - 1)
                def _():
                    add_from(z - h, q, from_down, rd_recv)
                sum_z(z - h, q, False).start()
    for q in range(parts):
        add_y(z, q)

        @pl.when(z > 0)
        def _():
            add_from(z, q, from_up, ru_recv)

        @pl.when(z < nz - 1)
        def _():
            add_from(z, q, from_down, rd_recv)
    fed = terms[0, pl.ds(pl.multiple_of(z * half, 16), half), :].astype(jnp.float32)
    result[...] = (resid[...] + rms(fed) * gain_post[...].astype(jnp.float32).reshape(1, -1)).astype(jnp.bfloat16)

    def drain(k, carry):
        log_copy(k).wait_send()
        return carry

    lax.fori_loop(1, count, drain, 0)

    def drain_weights(k, carry):
        for which in range(3):
            weight_copy(which, k).wait_send()
        return carry

    lax.fori_loop(1, places, drain_weights, 0)

    def drain_over(k, carry):
        for which in range(3):
            over_x(which, k).wait_send()
        halo_copy(k).wait_send()
        return carry

    lax.fori_loop(0, places, drain_over, 0)
    for k in range(1, 4):
        one_copy(k).wait_send()
        two_copy(k).wait_send()
    for k in range(1, nz):
        @pl.when(z + k < nz)
        def _():
            plane_copy(k).wait_send()
    for which in range(3):
        across(which).wait_send()
    mix_copy.wait_send()

    def drain_blocks(at, carry):
        for q in range(parts):
            over_y(at, q).wait_send()
            sum_y(at, q).wait_send()

            @pl.when(jnp.logical_and(z < nz - 1, at <= z))
            def _():
                flow(at, q, up_send, me + 4).wait_send()

            @pl.when(jnp.logical_and(z > 0, at >= z))
            def _():
                flow(at, q, dn_send, me - 4).wait_send()

            @pl.when(at > z)
            def _():
                sum_z(at, q, True).wait_send()

            @pl.when(at < z)
            def _():
                sum_z(at, q, False).wait_send()
        return carry

    lax.fori_loop(0, nz, drain_blocks, 0)


def fused_layer(
    stream, q_wide, k_wide, v_wide, q_narrow, k_narrow, v_narrow, gate_wide, gate_narrow, log_decay,
    gain_wide, gain_narrow, out_wide, out_narrow, gain_mix, gain_pre, gain_post,
    weight_gate, weight_lin, weight_down, taps_gate, taps_lin,
):
    count, n_tp = lax.axis_size("sp"), lax.axis_size("tp")
    rows, width = q_wide.shape[0], stream.shape[1]
    places, nz = count // 2, count // 4
    heads = q_wide.shape[1] // KW
    columns = weight_gate.shape[1]
    share = columns // places
    units = share * n_tp
    reach = taps_gate.shape[0] - 1
    state_rows = heads * (KW * VW + KN * VN) // LANES
    piece = state_rows // 4
    tap_rows = 2 * (reach + 1)
    tap_rows += -tap_rows % 8
    half = rows // n_tp
    parts = 2
    values = out_wide.shape[0] + out_narrow.shape[0]
    dims = dict(
        count=count, n_tp=n_tp, rows=rows, width=width, share=share, piece=piece, reach=reach,
        chunk=512,
    )
    vmem = pl.BlockSpec(memory_space=pltpu.VMEM)
    anywhere = pl.BlockSpec(memory_space=pl.ANY)
    bf, f32 = jnp.bfloat16, jnp.float32
    dma = pltpu.SemaphoreType.DMA
    scratch = [
        pltpu.VMEM((3, weight_gate.shape[0], columns), bf),
        pltpu.VMEM((3, columns, weight_gate.shape[0]), bf),
        pltpu.VMEM((values, width), bf),
        pltpu.VMEM((3, units, width), bf),
        pltpu.VMEM((2, PAD + nz * half, width), bf),
        pltpu.VMEM((2, nz * half, width), bf),
        pltpu.VMEM((nz, parts, half // parts, width), bf),
        pltpu.VMEM((nz, parts, half // parts, width), bf),
        pltpu.VMEM((nz, parts, half // parts, width), bf),
        pltpu.VMEM((rows, heads * (KW + KN)), bf),
        pltpu.VMEM((rows, values), f32),
        pltpu.VMEM((state_rows, LANES), bf),
        pltpu.VMEM((4, piece, LANES), bf),
        pltpu.VMEM((piece, LANES), bf),
        pltpu.VMEM((nz, piece, LANES), bf),
        pltpu.VMEM((piece, LANES), f32),
        pltpu.VMEM((4, piece, LANES), bf),
        pltpu.VMEM((state_rows, LANES), bf),
        pltpu.VMEM((rows, values), bf),
        pltpu.VMEM((count, 2 * heads, LANES), f32),
        pltpu.VMEM((tap_rows, columns), f32),
        pltpu.VMEM((2 * heads, LANES), f32),
        pltpu.VMEM((count, 2 * heads, LANES), f32),
        pltpu.VMEM((tap_rows, units), f32),
        pltpu.VMEM((tap_rows, units), f32),
        pltpu.VMEM((half, width), bf),
        pltpu.VMEM((half, width), bf),
        pltpu.VMEM((half, width), f32),
        pltpu.VMEM((16, reach * width // 16), f32),
        pltpu.VMEM((16, reach * width // 16), bf),
        pltpu.VMEM((places, 16, reach * width // 16), bf),
        pltpu.VMEM((2, PAD, width), f32),
        pltpu.VMEM((2, PAD + nz * half, units), f32),
        pltpu.VMEM((2, nz * half, units), bf),
        dma((3,)), dma((2,)), dma((3,)), dma((3, places)), dma((3, places)), dma((3, places)),
        dma((3, places)), dma((3,)), dma((3,)),
        dma((count,)), dma((count,)), dma((4,)), dma((4,)), dma((nz,)), dma((nz,)), dma((4,)), dma((4,)),
        dma((2,)), dma((2,)), dma((places,)), dma((places,)),
    ] + [dma((nz, parts)) for _ in range(11)]
    kernel = pl.pallas_call(
        functools.partial(layer_kernel, dims),
        out_shape=jax.ShapeDtypeStruct(stream.shape, bf),
        in_specs=[vmem] * 18 + [anywhere] * 5,
        out_specs=vmem,
        scratch_shapes=scratch,
        compiler_params=pltpu.CompilerParams(
            collective_id=0, has_side_effects=True, vmem_limit_bytes=VMEM_BYTES
        ),
    )
    return kernel(
        stream, q_wide, k_wide, v_wide, q_narrow, k_narrow, v_narrow, gate_wide, gate_narrow,
        log_decay, gain_wide, gain_narrow, gain_mix, gain_pre, gain_post,
        jnp.asarray(tables_of(count, rows)), taps_gate, taps_lin, out_wide, out_narrow,
        weight_gate, weight_lin, weight_down,
    )


def fits(stream, q_wide, log_decay, weight_gate, taps_gate):
    count, n_tp = lax.axis_size("sp"), lax.axis_size("tp")
    rows, width = q_wide.shape[0], stream.shape[1]
    if n_tp != 2 or count % 4 or count < 8 or rows != BLOCK or q_wide.shape[1] % (2 * KW):
        return False
    heads = q_wide.shape[1] // KW
    units = weight_gate.shape[1]
    state_rows = heads * (KW * VW + KN * VN) // LANES
    reach = taps_gate.shape[0] - 1
    held = units // (count // 2)
    return (
        2 * heads == 8
        and weight_gate.shape[0] == LANES
        and units % (count // 2 * 16) == 0
        and (n_tp * held) % LANES == 0
        and state_rows % (4 * 16) == 0
        and reach == 2
        and (count // 4) * reach <= PAD
        and width % 512 == 0
        and 3 * n_tp * held * width <= 5 * 2 ** 20
    )


def body(
    stream,
    wide_head_query,
    broad_attention_lookup_vectors,
    values_wide,
    query_narrow,
    keys_narrow,
    values_narrow,
    gate_wide,
    gate_narrow,
    log_decay,
    gain_wide,
    gain_narrow,
    out_wide,
    out_narrow,
    gain_mix,
    gain_pre,
    gain_post,
    weight_gate,
    weight_lin,
    weight_down,
    taps_gate,
    taps_lin,
):
    if fits(stream, wide_head_query, log_decay, weight_gate, taps_gate):
        return fused_layer(
            stream, wide_head_query, broad_attention_lookup_vectors, values_wide, query_narrow,
            keys_narrow, values_narrow, gate_wide, gate_narrow, log_decay, gain_wide, gain_narrow,
            out_wide, out_narrow, gain_mix, gain_pre, gain_post, weight_gate, weight_lin,
            weight_down, taps_gate, taps_lin,
        )
    rows = wide_head_query.shape[0]
    count = lax.axis_size("sp")
    n_tp = lax.axis_size("tp")
    width = stream.shape[1]
    units = weight_gate.shape[1]
    by_tokens = 2 * count * rows < 3 * units and units % (count * 16) == 0
    by_tokens = by_tokens and count & (count - 1) == 0
    if by_tokens:
        weights, taps = unit_slices(weight_gate, weight_lin, weight_down, taps_gate, taps_lin)
    offset = lax.axis_index("sp") * rows
    rates_wide = log_decay[0]
    rates_narrow = log_decay[1]
    rot_wide, local_wide, state_wide = kept_nearby_memory(
        wide_head_query, broad_attention_lookup_vectors, values_wide, rates_wide, KW, VW, offset
    )
    rot_narrow, local_narrow, state_narrow = kept_nearby_memory(
        query_narrow, keys_narrow, values_narrow, rates_narrow, KN, VN, offset
    )
    incoming = carried_in(
        (state_wide, state_narrow),
        (jnp.sum(rates_wide, axis=1), jnp.sum(rates_narrow, axis=1)),
        "sp",
    )
    gated_wide = gate_heads(
        local_wide + carried(rot_wide, rates_wide, incoming[0]), gain_wide, gate_wide
    )
    gated_narrow = gate_heads(
        local_narrow + carried(rot_narrow, rates_narrow, incoming[1]), gain_narrow, gate_narrow
    )
    part_wide = jnp.dot(gated_wide, out_wide, preferred_element_type=jnp.float32)
    part_narrow = jnp.dot(gated_narrow, out_narrow, preferred_element_type=jnp.float32)
    mixed = share_rows(
        (part_wide + part_narrow).astype(jnp.bfloat16).reshape(n_tp, rows // n_tp, width), "tp"
    )
    resid = (stream.astype(jnp.float32) + scale_rows(mixed, gain_mix)).astype(jnp.bfloat16)
    normed_in = scale_rows(resid.astype(jnp.float32), gain_pre).astype(jnp.bfloat16)
    if by_tokens:
        fed = feed_by_tokens(normed_in, weights, taps)
    else:
        fed = feed_by_weights(normed_in, weight_gate, weight_lin, weight_down, taps_gate, taps_lin)
    return (resid.astype(jnp.float32) + scale_rows(fed, gain_post)).astype(jnp.bfloat16)


def solution(mesh):
    in_specs = (
        P(("sp", "tp"), None),
        P("sp", "tp"),
        P("sp", "tp"),
        P("sp", "tp"),
        P("sp", "tp"),
        P("sp", "tp"),
        P("sp", "tp"),
        P("sp", "tp"),
        P("sp", "tp"),
        P(None, "tp", "sp"),
        P("tp"),
        P("tp"),
        P("tp", None),
        P("tp", None),
        P(),
        P(),
        P(),
        P("sp", "tp"),
        P("sp", "tp"),
        P("sp", "tp"),
        P(None, "tp"),
        P(None, "tp"),
    )
    out_specs = P(("sp", "tp"), None)
    return jax.shard_map(body, mesh=mesh, in_specs=in_specs, out_specs=out_specs, check_vma=False)
```

```python
import functools

import jax
import jax.numpy as jnp
import numpy as np
from jax import lax
from jax.experimental import pallas as pl
from jax.experimental.pallas import tpu as pltpu
from jax.sharding import PartitionSpec as P

KW = 128
VW = 256
KN = 64
VN = 128
BLOCK = 128


EPS = 1e-06
THETA = 10000.0
LANES = 128
PAD = 16
VMEM_BYTES = 60 * 2**20


def passed_along(value, axis, steps):
    count = lax.axis_size(axis)
    first, last = (max(0, -steps), min(count, count - steps))
    return lax.ppermute(value, axis, [(source, source + steps) for source in range(first, last)])


def rotate(block, positions):
    width = block.shape[-1]
    half = width // 2
    frequency = THETA ** (-(jnp.arange(half, dtype=jnp.float32) * 2.0 / width))
    angles = positions.astype(jnp.float32)[:, None] * frequency[None, :]
    cosine = jnp.cos(angles)[:, None, :]
    sine = jnp.sin(angles)[:, None, :]
    values = block.astype(jnp.float32)
    first = values[..., :half]
    second = values[..., half:]
    return jnp.concatenate(
        [first * cosine - second * sine, second * cosine + first * sine], axis=-1
    )


def block_step(state, inputs):
    query, keys, values, log_rate = inputs
    running = jnp.cumsum(log_rate, axis=1)
    length = running.shape[1]
    index = jnp.arange(length)
    lower = (index[:, None] >= index[None, :])[None]
    spread = jnp.where(
        lower, jnp.exp(jnp.where(lower, running[:, :, None] - running[:, None, :], 0.0)), 0.0
    )
    scores = (
        jnp.einsum("ihd,jhd->hij", query, keys, preferred_element_type=jnp.float32) * spread
    ).astype(jnp.bfloat16)
    inner = jnp.einsum("hij,jhe->ihe", scores, values, preferred_element_type=jnp.float32)
    lifted = query.astype(jnp.float32) * jnp.exp(running).T[:, :, None]
    cross = jnp.einsum("ihd,hde->ihe", lifted, state, precision=lax.Precision.HIGHEST)
    tail = running[:, -1:]
    scaled = (keys.astype(jnp.float32) * jnp.exp(tail - running).T[:, :, None]).astype(jnp.bfloat16)
    update = jnp.einsum("jhd,jhe->hde", scaled, values, preferred_element_type=jnp.float32)
    state = state * jnp.exp(tail)[:, :, None] + update
    return (state, inner + cross)


def kept_nearby_memory(query, keys, values, log_rate, head_dim, value_dim, offset):
    rows = query.shape[0]
    heads = query.shape[1] // head_dim
    positions = offset + jnp.arange(rows, dtype=jnp.int32)
    rotated_query = rotate(query.reshape(rows, heads, head_dim), positions).astype(jnp.bfloat16)
    rotated_keys = (
        rotate(keys.reshape(rows, heads, head_dim), positions) * head_dim ** (-0.5)
    ).astype(jnp.bfloat16)
    layer_groups_list = rows // BLOCK

    def split(array):
        return array.reshape(layer_groups_list, BLOCK, heads, array.shape[-1])

    rates = jnp.transpose(log_rate.reshape(heads, layer_groups_list, BLOCK), (1, 0, 2))
    start = jnp.zeros((heads, head_dim, value_dim), jnp.float32)
    inputs = (
        split(rotated_query),
        split(rotated_keys),
        split(values.reshape(rows, heads, value_dim)),
        rates,
    )
    state, outs = lax.scan(block_step, start, inputs)
    return (rotated_query, outs.reshape(rows, heads, value_dim), state)


def carried(rotated_query, log_rate, state_in):
    lifted = rotated_query.astype(jnp.float32) * jnp.exp(jnp.cumsum(log_rate, axis=1)).T[:, :, None]
    return jnp.einsum("ihd,hde->ihe", lifted, state_in, precision=lax.Precision.HIGHEST)


def gate_heads(retained, gain, gate):
    mean = jnp.mean(retained, axis=-1, keepdims=True)
    centred = retained - mean
    variance = jnp.mean(centred * centred, axis=-1, keepdims=True)
    normed = (centred * lax.rsqrt(variance + EPS)).reshape(retained.shape[0], -1)
    return (normed * gain.astype(jnp.float32) * jax.nn.silu(gate.astype(jnp.float32))).astype(
        jnp.bfloat16
    )


def scale_rows(rows, gain):
    return (
        rows
        * lax.rsqrt(jnp.mean(rows * rows, axis=-1, keepdims=True) + EPS)
        * gain.astype(jnp.float32)
    )


def causal_taps(upward, before, taps):
    width = taps.shape[0]
    total = upward.shape[0]
    padded_rows = jnp.concatenate([before, upward], axis=0).astype(jnp.float32)
    smooth = jnp.zeros((total, upward.shape[1]), jnp.float32)
    for tap_index in range(width):
        smooth = (
            smooth
            + taps[tap_index].astype(jnp.float32)[None, :]
            * padded_rows[tap_index : tap_index + total]
        )
    return smooth


def swap_blocks(blocks, axis):
    return lax.all_to_all(blocks, axis, 0, 0, tiled=False)


def share_rows(parts, axis):
    count = lax.axis_size(axis)
    place = lax.axis_index(axis)
    total = lax.dynamic_index_in_dim(parts, place, 0, False).astype(jnp.float32)
    for step in range(1, count):
        piece = lax.dynamic_index_in_dim(parts, (place + step) % count, 0, False)
        moved = lax.ppermute(piece, axis, [(i, (i + step) % count) for i in range(count)])
        total = total + moved.astype(jnp.float32)
    return total


def carried_in(states, totals, axis):
    count = lax.axis_size(axis)
    lanes = states[-1].shape[-1]
    flat = jnp.concatenate([s.reshape(-1, lanes) for s in states]).astype(jnp.bfloat16)
    rates = jnp.concatenate(
        [jnp.repeat(d, s.size // s.shape[0] // lanes) for s, d in zip(states, totals)]
    )
    share = flat.shape[0] // count
    rates = rates.reshape(count, share)
    rates = jnp.pad(rates, ((0, 0), (0, -share % lanes)))
    parts, left = [], rates
    for _ in range(3):
        parts.append(left.astype(jnp.bfloat16))
        left = left - parts[-1].astype(jnp.float32)
    parts = [part.reshape(count, -1, lanes) for part in parts]
    sent = jnp.concatenate([flat.reshape(count, share, lanes)] + parts, axis=1)
    got = swap_blocks(sent, axis).astype(jnp.float32)
    parts = jnp.split(got[:, share:], 3, axis=1)
    logs = (parts[0] + parts[1] + parts[2]).reshape(count, -1)[:, :share]
    own = got[:, :share]
    steps = jnp.arange(count)
    between = (steps[None, None] > steps[None, :, None]) & (
        steps[None, None] < steps[:, None, None]
    )
    span = jnp.sum(jnp.where(between[..., None], logs[None, None], 0.0), axis=2)
    factor = jnp.where((steps[None] < steps[:, None])[..., None], jnp.exp(span), 0.0)
    before = sum(factor[:, step, :, None] * own[step][None] for step in range(count))
    back = swap_blocks(before.astype(jnp.bfloat16), axis).reshape(-1, lanes).astype(jnp.float32)
    outs, at = [], 0
    for s in states:
        rows = s.size // lanes
        outs.append(back[at : at + rows].reshape(s.shape))
        at += rows
    return outs


def feed_by_weights(normed_in, weight_gate, weight_lin, weight_down, taps_gate, taps_lin):
    normed_all = lax.all_gather(normed_in, "tp", axis=0, tiled=True)
    rows = normed_all.shape[0]
    whole_gate, whole_lin = (
        lax.all_gather(weight_gate, "sp", axis=0, tiled=True),
        lax.all_gather(weight_lin, "sp", axis=0, tiled=True),
    )
    up_gate = jnp.dot(normed_all, whole_gate, preferred_element_type=jnp.float32).astype(
        jnp.bfloat16
    )
    up_lin = jnp.dot(normed_all, whole_lin, preferred_element_type=jnp.float32).astype(jnp.bfloat16)
    reach = taps_gate.shape[0] - 1
    before_gate, before_lin = passed_along(
        (up_gate[rows - reach :], up_lin[rows - reach :]), "sp", 1
    )
    smooth_gate = causal_taps(up_gate, before_gate, taps_gate)
    smooth_lin = causal_taps(up_lin, before_lin, taps_lin)
    hidden = (jax.nn.silu(smooth_gate) * smooth_lin).astype(jnp.bfloat16)
    terms = lax.dot_general(
        hidden,
        lax.all_gather(weight_down, "sp", axis=0, tiled=True),
        (((1,), (1,)), ((), ())),
        preferred_element_type=jnp.float32,
    )
    return lax.psum_scatter(
        terms.astype(jnp.bfloat16), "tp", scatter_dimension=0, tiled=True
    ).astype(jnp.float32)


def from_all(value, axis, dim):
    count = lax.axis_size(axis)
    found = [value]
    for step in range(1, count):
        found.append(lax.ppermute(value, axis, [(i, (i + step) % count) for i in range(count)]))
    return jnp.concatenate(found, axis=dim)


def unit_slices(weight_gate, weight_lin, weight_down, taps_gate, taps_lin):
    count = lax.axis_size("sp")
    place = lax.axis_index("sp")
    deep, units = weight_gate.shape
    share = units // count
    turned = jnp.stack([weight_gate.T, weight_lin.T, weight_down.T])
    blocks = turned.reshape(3, count, share, deep).transpose(1, 0, 2, 3)
    got = swap_blocks(blocks, "sp")
    mine = got.transpose(1, 2, 0, 3).reshape(3, share, count * deep)
    taps = jnp.stack([taps_gate, taps_lin])
    taps = lax.dynamic_slice_in_dim(taps, place * share, share, 2)
    return from_all(mine, "tp", 1), from_all(taps, "tp", 2)


def flip(value, axis, bit):
    return lax.ppermute(
        value, axis, [(i, i ^ (1 << bit)) for i in range(lax.axis_size(axis))]
    )


def bits_of(count, swapped):
    bits = list(range(count.bit_length() - 1))
    if swapped:
        bits[:2] = bits[:2][::-1]
    return bits


def gather_around(value, axis, swapped):
    bits = bits_of(lax.axis_size(axis), swapped)
    for bit in bits[::-1]:
        value = jnp.stack([value, flip(value, axis, bit)])
    order = [bits.index(bit) for bit in sorted(bits, reverse=True)]
    value = value.transpose(*order, *range(len(bits), value.ndim))
    return value.reshape(-1, *value.shape[len(bits) :])


def add_around(value, axis, swapped):
    bits = bits_of(lax.axis_size(axis), swapped)
    value = value.reshape(*[2] * len(bits), *value.shape[1:])
    dims = sorted(bits, reverse=True)
    for bit in bits:
        at = dims.index(bit)
        dims.remove(bit)
        kept = lax.index_in_dim(value, 0, at, False).astype(jnp.float32)
        sent = lax.index_in_dim(value, 1, at, False).astype(jnp.bfloat16)
        value = kept + flip(sent, axis, bit).astype(jnp.float32)
        if dims:
            value = value.astype(jnp.bfloat16)
    return value


def feed_by_tokens(normed_in, weights, taps):
    count = lax.axis_size("sp")
    n_tp = lax.axis_size("tp")
    rows, width = normed_in.shape
    place = lax.axis_index("sp")
    half = width // 2
    flat = weights[:2].reshape(-1, width)
    units = flat.shape[0] // 2
    ups = 0.0
    for part in range(2):
        cut = slice(part * half, (part + 1) * half)
        tokens = gather_around(normed_in[:, cut], "sp", part == 1)
        ups = ups + lax.dot_general(
            tokens.reshape(count * rows, half),
            flat[:, cut],
            (((1,), (1,)), ((), ())),
            preferred_element_type=jnp.float32,
        )
    ups = ups.astype(jnp.bfloat16).reshape(count, rows, 2 * units)
    reach = taps.shape[1] - 1
    tails = ups[:, rows - reach :]
    prior = lax.ppermute(tails, "tp", [(i, (i + 1) % n_tp) for i in range(n_tp)])
    prior = jnp.roll(prior.reshape(count, reach, 2, n_tp, -1), 1, axis=3).reshape(prior.shape)
    blocks = place ^ jnp.arange(count)
    follows = (blocks[:, None] == blocks[None, :] + 1).astype(jnp.bfloat16)
    shifted = jnp.dot(
        follows, prior.reshape(count, -1), preferred_element_type=jnp.float32
    ).astype(jnp.bfloat16).reshape(prior.shape)
    prior = jnp.where(lax.axis_index("tp") == 0, shifted, prior)
    padded = jnp.concatenate([prior, ups], axis=1).astype(jnp.float32)
    taps = jnp.concatenate([taps[0], taps[1]], axis=1).astype(jnp.float32)
    smooth = sum(taps[j] * padded[:, j : j + rows] for j in range(reach + 1))
    hidden = (jax.nn.silu(smooth[..., :units]) * smooth[..., units:]).astype(jnp.bfloat16)
    hidden = hidden.reshape(count * rows, units)
    sums = []
    for part in range(2):
        cut = slice(part * half, (part + 1) * half)
        terms = jnp.dot(hidden, weights[2][:, cut], preferred_element_type=jnp.float32)
        terms = terms.astype(jnp.bfloat16).reshape(count, rows, half)
        sums.append(add_around(terms, "sp", part == 1))
    return jnp.concatenate(sums, axis=1)


def tables_of(count, rows):
    def angles(positions, width):
        half = width // 2
        frequency = THETA ** (-(np.arange(half, dtype=np.float64) * 2.0 / width))
        return np.tile(positions[:, None] * frequency[None, :], (1, LANES // half))

    positions = np.concatenate([np.arange(rows), np.arange(count) * rows]).astype(np.float64)
    found = []
    for width in (KW, KN):
        turned = angles(positions, width)
        found += [np.cos(turned), np.sin(turned)]
    return np.stack(found).astype(np.float32)


def remote(source, target, sent, got, sp, tp):
    return pltpu.make_async_remote_copy(
        src_ref=source, dst_ref=target, send_sem=sent, recv_sem=got,
        device_id=(sp, tp), device_id_type=pl.DeviceIdType.MESH,
    )


def silu(value):
    return value / (1.0 + jnp.exp(-value))


def rms(value):
    return value * lax.rsqrt(jnp.mean(value * value, axis=-1, keepdims=True) + EPS)


def layer_kernel(
    dims,
    stream, q_wide, k_wide, v_wide, q_narrow, k_narrow, v_narrow, gate_wide, gate_narrow,
    decay, gain_wide, gain_narrow, gain_mix, gain_pre, gain_post, tables, taps_gate, taps_lin,
    out_wide_hbm, out_narrow_hbm, weight_gate, weight_lin, weight_down,
    result,
    raw, turned, out_w, weights, tokens, terms, from_y, from_up, from_down, rotated, local, states,
    got, plane_sum, planes, carry, before, state_in, gated, fades, taps_all, logs_own, logs, taps_own, taps_got, mix_sent, mix_got, resid, tail_f, tail, halos, halo_f,
    padded, hidden,
    raw_sem, out_sem, own_sem, w_send, w_recv, xw_send, xw_recv, dw_send, dw_recv,
    log_send, log_recv, one_send, one_recv, z_sum_send, z_sum_recv, two_send, two_recv, tap_sem, mix_sem,
    halo_send, halo_recv, up_send, dn_send, y_send, z_recv, y_recv,
    ry_send, ry_recv, ru_send, ru_recv, rd_send, rd_recv,
):
    count, n_tp = dims["count"], dims["n_tp"]
    rows, width = dims["rows"], dims["width"]
    half = rows // n_tp
    places = count // 2
    nz = count // 4
    share = dims["share"]
    n_tiles = share * places // LANES
    units = n_tp * share
    piece = dims["piece"]
    reach = dims["reach"]
    parts = 2
    step_rows = half // parts
    pad = PAD
    me = lax.axis_index("sp")
    core = lax.axis_index("tp")
    other = 1 - core
    x = me % 2
    y = (me // 2) % 2
    z = me // 4
    place = me // 2
    x_mate = me + 1 - 2 * x
    y_mate = me + 2 - 4 * y
    mine = pl.multiple_of(me * LANES, LANES)

    def in_plane(k):
        at = (place + k) % places
        return at, 2 * at + x

    barrier = pltpu.get_barrier_semaphore()

    def greet(k, carry):
        to = (me * n_tp + core + k) % (count * n_tp)
        pl.semaphore_signal(
            barrier, inc=1, device_id=(to // n_tp, to % n_tp),
            device_id_type=pl.DeviceIdType.MESH,
        )
        return carry

    lax.fori_loop(1, count * n_tp, greet, 0)

    wide_rows = out_wide_hbm.shape[0]
    narrow_rows = out_narrow_hbm.shape[0]
    out_copies = [
        pltpu.make_async_copy(out_wide_hbm, out_w.at[pl.ds(0, wide_rows)], out_sem.at[0]),
        pltpu.make_async_copy(out_narrow_hbm, out_w.at[pl.ds(wide_rows, narrow_rows)], out_sem.at[1]),
    ]
    raw_copies = [
        pltpu.make_async_copy(source, raw.at[which], raw_sem.at[which])
        for which, source in enumerate((weight_gate, weight_lin, weight_down))
    ]
    for copy in raw_copies + out_copies:
        copy.start()

    def own_rows(at):
        return pl.ds(pl.multiple_of(at * share, 16), share)

    core_rows = pl.ds(pl.multiple_of(core * share, 16), share)

    def weight_copy(which, k):
        at, to = in_plane(k)
        return remote(
            turned.at[which, own_rows(at)], weights.at[which, core_rows, pl.ds(mine, LANES)],
            w_send.at[which, k], w_recv.at[which, k], to, core,
        )

    def weight_wait(which, k):
        from_at = (place + places - k) % places
        columns = pl.ds(pl.multiple_of((2 * from_at + x) * LANES, LANES), LANES)
        spot = weights.at[which, core_rows, columns]
        remote(spot, spot, w_send.at[which, k], w_recv.at[which, k], x_mate, core).wait_recv()

    def over_x(which, k):
        from_at = (place + places - k) % places
        columns = pl.ds(pl.multiple_of((2 * from_at + x) * LANES, LANES), LANES)
        spot = weights.at[which, core_rows, columns]
        return remote(spot, spot, xw_send.at[which, k], xw_recv.at[which, k], x_mate, core)

    def over_x_wait(which, k):
        from_at = (place + places - k) % places
        columns = pl.ds(pl.multiple_of((2 * from_at + 1 - x) * LANES, LANES), LANES)
        spot = weights.at[which, core_rows, columns]
        remote(spot, spot, xw_send.at[which, k], xw_recv.at[which, k], x_mate, core).wait_recv()

    def columns_of(side, k):
        from_at = (place + places - k) % places
        column = 2 * from_at + (x if side == 0 else 1 - x)
        return pl.ds(pl.multiple_of(column * LANES, LANES), LANES)

    def across(which, side, k):
        spot = weights.at[which, core_rows, columns_of(side, k)]
        return remote(spot, spot, dw_send.at[which, side, k], dw_recv.at[which, side, k], me, other)

    def across_wait(which):
        other_rows = pl.ds(pl.multiple_of(other * share, 16), share)
        for side in range(2):
            def go(k, carried_):
                spot = weights.at[which, other_rows, columns_of(side, k)]
                remote(
                    spot, spot, dw_send.at[which, side, k], dw_recv.at[which, side, k], me, other
                ).wait_recv()
                return carried_
            lax.fori_loop(0, places, go, 0)

    def own_copy(which):
        return pltpu.make_async_copy(
            turned.at[which, own_rows(place)], weights.at[which, core_rows, pl.ds(mine, LANES)],
            own_sem.at[which],
        )

    def send_weights(which, first=1, step=1):
        def go(i, carried_):
            weight_copy(which, first + step * i).start()
            return carried_
        lax.fori_loop(0, (places - 1 - first) // step + 1, go, 0)

    def forward_weights(which, first=0, step=1, last=places):
        if first == 0:
            own_copy(which).wait()
            over_x(which, 0).start()
            across(which, 0, 0).start()
            first = step

        def go(i, carried_):
            k = first + step * i
            weight_wait(which, k)
            over_x(which, k).start()
            across(which, 0, k).start()
            return carried_
        lax.fori_loop(0, (last - 1 - first) // step + 1, go, 0)

    def pass_weights(which):
        def go(k, carried_):
            over_x_wait(which, k)
            across(which, 1, k).start()
            return carried_
        lax.fori_loop(0, places, go, 0)

    def turn(which):
        raw_copies[which].wait()
        for at in range(n_tiles):
            cut = slice(at * LANES, (at + 1) * LANES)
            turned[which, cut, :] = raw[which, :, cut].T
        own_copy(which).start()

    i_at = lax.broadcasted_iota(jnp.int32, (rows, rows), 0)
    j_at = lax.broadcasted_iota(jnp.int32, (rows, rows), 1)
    lower = i_at >= j_at
    lower_f = lower.astype(jnp.float32)
    upper_f = (i_at <= j_at).astype(jnp.float32)
    rates = decay[...].reshape(-1, rows)
    run_rows = lax.dot_general(
        rates, upper_f, (((1,), (0,)), ((), ())), precision=lax.Precision.HIGHEST,
        preferred_element_type=jnp.float32,
    )
    run_cols = lax.dot_general(
        lower_f, rates, (((1,), (1,)), ((), ())), precision=lax.Precision.HIGHEST,
        preferred_element_type=jnp.float32,
    )
    totals = run_rows[:, rows - 1 : rows]
    logs_own[...] = jnp.broadcast_to(totals, logs_own.shape)
    logs[me] = jnp.broadcast_to(totals, logs_own.shape)

    def peer(k):
        return (me + k) % count

    def log_copy(k):
        return remote(logs_own, logs.at[me], log_send.at[k], log_recv.at[k], peer(k), core)

    def send_logs(k, carry):
        log_copy(k).start()
        return carry

    heads = wide_rows // VW
    lane = lax.broadcasted_iota(jnp.int32, (rows, LANES), 1)

    def angle_table(first, half_width):
        cos_i, sin_i = tables[first, 0:rows, :], tables[first + 1, 0:rows, :]
        cos_o = tables[first, pl.ds(rows + me, 1), :]
        sin_o = tables[first + 1, pl.ds(rows + me, 1), :]
        cosine = cos_o * cos_i - sin_o * sin_i
        sine = sin_o * cos_i + cos_o * sin_i
        early = lane % (2 * half_width) < half_width
        return cosine, jnp.where(early, -sine, sine), early

    cos_w, sin_w, _ = angle_table(0, KW // 2)

    def dot(a, b, dims_):
        return lax.dot_general(a, b, (dims_, ((), ())), preferred_element_type=jnp.float32)

    def spread_of(column, row):
        return jnp.where(lower, jnp.exp(jnp.where(lower, column - row, 0.0)), 0.0)

    for h in range(heads):
        cut = slice(h * KW, (h + 1) * KW)
        query = q_wide[:, cut].astype(jnp.float32)
        query = (query * cos_w + pltpu.roll(query, KW // 2, 1) * sin_w).astype(jnp.bfloat16)
        keys = k_wide[:, cut].astype(jnp.float32)
        keys = ((keys * cos_w + pltpu.roll(keys, KW // 2, 1) * sin_w) * KW ** (-0.5)).astype(jnp.bfloat16)
        column, row = run_cols[:, h : h + 1], run_rows[h : h + 1, :]
        scores = (dot(query, keys, ((1,), (1,))) * spread_of(column, row)).astype(jnp.bfloat16)
        values = v_wide[:, h * VW : (h + 1) * VW]
        local[:, h * VW : (h + 1) * VW] = dot(scores, values, ((1,), (0,)))
        last = totals[h : h + 1, :]
        scaled = (keys.astype(jnp.float32) * jnp.exp(last - column)).astype(jnp.bfloat16)
        state = dot(scaled, values, ((0,), (0,))).astype(jnp.bfloat16)
        for e in range(VW // LANES):
            at = (h * (VW // LANES) + e) * KW
            states[at : at + KW, :] = state[:, e * LANES : (e + 1) * LANES]
        rotated[:, cut] = (query.astype(jnp.float32) * jnp.exp(column)).astype(jnp.bfloat16)

    cos_n, sin_n, early_n = angle_table(2, KN // 2)

    def swap_narrow(value):
        return jnp.where(
            early_n, pltpu.roll(value, LANES - KN // 2, 1), pltpu.roll(value, KN // 2, 1)
        )

    base_wide = wide_rows // LANES * KW
    first_head = lane < KN
    for g in range(heads // 2):
        cut = slice(g * LANES, (g + 1) * LANES)
        query = q_narrow[:, cut].astype(jnp.float32)
        query = (query * cos_n + swap_narrow(query) * sin_n).astype(jnp.bfloat16)
        keys = k_narrow[:, cut].astype(jnp.float32)
        keys = ((keys * cos_n + swap_narrow(keys) * sin_n) * KN ** (-0.5)).astype(jnp.bfloat16)
        spot = heads + 2 * g
        columns = [run_cols[:, spot + e : spot + e + 1] for e in range(2)]
        lasts = [totals[spot + e : spot + e + 1, :] for e in range(2)]
        falls = jnp.where(
            first_head, jnp.exp(lasts[0] - columns[0]), jnp.exp(lasts[1] - columns[1])
        )
        scaled = (keys.astype(jnp.float32) * falls).astype(jnp.bfloat16)
        rises = jnp.where(first_head, jnp.exp(columns[0]), jnp.exp(columns[1]))
        query_f = query.astype(jnp.float32)
        rotated[:, heads * KW + g * LANES : heads * KW + (g + 1) * LANES] = (
            query_f * rises
        ).astype(jnp.bfloat16)
        for e in range(2):
            h = 2 * g + e
            own = first_head if e == 0 else jnp.logical_not(first_head)
            masked = jnp.where(own, query_f, 0.0).astype(jnp.bfloat16)
            scores = (
                dot(masked, keys, ((1,), (1,)))
                * spread_of(columns[e], run_rows[spot + e : spot + e + 1, :])
            ).astype(jnp.bfloat16)
            values = v_narrow[:, h * VN : (h + 1) * VN]
            local[:, wide_rows + h * VN : wide_rows + (h + 1) * VN] = dot(scores, values, ((1,), (0,)))
            state = dot(scaled, values, ((0,), (0,))).astype(jnp.bfloat16)
            at = base_wide + h * KN
            states[at : at + KN, :] = state[e * KN : (e + 1) * KN, :]

    pl.semaphore_wait(barrier, count * n_tp - 1)
    spot_in = me % 4
    plane_at = z * 4

    def piece_rows(at):
        return pl.ds(pl.multiple_of(at * piece, 16), piece)

    def mate(k):
        return (spot_in + k) % 4

    def one_copy(k):
        return remote(
            states.at[piece_rows(mate(k))], got.at[spot_in], one_send.at[k], one_recv.at[k],
            plane_at + mate(k), core,
        )

    for k in range(1, 4):
        one_copy(k).start()
    lax.fori_loop(1, count, send_logs, 0)
    got[spot_in] = states[piece_rows(spot_in), :]
    turn(0)
    send_weights(0, 2, 2)
    taps_all[...] = jnp.zeros_like(taps_all)
    taps_all[0 : reach + 1, :] = taps_gate[...].astype(jnp.float32)
    taps_all[reach + 1 : 2 * (reach + 1), :] = taps_lin[...].astype(jnp.float32)
    taps_mine = pltpu.roll(taps_all[...], (share * places - place * share) % (share * places), 1)[:, :units]
    taps_lane = lax.broadcasted_iota(jnp.int32, taps_own.shape, 1)
    taps_mine = jnp.where(taps_lane < share, taps_mine, 0.0)
    taps_own[...] = jnp.where(core == 0, taps_mine, pltpu.roll(taps_mine, share, 1))
    taps_copy = remote(taps_own, taps_got, tap_sem.at[0], tap_sem.at[1], me, other)
    taps_copy.start()

    def source(k):
        return (me + count - k) % count

    def wait_logs(k, carried_):
        at = source(k)
        remote(logs.at[at], logs.at[at], log_send.at[k], log_recv.at[k], at, core).wait_recv()
        return carried_

    for k in range(1, 4):
        at = (spot_in + 4 - k) % 4
        remote(got.at[at], got.at[at], one_send.at[k], one_recv.at[k], plane_at + at, core).wait_recv()
    lax.fori_loop(1, count, wait_logs, 0)
    fades[...] = jnp.exp(logs[...])
    groups_wide = VW // LANES * KW // 16
    groups_narrow = KN // 16

    def head_of(i):
        g = spot_in * (piece // 16) + i
        head = jnp.where(
            g < heads * groups_wide, g // groups_wide,
            heads + (g - heads * groups_wide) // groups_narrow,
        )
        return jnp.minimum(head, 2 * heads - 1)

    def fade_of(chip, i):
        return fades[chip, pl.ds(head_of(i), 1), :]

    for i in range(piece // 16):
        cut = slice(i * 16, (i + 1) * 16)
        total = got[0, cut, :].astype(jnp.float32)
        for t in range(1, 4):
            total = total * fade_of(plane_at + t, i) + got[t, cut, :].astype(jnp.float32)
        plane_sum[cut, :] = total.astype(jnp.bfloat16)

    def plane_copy(k):
        return remote(plane_sum, planes.at[z], z_sum_send.at[k], z_sum_recv.at[k], me + 4 * k, core)

    for k in range(1, nz):
        @pl.when(z + k < nz)
        def _():
            plane_copy(k).start()
    carry[...] = jnp.zeros_like(carry)
    turn(1)
    turn(2)

    def add_plane(at, carried_):
        k = z - at
        remote(planes.at[at], planes.at[at], z_sum_send.at[k], z_sum_recv.at[k], me - 4 * k, core).wait_recv()
        for i in range(piece // 16):
            cut = slice(i * 16, (i + 1) * 16)
            fade = fade_of(at * 4, i)
            for t in range(1, 4):
                fade = fade * fade_of(at * 4 + t, i)
            carry[cut, :] = carry[cut, :] * fade + planes[at, cut, :].astype(jnp.float32)
        return carried_

    lax.fori_loop(0, z, add_plane, 0)
    for i in range(piece // 16):
        cut = slice(i * 16, (i + 1) * 16)
        total = carry[cut, :]
        for t in range(4):
            before[t, cut, :] = total.astype(jnp.bfloat16)
            if t < 3:
                total = total * fade_of(plane_at + t, i) + got[t, cut, :].astype(jnp.float32)

    def two_copy(k):
        return remote(
            before.at[mate(k)], state_in.at[piece_rows(spot_in)], two_send.at[k], two_recv.at[k],
            plane_at + mate(k), core,
        )

    for k in range(1, 4):
        two_copy(k).start()
    state_in[piece_rows(spot_in), :] = before[spot_in]
    send_weights(0, 1, 2)
    send_weights(1)
    forward_weights(0, 0, 2)
    for copy in out_copies:
        copy.wait()

    for k in range(1, 4):
        at = (spot_in + 4 - k) % 4
        spot = state_in.at[piece_rows(at)]
        remote(spot, spot, two_send.at[k], two_recv.at[k], plane_at + at, core).wait_recv()

    def gate_head(retained, gain, gate):
        centred = retained - jnp.mean(retained, axis=-1, keepdims=True)
        variance = jnp.mean(centred * centred, axis=-1, keepdims=True)
        normed = centred * lax.rsqrt(variance + EPS)
        return (normed * gain * silu(gate.astype(jnp.float32))).astype(jnp.bfloat16)

    for h in range(heads):
        lifted = rotated[:, h * KW : (h + 1) * KW]
        crosses = []
        for e in range(VW // LANES):
            at = (h * (VW // LANES) + e) * KW
            crosses.append(dot(lifted, state_in[at : at + KW, :], ((1,), (0,))))
        cut = slice(h * VW, (h + 1) * VW)
        gated[:, cut] = gate_head(
            local[:, cut] + jnp.concatenate(crosses, axis=1), gain_wide[cut].astype(jnp.float32).reshape(1, -1), gate_wide[:, cut]
        )
    for h in range(heads):
        g, e = h // 2, h % 2
        own = first_head if e == 0 else jnp.logical_not(first_head)
        lifted = rotated[:, heads * KW + g * LANES : heads * KW + (g + 1) * LANES]
        lifted = jnp.where(own, lifted.astype(jnp.float32), 0.0).astype(jnp.bfloat16)
        at = base_wide + g * LANES
        cross = dot(lifted, state_in[at : at + LANES, :], ((1,), (0,)))
        cut = slice(h * VN, (h + 1) * VN)
        spot = slice(wide_rows + h * VN, wide_rows + (h + 1) * VN)
        gated[:, spot] = gate_head(local[:, spot] + cross, gain_narrow[cut].astype(jnp.float32).reshape(1, -1), gate_narrow[:, cut])

    mine_f = []
    chunk = dims["chunk"]
    for n in range(width // chunk):
        cut = slice(n * chunk, (n + 1) * chunk)
        product = dot(gated[...], out_w[:, cut], ((1,), (0,))).astype(jnp.bfloat16)
        low, high = product[:half], product[half:]
        first = core == 0
        mix_sent[:, cut] = jnp.where(first, high.astype(jnp.float32), low.astype(jnp.float32)).astype(jnp.bfloat16)
        resid[:, cut] = jnp.where(first, low.astype(jnp.float32), high.astype(jnp.float32))
    mix_copy = remote(mix_sent, mix_got, mix_sem.at[0], mix_sem.at[1], me, other)
    mix_copy.start()
    mix_copy.wait_recv()
    mixed = resid[...] + mix_got[...].astype(jnp.float32)
    stay = (
        stream[...].astype(jnp.float32) + rms(mixed) * gain_mix[...].astype(jnp.float32).reshape(1, -1)
    ).astype(jnp.bfloat16).astype(jnp.float32)
    resid[...] = stay
    normed = rms(stay) * gain_pre[...].astype(jnp.float32).reshape(1, -1)
    tokens[0, pl.ds(pl.multiple_of(pad + z * half, 16), half), :] = normed.astype(jnp.bfloat16)
    span = reach * width // 16
    for r in range(reach):
        for j in range(16 // reach):
            at = r * (16 // reach) + j
            tail_f[at : at + 1, :] = normed[half - reach + r : half - reach + r + 1, j * span : (j + 1) * span]
    tail[...] = tail_f[...].astype(jnp.bfloat16)

    def block(side, at, q):
        return tokens.at[side, pl.ds(pl.multiple_of(pad + at * half + q * step_rows, 16), step_rows)]

    def flow(at, q, sems, to):
        return remote(block(0, at, q), block(0, at, q), sems.at[at, q], z_recv.at[at, q], to, core)

    def over_y(at, q):
        return remote(block(0, at, q), block(1, at, q), y_send.at[at, q], y_recv.at[at, q], y_mate, core)

    def z_wait(at, q):
        remote(block(0, at, q), block(0, at, q), up_send.at[at, q], z_recv.at[at, q], y_mate, core).wait_recv()

    def pass_on(at, q, up, down):
        if up:
            @pl.when(z < nz - 1)
            def _():
                flow(at, q, up_send, me + 4).start()
        if down:
            @pl.when(z > 0)
            def _():
                flow(at, q, dn_send, me - 4).start()
        over_y(at, q).start()

    for q in range(parts):
        pass_on(z, q, True, True)

    next_chip = jnp.where(core == 0, me, (me + 1) % count)

    def halo_copy(k):
        at = (place + k) % places
        return remote(
            tail, halos.at[next_chip // 2], halo_send.at[k], halo_recv.at[next_chip // 2],
            2 * at + next_chip % 2, other,
        )

    def send_halo(k, carry):
        halo_copy(k).start()
        return carry

    lax.fori_loop(0, places, send_halo, 0)
    forward_weights(0, 1, 2)
    pass_weights(0)
    forward_weights(1)

    for h in range(1, nz):
        for q in range(parts):
            @pl.when(z - h >= 0)
            def _():
                z_wait(z - h, q)
                pass_on(z - h, q, True, False)

            @pl.when(z + h < nz)
            def _():
                z_wait(z + h, q)
                pass_on(z + h, q, False, True)

        if h == 1:
            send_weights(2)
            forward_weights(2, 0, 1, 1)
        if h == 2:
            forward_weights(2, 1, 1, places // 2)

    def wait_halo(at, carry):
        remote(halos.at[at], halos.at[at], halo_send.at[at], halo_recv.at[at], me, other).wait_recv()
        return carry

    lax.fori_loop(0, places, wait_halo, 0)
    for side in range(2):
        for at in range(nz):
            p = at * 2 + jnp.where(side == 0, y, 1 - y)
            start = jnp.logical_and(jnp.logical_and(p == 0, x == 0), core == 0)
            block_tail = halos[p].astype(jnp.float32)
            block_tail = jnp.where(start, 0.0, block_tail)
            for r in range(reach):
                for j in range(16 // reach):
                    spot = r * (16 // reach) + j
                    halo_f[side, at * reach + r : at * reach + r + 1, j * span : (j + 1) * span] = (
                        block_tail[spot : spot + 1, :]
                    )
        tokens[side, 0:pad, :] = halo_f[side].astype(jnp.bfloat16)
    pass_weights(1)
    taps_copy.wait()
    forward_weights(2, places // 2)
    across_wait(0)
    across_wait(1)

    def feed(side):
        rows_in = tokens[side]
        ups = []
        for which in range(2):
            ups.append(
                dot(rows_in, weights[which], ((1,), (1,))).astype(jnp.bfloat16).astype(jnp.float32)
            )
        padded[0] = ups[0]
        padded[1] = ups[1]
        taps = taps_own[...] + taps_got[...]
        for at in range(nz):
            for u in range(units // LANES):
                cut = slice(u * LANES, (u + 1) * LANES)
                smooth = []
                for which in range(2):
                    rows_u = padded[which, pad + at * half : pad + (at + 1) * half, cut]
                    place_u = lax.broadcasted_iota(jnp.int32, (half, LANES), 0)
                    total = 0.0
                    for j in range(reach + 1):
                        back = reach - j
                        shifted = rows_u
                        if back:
                            shifted = pltpu.roll(rows_u, back, 0)
                            for r in range(back):
                                spot = at * reach + reach - back + r
                                shifted = jnp.where(
                                    place_u == r, padded[which, spot : spot + 1, cut], shifted
                                )
                        tap = which * (reach + 1) + j
                        total = total + taps[tap : tap + 1, cut] * shifted
                    smooth.append(total)
                hidden[side, at * half : (at + 1) * half, cut] = (silu(smooth[0]) * smooth[1]).astype(jnp.bfloat16)

    def lower_rows(side, at):
        spot = slice(at * half, (at + 1) * half)
        for n in range(width // chunk):
            cut = slice(n * chunk, (n + 1) * chunk)
            terms[side, spot, cut] = dot(
                hidden[side, spot, :], weights[2, :, cut], ((1,), (0,))
            ).astype(jnp.bfloat16)

    def down(side):
        for n in range(width // chunk):
            cut = slice(n * chunk, (n + 1) * chunk)
            terms[side, :, cut] = dot(
                hidden[side], weights[2, :, cut], ((1,), (0,))
            ).astype(jnp.bfloat16)

    feed(0)
    for at in range(nz):
        for q in range(parts):
            remote(block(1, at, q), block(1, at, q), y_send.at[at, q], y_recv.at[at, q], y_mate, core).wait_recv()
    feed(1)
    pass_weights(2)
    across_wait(2)
    down(1)

    def part_of(ref, lead, at, q):
        return ref.at[lead, pl.ds(pl.multiple_of(at * half + q * step_rows, 16), step_rows)]

    def sum_y(at, q):
        return remote(
            part_of(terms, 1, at, q), from_y.at[at, q], ry_send.at[at, q], ry_recv.at[at, q],
            y_mate, core,
        )

    def sum_z(at, q, upward):
        if upward:
            return remote(
                part_of(terms, 0, at, q), from_up.at[at, q], ru_send.at[at, q], ru_recv.at[at, q],
                me + 4, core,
            )
        return remote(
            part_of(terms, 0, at, q), from_down.at[at, q], rd_send.at[at, q], rd_recv.at[at, q],
            me - 4, core,
        )

    for h in list(range(nz - 1, 0, -1)):
        for q in range(parts):
            @pl.when(z + h < nz)
            def _():
                sum_y(z + h, q).start()

            @pl.when(z - h >= 0)
            def _():
                sum_y(z - h, q).start()
    for q in range(parts):
        sum_y(z, q).start()
    down(0)

    def rows_at(at, q):
        return pl.ds(pl.multiple_of(at * half + q * step_rows, 16), step_rows)

    def add_y(at, q):
        sum_y(at, q).wait_recv()
        terms[0, rows_at(at, q), :] = (
            terms[0, rows_at(at, q), :].astype(jnp.float32) + from_y[at, q].astype(jnp.float32)
        ).astype(jnp.bfloat16)

    def add_from(at, q, ref, sem):
        remote(ref.at[at, q], ref.at[at, q], ru_send.at[at, q], sem.at[at, q], y_mate, core).wait_recv()
        terms[0, rows_at(at, q), :] = (
            terms[0, rows_at(at, q), :].astype(jnp.float32) + ref[at, q].astype(jnp.float32)
        ).astype(jnp.bfloat16)

    for h in list(range(nz - 1, 0, -1)):
        for q in range(parts):
            @pl.when(z + h < nz)
            def _():
                add_y(z + h, q)

                @pl.when(z > 0)
                def _():
                    add_from(z + h, q, from_up, ru_recv)
                sum_z(z + h, q, True).start()

            @pl.when(z - h >= 0)
            def _():
                add_y(z - h, q)

                @pl.when(z < nz - 1)
                def _():
                    add_from(z - h, q, from_down, rd_recv)
                sum_z(z - h, q, False).start()
    for q in range(parts):
        add_y(z, q)

        @pl.when(z > 0)
        def _():
            add_from(z, q, from_up, ru_recv)

        @pl.when(z < nz - 1)
        def _():
            add_from(z, q, from_down, rd_recv)
    fed = terms[0, pl.ds(pl.multiple_of(z * half, 16), half), :].astype(jnp.float32)
    result[...] = (resid[...] + rms(fed) * gain_post[...].astype(jnp.float32).reshape(1, -1)).astype(jnp.bfloat16)

    def drain(k, carry):
        log_copy(k).wait_send()
        return carry

    lax.fori_loop(1, count, drain, 0)

    def drain_weights(k, carry):
        for which in range(3):
            weight_copy(which, k).wait_send()
        return carry

    lax.fori_loop(1, places, drain_weights, 0)

    def drain_over(k, carry):
        for which in range(3):
            over_x(which, k).wait_send()
            for side in range(2):
                across(which, side, k).wait_send()
        halo_copy(k).wait_send()
        return carry

    lax.fori_loop(0, places, drain_over, 0)
    for k in range(1, 4):
        one_copy(k).wait_send()
        two_copy(k).wait_send()
    for k in range(1, nz):
        @pl.when(z + k < nz)
        def _():
            plane_copy(k).wait_send()
    mix_copy.wait_send()

    def drain_blocks(at, carry):
        for q in range(parts):
            over_y(at, q).wait_send()
            sum_y(at, q).wait_send()

            @pl.when(jnp.logical_and(z < nz - 1, at <= z))
            def _():
                flow(at, q, up_send, me + 4).wait_send()

            @pl.when(jnp.logical_and(z > 0, at >= z))
            def _():
                flow(at, q, dn_send, me - 4).wait_send()

            @pl.when(at > z)
            def _():
                sum_z(at, q, True).wait_send()

            @pl.when(at < z)
            def _():
                sum_z(at, q, False).wait_send()
        return carry

    lax.fori_loop(0, nz, drain_blocks, 0)


def fused_layer(
    stream, q_wide, k_wide, v_wide, q_narrow, k_narrow, v_narrow, gate_wide, gate_narrow, log_decay,
    gain_wide, gain_narrow, out_wide, out_narrow, gain_mix, gain_pre, gain_post,
    weight_gate, weight_lin, weight_down, taps_gate, taps_lin,
):
    count, n_tp = lax.axis_size("sp"), lax.axis_size("tp")
    rows, width = q_wide.shape[0], stream.shape[1]
    places, nz = count // 2, count // 4
    heads = q_wide.shape[1] // KW
    columns = weight_gate.shape[1]
    share = columns // places
    units = share * n_tp
    reach = taps_gate.shape[0] - 1
    state_rows = heads * (KW * VW + KN * VN) // LANES
    piece = state_rows // 4
    tap_rows = 2 * (reach + 1)
    tap_rows += -tap_rows % 8
    half = rows // n_tp
    parts = 2
    values = out_wide.shape[0] + out_narrow.shape[0]
    dims = dict(
        count=count, n_tp=n_tp, rows=rows, width=width, share=share, piece=piece, reach=reach,
        chunk=512,
    )
    vmem = pl.BlockSpec(memory_space=pltpu.VMEM)
    anywhere = pl.BlockSpec(memory_space=pl.ANY)
    bf, f32 = jnp.bfloat16, jnp.float32
    dma = pltpu.SemaphoreType.DMA
    scratch = [
        pltpu.VMEM((3, weight_gate.shape[0], columns), bf),
        pltpu.VMEM((3, columns, weight_gate.shape[0]), bf),
        pltpu.VMEM((values, width), bf),
        pltpu.VMEM((3, units, width), bf),
        pltpu.VMEM((2, PAD + nz * half, width), bf),
        pltpu.VMEM((2, nz * half, width), bf),
        pltpu.VMEM((nz, parts, half // parts, width), bf),
        pltpu.VMEM((nz, parts, half // parts, width), bf),
        pltpu.VMEM((nz, parts, half // parts, width), bf),
        pltpu.VMEM((rows, heads * (KW + KN)), bf),
        pltpu.VMEM((rows, values), f32),
        pltpu.VMEM((state_rows, LANES), bf),
        pltpu.VMEM((4, piece, LANES), bf),
        pltpu.VMEM((piece, LANES), bf),
        pltpu.VMEM((nz, piece, LANES), bf),
        pltpu.VMEM((piece, LANES), f32),
        pltpu.VMEM((4, piece, LANES), bf),
        pltpu.VMEM((state_rows, LANES), bf),
        pltpu.VMEM((rows, values), bf),
        pltpu.VMEM((count, 2 * heads, LANES), f32),
        pltpu.VMEM((tap_rows, columns), f32),
        pltpu.VMEM((2 * heads, LANES), f32),
        pltpu.VMEM((count, 2 * heads, LANES), f32),
        pltpu.VMEM((tap_rows, units), f32),
        pltpu.VMEM((tap_rows, units), f32),
        pltpu.VMEM((half, width), bf),
        pltpu.VMEM((half, width), bf),
        pltpu.VMEM((half, width), f32),
        pltpu.VMEM((16, reach * width // 16), f32),
        pltpu.VMEM((16, reach * width // 16), bf),
        pltpu.VMEM((places, 16, reach * width // 16), bf),
        pltpu.VMEM((2, PAD, width), f32),
        pltpu.VMEM((2, PAD + nz * half, units), f32),
        pltpu.VMEM((2, nz * half, units), bf),
        dma((3,)), dma((2,)), dma((3,)), dma((3, places)), dma((3, places)), dma((3, places)),
        dma((3, places)), dma((3, 2, places)), dma((3, 2, places)),
        dma((count,)), dma((count,)), dma((4,)), dma((4,)), dma((nz,)), dma((nz,)), dma((4,)), dma((4,)),
        dma((2,)), dma((2,)), dma((places,)), dma((places,)),
    ] + [dma((nz, parts)) for _ in range(11)]
    kernel = pl.pallas_call(
        functools.partial(layer_kernel, dims),
        out_shape=jax.ShapeDtypeStruct(stream.shape, bf),
        in_specs=[vmem] * 18 + [anywhere] * 5,
        out_specs=vmem,
        scratch_shapes=scratch,
        compiler_params=pltpu.CompilerParams(
            collective_id=0, has_side_effects=True, vmem_limit_bytes=VMEM_BYTES
        ),
    )
    return kernel(
        stream, q_wide, k_wide, v_wide, q_narrow, k_narrow, v_narrow, gate_wide, gate_narrow,
        log_decay, gain_wide, gain_narrow, gain_mix, gain_pre, gain_post,
        jnp.asarray(tables_of(count, rows)), taps_gate, taps_lin, out_wide, out_narrow,
        weight_gate, weight_lin, weight_down,
    )


def fits(stream, q_wide, log_decay, weight_gate, taps_gate):
    count, n_tp = lax.axis_size("sp"), lax.axis_size("tp")
    rows, width = q_wide.shape[0], stream.shape[1]
    if n_tp != 2 or count % 4 or count < 8 or rows != BLOCK or q_wide.shape[1] % (2 * KW):
        return False
    heads = q_wide.shape[1] // KW
    units = weight_gate.shape[1]
    state_rows = heads * (KW * VW + KN * VN) // LANES
    reach = taps_gate.shape[0] - 1
    held = units // (count // 2)
    return (
        2 * heads == 8
        and weight_gate.shape[0] == LANES
        and units % (count // 2 * 16) == 0
        and (n_tp * held) % LANES == 0
        and state_rows % (4 * 16) == 0
        and reach == 2
        and (count // 4) * reach <= PAD
        and width % 512 == 0
        and 3 * n_tp * held * width <= 5 * 2 ** 20
    )


def body(
    stream,
    wide_head_query,
    broad_attention_lookup_vectors,
    values_wide,
    query_narrow,
    keys_narrow,
    values_narrow,
    gate_wide,
    gate_narrow,
    log_decay,
    gain_wide,
    gain_narrow,
    out_wide,
    out_narrow,
    gain_mix,
    gain_pre,
    gain_post,
    weight_gate,
    weight_lin,
    weight_down,
    taps_gate,
    taps_lin,
):
    if fits(stream, wide_head_query, log_decay, weight_gate, taps_gate):
        return fused_layer(
            stream, wide_head_query, broad_attention_lookup_vectors, values_wide, query_narrow,
            keys_narrow, values_narrow, gate_wide, gate_narrow, log_decay, gain_wide, gain_narrow,
            out_wide, out_narrow, gain_mix, gain_pre, gain_post, weight_gate, weight_lin,
            weight_down, taps_gate, taps_lin,
        )
    rows = wide_head_query.shape[0]
    count = lax.axis_size("sp")
    n_tp = lax.axis_size("tp")
    width = stream.shape[1]
    units = weight_gate.shape[1]
    by_tokens = 2 * count * rows < 3 * units and units % (count * 16) == 0
    by_tokens = by_tokens and count & (count - 1) == 0
    if by_tokens:
        weights, taps = unit_slices(weight_gate, weight_lin, weight_down, taps_gate, taps_lin)
    offset = lax.axis_index("sp") * rows
    rates_wide = log_decay[0]
    rates_narrow = log_decay[1]
    rot_wide, local_wide, state_wide = kept_nearby_memory(
        wide_head_query, broad_attention_lookup_vectors, values_wide, rates_wide, KW, VW, offset
    )
    rot_narrow, local_narrow, state_narrow = kept_nearby_memory(
        query_narrow, keys_narrow, values_narrow, rates_narrow, KN, VN, offset
    )
    incoming = carried_in(
        (state_wide, state_narrow),
        (jnp.sum(rates_wide, axis=1), jnp.sum(rates_narrow, axis=1)),
        "sp",
    )
    gated_wide = gate_heads(
        local_wide + carried(rot_wide, rates_wide, incoming[0]), gain_wide, gate_wide
    )
    gated_narrow = gate_heads(
        local_narrow + carried(rot_narrow, rates_narrow, incoming[1]), gain_narrow, gate_narrow
    )
    part_wide = jnp.dot(gated_wide, out_wide, preferred_element_type=jnp.float32)
    part_narrow = jnp.dot(gated_narrow, out_narrow, preferred_element_type=jnp.float32)
    mixed = share_rows(
        (part_wide + part_narrow).astype(jnp.bfloat16).reshape(n_tp, rows // n_tp, width), "tp"
    )
    resid = (stream.astype(jnp.float32) + scale_rows(mixed, gain_mix)).astype(jnp.bfloat16)
    normed_in = scale_rows(resid.astype(jnp.float32), gain_pre).astype(jnp.bfloat16)
    if by_tokens:
        fed = feed_by_tokens(normed_in, weights, taps)
    else:
        fed = feed_by_weights(normed_in, weight_gate, weight_lin, weight_down, taps_gate, taps_lin)
    return (resid.astype(jnp.float32) + scale_rows(fed, gain_post)).astype(jnp.bfloat16)


def solution(mesh):
    in_specs = (
        P(("sp", "tp"), None),
        P("sp", "tp"),
        P("sp", "tp"),
        P("sp", "tp"),
        P("sp", "tp"),
        P("sp", "tp"),
        P("sp", "tp"),
        P("sp", "tp"),
        P("sp", "tp"),
        P(None, "tp", "sp"),
        P("tp"),
        P("tp"),
        P("tp", None),
        P("tp", None),
        P(),
        P(),
        P(),
        P("sp", "tp"),
        P("sp", "tp"),
        P("sp", "tp"),
        P(None, "tp"),
        P(None, "tp"),
    )
    out_specs = P(("sp", "tp"), None)
    return jax.shard_map(body, mesh=mesh, in_specs=in_specs, out_specs=out_specs, check_vma=False)
```

```python
import functools

import jax
import jax.numpy as jnp
import numpy as np
from jax import lax
from jax.experimental import pallas as pl
from jax.experimental.pallas import tpu as pltpu
from jax.sharding import PartitionSpec as P

KW = 128
VW = 256
KN = 64
VN = 128
BLOCK = 128


EPS = 1e-06
THETA = 10000.0
LANES = 128
PAD = 16
VMEM_BYTES = 60 * 2**20


def passed_along(value, axis, steps):
    count = lax.axis_size(axis)
    first, last = (max(0, -steps), min(count, count - steps))
    return lax.ppermute(value, axis, [(source, source + steps) for source in range(first, last)])


def rotate(block, positions):
    width = block.shape[-1]
    half = width // 2
    frequency = THETA ** (-(jnp.arange(half, dtype=jnp.float32) * 2.0 / width))
    angles = positions.astype(jnp.float32)[:, None] * frequency[None, :]
    cosine = jnp.cos(angles)[:, None, :]
    sine = jnp.sin(angles)[:, None, :]
    values = block.astype(jnp.float32)
    first = values[..., :half]
    second = values[..., half:]
    return jnp.concatenate(
        [first * cosine - second * sine, second * cosine + first * sine], axis=-1
    )


def block_step(state, inputs):
    query, keys, values, log_rate = inputs
    running = jnp.cumsum(log_rate, axis=1)
    length = running.shape[1]
    index = jnp.arange(length)
    lower = (index[:, None] >= index[None, :])[None]
    spread = jnp.where(
        lower, jnp.exp(jnp.where(lower, running[:, :, None] - running[:, None, :], 0.0)), 0.0
    )
    scores = (
        jnp.einsum("ihd,jhd->hij", query, keys, preferred_element_type=jnp.float32) * spread
    ).astype(jnp.bfloat16)
    inner = jnp.einsum("hij,jhe->ihe", scores, values, preferred_element_type=jnp.float32)
    lifted = query.astype(jnp.float32) * jnp.exp(running).T[:, :, None]
    cross = jnp.einsum("ihd,hde->ihe", lifted, state, precision=lax.Precision.HIGHEST)
    tail = running[:, -1:]
    scaled = (keys.astype(jnp.float32) * jnp.exp(tail - running).T[:, :, None]).astype(jnp.bfloat16)
    update = jnp.einsum("jhd,jhe->hde", scaled, values, preferred_element_type=jnp.float32)
    state = state * jnp.exp(tail)[:, :, None] + update
    return (state, inner + cross)


def kept_nearby_memory(query, keys, values, log_rate, head_dim, value_dim, offset):
    rows = query.shape[0]
    heads = query.shape[1] // head_dim
    positions = offset + jnp.arange(rows, dtype=jnp.int32)
    rotated_query = rotate(query.reshape(rows, heads, head_dim), positions).astype(jnp.bfloat16)
    rotated_keys = (
        rotate(keys.reshape(rows, heads, head_dim), positions) * head_dim ** (-0.5)
    ).astype(jnp.bfloat16)
    layer_groups_list = rows // BLOCK

    def split(array):
        return array.reshape(layer_groups_list, BLOCK, heads, array.shape[-1])

    rates = jnp.transpose(log_rate.reshape(heads, layer_groups_list, BLOCK), (1, 0, 2))
    start = jnp.zeros((heads, head_dim, value_dim), jnp.float32)
    inputs = (
        split(rotated_query),
        split(rotated_keys),
        split(values.reshape(rows, heads, value_dim)),
        rates,
    )
    state, outs = lax.scan(block_step, start, inputs)
    return (rotated_query, outs.reshape(rows, heads, value_dim), state)


def carried(rotated_query, log_rate, state_in):
    lifted = rotated_query.astype(jnp.float32) * jnp.exp(jnp.cumsum(log_rate, axis=1)).T[:, :, None]
    return jnp.einsum("ihd,hde->ihe", lifted, state_in, precision=lax.Precision.HIGHEST)


def gate_heads(retained, gain, gate):
    mean = jnp.mean(retained, axis=-1, keepdims=True)
    centred = retained - mean
    variance = jnp.mean(centred * centred, axis=-1, keepdims=True)
    normed = (centred * lax.rsqrt(variance + EPS)).reshape(retained.shape[0], -1)
    return (normed * gain.astype(jnp.float32) * jax.nn.silu(gate.astype(jnp.float32))).astype(
        jnp.bfloat16
    )


def scale_rows(rows, gain):
    return (
        rows
        * lax.rsqrt(jnp.mean(rows * rows, axis=-1, keepdims=True) + EPS)
        * gain.astype(jnp.float32)
    )


def causal_taps(upward, before, taps):
    width = taps.shape[0]
    total = upward.shape[0]
    padded_rows = jnp.concatenate([before, upward], axis=0).astype(jnp.float32)
    smooth = jnp.zeros((total, upward.shape[1]), jnp.float32)
    for tap_index in range(width):
        smooth = (
            smooth
            + taps[tap_index].astype(jnp.float32)[None, :]
            * padded_rows[tap_index : tap_index + total]
        )
    return smooth


def swap_blocks(blocks, axis):
    return lax.all_to_all(blocks, axis, 0, 0, tiled=False)


def share_rows(parts, axis):
    count = lax.axis_size(axis)
    place = lax.axis_index(axis)
    total = lax.dynamic_index_in_dim(parts, place, 0, False).astype(jnp.float32)
    for step in range(1, count):
        piece = lax.dynamic_index_in_dim(parts, (place + step) % count, 0, False)
        moved = lax.ppermute(piece, axis, [(i, (i + step) % count) for i in range(count)])
        total = total + moved.astype(jnp.float32)
    return total


def carried_in(states, totals, axis):
    count = lax.axis_size(axis)
    lanes = states[-1].shape[-1]
    flat = jnp.concatenate([s.reshape(-1, lanes) for s in states]).astype(jnp.bfloat16)
    rates = jnp.concatenate(
        [jnp.repeat(d, s.size // s.shape[0] // lanes) for s, d in zip(states, totals)]
    )
    share = flat.shape[0] // count
    rates = rates.reshape(count, share)
    rates = jnp.pad(rates, ((0, 0), (0, -share % lanes)))
    parts, left = [], rates
    for _ in range(3):
        parts.append(left.astype(jnp.bfloat16))
        left = left - parts[-1].astype(jnp.float32)
    parts = [part.reshape(count, -1, lanes) for part in parts]
    sent = jnp.concatenate([flat.reshape(count, share, lanes)] + parts, axis=1)
    got = swap_blocks(sent, axis).astype(jnp.float32)
    parts = jnp.split(got[:, share:], 3, axis=1)
    logs = (parts[0] + parts[1] + parts[2]).reshape(count, -1)[:, :share]
    own = got[:, :share]
    steps = jnp.arange(count)
    between = (steps[None, None] > steps[None, :, None]) & (
        steps[None, None] < steps[:, None, None]
    )
    span = jnp.sum(jnp.where(between[..., None], logs[None, None], 0.0), axis=2)
    factor = jnp.where((steps[None] < steps[:, None])[..., None], jnp.exp(span), 0.0)
    before = sum(factor[:, step, :, None] * own[step][None] for step in range(count))
    back = swap_blocks(before.astype(jnp.bfloat16), axis).reshape(-1, lanes).astype(jnp.float32)
    outs, at = [], 0
    for s in states:
        rows = s.size // lanes
        outs.append(back[at : at + rows].reshape(s.shape))
        at += rows
    return outs


def feed_by_weights(normed_in, weight_gate, weight_lin, weight_down, taps_gate, taps_lin):
    normed_all = lax.all_gather(normed_in, "tp", axis=0, tiled=True)
    rows = normed_all.shape[0]
    whole_gate, whole_lin = (
        lax.all_gather(weight_gate, "sp", axis=0, tiled=True),
        lax.all_gather(weight_lin, "sp", axis=0, tiled=True),
    )
    up_gate = jnp.dot(normed_all, whole_gate, preferred_element_type=jnp.float32).astype(
        jnp.bfloat16
    )
    up_lin = jnp.dot(normed_all, whole_lin, preferred_element_type=jnp.float32).astype(jnp.bfloat16)
    reach = taps_gate.shape[0] - 1
    before_gate, before_lin = passed_along(
        (up_gate[rows - reach :], up_lin[rows - reach :]), "sp", 1
    )
    smooth_gate = causal_taps(up_gate, before_gate, taps_gate)
    smooth_lin = causal_taps(up_lin, before_lin, taps_lin)
    hidden = (jax.nn.silu(smooth_gate) * smooth_lin).astype(jnp.bfloat16)
    terms = lax.dot_general(
        hidden,
        lax.all_gather(weight_down, "sp", axis=0, tiled=True),
        (((1,), (1,)), ((), ())),
        preferred_element_type=jnp.float32,
    )
    return lax.psum_scatter(
        terms.astype(jnp.bfloat16), "tp", scatter_dimension=0, tiled=True
    ).astype(jnp.float32)


def from_all(value, axis, dim):
    count = lax.axis_size(axis)
    found = [value]
    for step in range(1, count):
        found.append(lax.ppermute(value, axis, [(i, (i + step) % count) for i in range(count)]))
    return jnp.concatenate(found, axis=dim)


def unit_slices(weight_gate, weight_lin, weight_down, taps_gate, taps_lin):
    count = lax.axis_size("sp")
    place = lax.axis_index("sp")
    deep, units = weight_gate.shape
    share = units // count
    turned = jnp.stack([weight_gate.T, weight_lin.T, weight_down.T])
    blocks = turned.reshape(3, count, share, deep).transpose(1, 0, 2, 3)
    got = swap_blocks(blocks, "sp")
    mine = got.transpose(1, 2, 0, 3).reshape(3, share, count * deep)
    taps = jnp.stack([taps_gate, taps_lin])
    taps = lax.dynamic_slice_in_dim(taps, place * share, share, 2)
    return from_all(mine, "tp", 1), from_all(taps, "tp", 2)


def flip(value, axis, bit):
    return lax.ppermute(
        value, axis, [(i, i ^ (1 << bit)) for i in range(lax.axis_size(axis))]
    )


def bits_of(count, swapped):
    bits = list(range(count.bit_length() - 1))
    if swapped:
        bits[:2] = bits[:2][::-1]
    return bits


def gather_around(value, axis, swapped):
    bits = bits_of(lax.axis_size(axis), swapped)
    for bit in bits[::-1]:
        value = jnp.stack([value, flip(value, axis, bit)])
    order = [bits.index(bit) for bit in sorted(bits, reverse=True)]
    value = value.transpose(*order, *range(len(bits), value.ndim))
    return value.reshape(-1, *value.shape[len(bits) :])


def add_around(value, axis, swapped):
    bits = bits_of(lax.axis_size(axis), swapped)
    value = value.reshape(*[2] * len(bits), *value.shape[1:])
    dims = sorted(bits, reverse=True)
    for bit in bits:
        at = dims.index(bit)
        dims.remove(bit)
        kept = lax.index_in_dim(value, 0, at, False).astype(jnp.float32)
        sent = lax.index_in_dim(value, 1, at, False).astype(jnp.bfloat16)
        value = kept + flip(sent, axis, bit).astype(jnp.float32)
        if dims:
            value = value.astype(jnp.bfloat16)
    return value


def feed_by_tokens(normed_in, weights, taps):
    count = lax.axis_size("sp")
    n_tp = lax.axis_size("tp")
    rows, width = normed_in.shape
    place = lax.axis_index("sp")
    half = width // 2
    flat = weights[:2].reshape(-1, width)
    units = flat.shape[0] // 2
    ups = 0.0
    for part in range(2):
        cut = slice(part * half, (part + 1) * half)
        tokens = gather_around(normed_in[:, cut], "sp", part == 1)
        ups = ups + lax.dot_general(
            tokens.reshape(count * rows, half),
            flat[:, cut],
            (((1,), (1,)), ((), ())),
            preferred_element_type=jnp.float32,
        )
    ups = ups.astype(jnp.bfloat16).reshape(count, rows, 2 * units)
    reach = taps.shape[1] - 1
    tails = ups[:, rows - reach :]
    prior = lax.ppermute(tails, "tp", [(i, (i + 1) % n_tp) for i in range(n_tp)])
    prior = jnp.roll(prior.reshape(count, reach, 2, n_tp, -1), 1, axis=3).reshape(prior.shape)
    blocks = place ^ jnp.arange(count)
    follows = (blocks[:, None] == blocks[None, :] + 1).astype(jnp.bfloat16)
    shifted = jnp.dot(
        follows, prior.reshape(count, -1), preferred_element_type=jnp.float32
    ).astype(jnp.bfloat16).reshape(prior.shape)
    prior = jnp.where(lax.axis_index("tp") == 0, shifted, prior)
    padded = jnp.concatenate([prior, ups], axis=1).astype(jnp.float32)
    taps = jnp.concatenate([taps[0], taps[1]], axis=1).astype(jnp.float32)
    smooth = sum(taps[j] * padded[:, j : j + rows] for j in range(reach + 1))
    hidden = (jax.nn.silu(smooth[..., :units]) * smooth[..., units:]).astype(jnp.bfloat16)
    hidden = hidden.reshape(count * rows, units)
    sums = []
    for part in range(2):
        cut = slice(part * half, (part + 1) * half)
        terms = jnp.dot(hidden, weights[2][:, cut], preferred_element_type=jnp.float32)
        terms = terms.astype(jnp.bfloat16).reshape(count, rows, half)
        sums.append(add_around(terms, "sp", part == 1))
    return jnp.concatenate(sums, axis=1)


def tables_of(count, rows):
    def angles(positions, width):
        half = width // 2
        frequency = THETA ** (-(np.arange(half, dtype=np.float64) * 2.0 / width))
        return np.tile(positions[:, None] * frequency[None, :], (1, LANES // half))

    positions = np.concatenate([np.arange(rows), np.arange(count) * rows]).astype(np.float64)
    found = []
    for width in (KW, KN):
        turned = angles(positions, width)
        found += [np.cos(turned), np.sin(turned)]
    return np.stack(found).astype(np.float32)


def remote(source, target, sent, got, sp, tp):
    return pltpu.make_async_remote_copy(
        src_ref=source, dst_ref=target, send_sem=sent, recv_sem=got,
        device_id=(sp, tp), device_id_type=pl.DeviceIdType.MESH,
    )


def silu(value):
    return value / (1.0 + jnp.exp(-value))


def rms(value):
    return value * lax.rsqrt(jnp.mean(value * value, axis=-1, keepdims=True) + EPS)


def layer_kernel(
    dims,
    stream_hbm, q_wide, k_wide, v_wide, q_narrow, k_narrow, v_narrow, gate_wide_hbm, gate_narrow_hbm,
    decay, gain_wide, gain_narrow, gain_mix, gain_pre, gain_post, tables, taps_gate, taps_lin,
    out_wide_hbm, out_narrow_hbm, weight_gate, weight_lin, weight_down,
    result,
    stream, gate_wide, gate_narrow, raw, turned, out_w, weights, tokens, terms, from_y, from_up, from_down, rotated, local, states,
    got, plane_sum, planes, carry, before, state_in, gated, fades, taps_all, logs_own, logs, taps_own, taps_got, mix_sent, mix_got, resid, tail_f, tail, halos, halo_f,
    padded, hidden,
    late_sem, raw_sem, out_sem, own_sem, w_send, w_recv, xw_send, xw_recv, dw_send, dw_recv,
    log_send, log_recv, one_send, one_recv, z_sum_send, z_sum_recv, two_send, two_recv, tap_sem, mix_sem,
    halo_send, halo_recv, up_send, dn_send, y_send, z_recv, y_recv,
    ry_send, ry_recv, ru_send, ru_recv, rd_send, rd_recv,
):
    count, n_tp = dims["count"], dims["n_tp"]
    rows, width = dims["rows"], dims["width"]
    half = rows // n_tp
    places = count // 2
    nz = count // 4
    share = dims["share"]
    n_tiles = share * places // LANES
    units = n_tp * share
    piece = dims["piece"]
    reach = dims["reach"]
    parts = 4
    step_rows = half // parts
    pad = PAD
    me = lax.axis_index("sp")
    core = lax.axis_index("tp")
    other = 1 - core
    x = me % 2
    y = (me // 2) % 2
    z = me // 4
    place = me // 2
    x_mate = me + 1 - 2 * x
    y_mate = me + 2 - 4 * y
    mine = pl.multiple_of(me * LANES, LANES)

    def in_plane(k):
        at = (place + k) % places
        return at, 2 * at + x

    barrier = pltpu.get_barrier_semaphore()

    def greet(k, carry):
        to = (me * n_tp + core + k) % (count * n_tp)
        pl.semaphore_signal(
            barrier, inc=1, device_id=(to // n_tp, to % n_tp),
            device_id_type=pl.DeviceIdType.MESH,
        )
        return carry

    lax.fori_loop(1, count * n_tp, greet, 0)

    wide_rows = out_wide_hbm.shape[0]
    narrow_rows = out_narrow_hbm.shape[0]
    out_copies = [
        pltpu.make_async_copy(out_wide_hbm, out_w.at[pl.ds(0, wide_rows)], out_sem.at[0]),
        pltpu.make_async_copy(out_narrow_hbm, out_w.at[pl.ds(wide_rows, narrow_rows)], out_sem.at[1]),
    ]
    raw_copies = [
        pltpu.make_async_copy(source, raw.at[which], raw_sem.at[which])
        for which, source in enumerate((weight_gate, weight_lin, weight_down))
    ]
    late_copies = [
        pltpu.make_async_copy(gate_wide_hbm, gate_wide, late_sem.at[0]),
        pltpu.make_async_copy(gate_narrow_hbm, gate_narrow, late_sem.at[1]),
        pltpu.make_async_copy(stream_hbm, stream, late_sem.at[2]),
    ]
    for copy in raw_copies + late_copies + out_copies:
        copy.start()

    def own_rows(at):
        return pl.ds(pl.multiple_of(at * share, 16), share)

    core_rows = pl.ds(pl.multiple_of(core * share, 16), share)

    def weight_copy(which, k):
        at, to = in_plane(k)
        return remote(
            turned.at[which, own_rows(at)], weights.at[which, core_rows, pl.ds(mine, LANES)],
            w_send.at[which, k], w_recv.at[which, k], to, core,
        )

    def weight_wait(which, k):
        from_at = (place + places - k) % places
        columns = pl.ds(pl.multiple_of((2 * from_at + x) * LANES, LANES), LANES)
        spot = weights.at[which, core_rows, columns]
        remote(spot, spot, w_send.at[which, k], w_recv.at[which, k], x_mate, core).wait_recv()

    def over_x(which, k):
        from_at = (place + places - k) % places
        columns = pl.ds(pl.multiple_of((2 * from_at + x) * LANES, LANES), LANES)
        spot = weights.at[which, core_rows, columns]
        return remote(spot, spot, xw_send.at[which, k], xw_recv.at[which, k], x_mate, core)

    def over_x_wait(which, k):
        from_at = (place + places - k) % places
        columns = pl.ds(pl.multiple_of((2 * from_at + 1 - x) * LANES, LANES), LANES)
        spot = weights.at[which, core_rows, columns]
        remote(spot, spot, xw_send.at[which, k], xw_recv.at[which, k], x_mate, core).wait_recv()

    def columns_of(side, k):
        from_at = (place + places - k) % places
        column = 2 * from_at + (x if side == 0 else 1 - x)
        return pl.ds(pl.multiple_of(column * LANES, LANES), LANES)

    def across(which, side, k):
        spot = weights.at[which, core_rows, columns_of(side, k)]
        return remote(spot, spot, dw_send.at[which, side, k], dw_recv.at[which, side, k], me, other)

    def across_wait(which):
        other_rows = pl.ds(pl.multiple_of(other * share, 16), share)
        for side in range(2):
            def go(k, carried_):
                spot = weights.at[which, other_rows, columns_of(side, k)]
                remote(
                    spot, spot, dw_send.at[which, side, k], dw_recv.at[which, side, k], me, other
                ).wait_recv()
                return carried_
            lax.fori_loop(0, places, go, 0)

    def own_copy(which):
        return pltpu.make_async_copy(
            turned.at[which, own_rows(place)], weights.at[which, core_rows, pl.ds(mine, LANES)],
            own_sem.at[which],
        )

    def send_weights(which, first=1, step=1):
        def go(i, carried_):
            weight_copy(which, first + step * i).start()
            return carried_
        lax.fori_loop(0, (places - 1 - first) // step + 1, go, 0)

    def forward_weights(which, first=0, step=1, last=places):
        if first == 0:
            own_copy(which).wait()
            over_x(which, 0).start()
            across(which, 0, 0).start()
            first = step

        def go(i, carried_):
            k = first + step * i
            weight_wait(which, k)
            over_x(which, k).start()
            across(which, 0, k).start()
            return carried_
        lax.fori_loop(0, (last - 1 - first) // step + 1, go, 0)

    def pass_weights(which):
        def go(k, carried_):
            over_x_wait(which, k)
            across(which, 1, k).start()
            return carried_
        lax.fori_loop(0, places, go, 0)

    def turn(which):
        raw_copies[which].wait()
        for at in range(n_tiles):
            cut = slice(at * LANES, (at + 1) * LANES)
            turned[which, cut, :] = raw[which, :, cut].T
        own_copy(which).start()

    i_at = lax.broadcasted_iota(jnp.int32, (rows, rows), 0)
    j_at = lax.broadcasted_iota(jnp.int32, (rows, rows), 1)
    lower = i_at >= j_at
    lower_f = lower.astype(jnp.float32)
    upper_f = (i_at <= j_at).astype(jnp.float32)
    rates = decay[...].reshape(-1, rows)
    run_rows = lax.dot_general(
        rates, upper_f, (((1,), (0,)), ((), ())), precision=lax.Precision.HIGHEST,
        preferred_element_type=jnp.float32,
    )
    run_cols = lax.dot_general(
        lower_f, rates, (((1,), (1,)), ((), ())), precision=lax.Precision.HIGHEST,
        preferred_element_type=jnp.float32,
    )
    totals = run_rows[:, rows - 1 : rows]
    logs_own[...] = jnp.broadcast_to(totals, logs_own.shape)
    logs[me] = jnp.broadcast_to(totals, logs_own.shape)

    def peer(k):
        return (me + k) % count

    def log_copy(k):
        return remote(logs_own, logs.at[me], log_send.at[k], log_recv.at[k], peer(k), core)

    def send_logs(k, carry):
        log_copy(k).start()
        return carry

    heads = wide_rows // VW
    lane = lax.broadcasted_iota(jnp.int32, (rows, LANES), 1)

    def angle_table(first, half_width):
        cos_i, sin_i = tables[first, 0:rows, :], tables[first + 1, 0:rows, :]
        cos_o = tables[first, pl.ds(rows + me, 1), :]
        sin_o = tables[first + 1, pl.ds(rows + me, 1), :]
        cosine = cos_o * cos_i - sin_o * sin_i
        sine = sin_o * cos_i + cos_o * sin_i
        early = lane % (2 * half_width) < half_width
        return cosine, jnp.where(early, -sine, sine), early

    cos_w, sin_w, _ = angle_table(0, KW // 2)

    def dot(a, b, dims_):
        return lax.dot_general(a, b, (dims_, ((), ())), preferred_element_type=jnp.float32)

    def spread_of(column, row):
        return jnp.where(lower, jnp.exp(jnp.where(lower, column - row, 0.0)), 0.0)

    for h in range(heads):
        cut = slice(h * KW, (h + 1) * KW)
        query = q_wide[:, cut].astype(jnp.float32)
        query = (query * cos_w + pltpu.roll(query, KW // 2, 1) * sin_w).astype(jnp.bfloat16)
        keys = k_wide[:, cut].astype(jnp.float32)
        keys = ((keys * cos_w + pltpu.roll(keys, KW // 2, 1) * sin_w) * KW ** (-0.5)).astype(jnp.bfloat16)
        column, row = run_cols[:, h : h + 1], run_rows[h : h + 1, :]
        scores = (dot(query, keys, ((1,), (1,))) * spread_of(column, row)).astype(jnp.bfloat16)
        values = v_wide[:, h * VW : (h + 1) * VW]
        local[:, h * VW : (h + 1) * VW] = dot(scores, values, ((1,), (0,)))
        last = totals[h : h + 1, :]
        scaled = (keys.astype(jnp.float32) * jnp.exp(last - column)).astype(jnp.bfloat16)
        state = dot(scaled, values, ((0,), (0,))).astype(jnp.bfloat16)
        for e in range(VW // LANES):
            at = (h * (VW // LANES) + e) * KW
            states[at : at + KW, :] = state[:, e * LANES : (e + 1) * LANES]
        rotated[:, cut] = (query.astype(jnp.float32) * jnp.exp(column)).astype(jnp.bfloat16)

    cos_n, sin_n, early_n = angle_table(2, KN // 2)

    def swap_narrow(value):
        return jnp.where(
            early_n, pltpu.roll(value, LANES - KN // 2, 1), pltpu.roll(value, KN // 2, 1)
        )

    base_wide = wide_rows // LANES * KW
    first_head = lane < KN
    for g in range(heads // 2):
        cut = slice(g * LANES, (g + 1) * LANES)
        query = q_narrow[:, cut].astype(jnp.float32)
        query = (query * cos_n + swap_narrow(query) * sin_n).astype(jnp.bfloat16)
        keys = k_narrow[:, cut].astype(jnp.float32)
        keys = ((keys * cos_n + swap_narrow(keys) * sin_n) * KN ** (-0.5)).astype(jnp.bfloat16)
        spot = heads + 2 * g
        columns = [run_cols[:, spot + e : spot + e + 1] for e in range(2)]
        lasts = [totals[spot + e : spot + e + 1, :] for e in range(2)]
        falls = jnp.where(
            first_head, jnp.exp(lasts[0] - columns[0]), jnp.exp(lasts[1] - columns[1])
        )
        scaled = (keys.astype(jnp.float32) * falls).astype(jnp.bfloat16)
        rises = jnp.where(first_head, jnp.exp(columns[0]), jnp.exp(columns[1]))
        query_f = query.astype(jnp.float32)
        rotated[:, heads * KW + g * LANES : heads * KW + (g + 1) * LANES] = (
            query_f * rises
        ).astype(jnp.bfloat16)
        for e in range(2):
            h = 2 * g + e
            own = first_head if e == 0 else jnp.logical_not(first_head)
            masked = jnp.where(own, query_f, 0.0).astype(jnp.bfloat16)
            scores = (
                dot(masked, keys, ((1,), (1,)))
                * spread_of(columns[e], run_rows[spot + e : spot + e + 1, :])
            ).astype(jnp.bfloat16)
            values = v_narrow[:, h * VN : (h + 1) * VN]
            local[:, wide_rows + h * VN : wide_rows + (h + 1) * VN] = dot(scores, values, ((1,), (0,)))
            state = dot(scaled, values, ((0,), (0,))).astype(jnp.bfloat16)
            at = base_wide + h * KN
            states[at : at + KN, :] = state[e * KN : (e + 1) * KN, :]

    pl.semaphore_wait(barrier, count * n_tp - 1)
    spot_in = me % 4
    plane_at = z * 4

    def piece_rows(at):
        return pl.ds(pl.multiple_of(at * piece, 16), piece)

    def mate(k):
        return (spot_in + k) % 4

    def one_copy(k):
        return remote(
            states.at[piece_rows(mate(k))], got.at[spot_in], one_send.at[k], one_recv.at[k],
            plane_at + mate(k), core,
        )

    for k in range(1, 4):
        one_copy(k).start()
    lax.fori_loop(1, count, send_logs, 0)
    got[spot_in] = states[piece_rows(spot_in), :]
    turn(0)
    send_weights(0, 2, 2)
    taps_all[...] = jnp.zeros_like(taps_all)
    taps_all[0 : reach + 1, :] = taps_gate[...].astype(jnp.float32)
    taps_all[reach + 1 : 2 * (reach + 1), :] = taps_lin[...].astype(jnp.float32)
    taps_mine = pltpu.roll(taps_all[...], (share * places - place * share) % (share * places), 1)[:, :units]
    taps_lane = lax.broadcasted_iota(jnp.int32, taps_own.shape, 1)
    taps_mine = jnp.where(taps_lane < share, taps_mine, 0.0)
    taps_own[...] = jnp.where(core == 0, taps_mine, pltpu.roll(taps_mine, share, 1))
    taps_copy = remote(taps_own, taps_got, tap_sem.at[0], tap_sem.at[1], me, other)
    taps_copy.start()

    def source(k):
        return (me + count - k) % count

    def wait_logs(k, carried_):
        at = source(k)
        remote(logs.at[at], logs.at[at], log_send.at[k], log_recv.at[k], at, core).wait_recv()
        return carried_

    for k in range(1, 4):
        at = (spot_in + 4 - k) % 4
        remote(got.at[at], got.at[at], one_send.at[k], one_recv.at[k], plane_at + at, core).wait_recv()
    lax.fori_loop(1, count, wait_logs, 0)
    fades[...] = jnp.exp(logs[...])
    groups_wide = VW // LANES * KW // 16
    groups_narrow = KN // 16

    def head_of(i):
        g = spot_in * (piece // 16) + i
        head = jnp.where(
            g < heads * groups_wide, g // groups_wide,
            heads + (g - heads * groups_wide) // groups_narrow,
        )
        return jnp.minimum(head, 2 * heads - 1)

    def fade_of(chip, i):
        return fades[chip, pl.ds(head_of(i), 1), :]

    for i in range(piece // 16):
        cut = slice(i * 16, (i + 1) * 16)
        total = got[0, cut, :].astype(jnp.float32)
        for t in range(1, 4):
            total = total * fade_of(plane_at + t, i) + got[t, cut, :].astype(jnp.float32)
        plane_sum[cut, :] = total.astype(jnp.bfloat16)

    def plane_copy(k):
        return remote(plane_sum, planes.at[z], z_sum_send.at[k], z_sum_recv.at[k], me + 4 * k, core)

    for k in range(1, nz):
        @pl.when(z + k < nz)
        def _():
            plane_copy(k).start()
    carry[...] = jnp.zeros_like(carry)
    turn(1)
    turn(2)

    def add_plane(at, carried_):
        k = z - at
        remote(planes.at[at], planes.at[at], z_sum_send.at[k], z_sum_recv.at[k], me - 4 * k, core).wait_recv()
        for i in range(piece // 16):
            cut = slice(i * 16, (i + 1) * 16)
            fade = fade_of(at * 4, i)
            for t in range(1, 4):
                fade = fade * fade_of(at * 4 + t, i)
            carry[cut, :] = carry[cut, :] * fade + planes[at, cut, :].astype(jnp.float32)
        return carried_

    lax.fori_loop(0, z, add_plane, 0)
    for i in range(piece // 16):
        cut = slice(i * 16, (i + 1) * 16)
        total = carry[cut, :]
        for t in range(4):
            before[t, cut, :] = total.astype(jnp.bfloat16)
            if t < 3:
                total = total * fade_of(plane_at + t, i) + got[t, cut, :].astype(jnp.float32)

    def two_copy(k):
        return remote(
            before.at[mate(k)], state_in.at[piece_rows(spot_in)], two_send.at[k], two_recv.at[k],
            plane_at + mate(k), core,
        )

    for k in range(1, 4):
        two_copy(k).start()
    state_in[piece_rows(spot_in), :] = before[spot_in]
    send_weights(0, 1, 2)
    send_weights(1)
    forward_weights(0, 0, 2)
    for copy in late_copies + out_copies:
        copy.wait()

    for k in range(1, 4):
        at = (spot_in + 4 - k) % 4
        spot = state_in.at[piece_rows(at)]
        remote(spot, spot, two_send.at[k], two_recv.at[k], plane_at + at, core).wait_recv()

    def gate_head(retained, gain, gate):
        centred = retained - jnp.mean(retained, axis=-1, keepdims=True)
        variance = jnp.mean(centred * centred, axis=-1, keepdims=True)
        normed = centred * lax.rsqrt(variance + EPS)
        return (normed * gain * silu(gate.astype(jnp.float32))).astype(jnp.bfloat16)

    for h in range(heads):
        lifted = rotated[:, h * KW : (h + 1) * KW]
        crosses = []
        for e in range(VW // LANES):
            at = (h * (VW // LANES) + e) * KW
            crosses.append(dot(lifted, state_in[at : at + KW, :], ((1,), (0,))))
        cut = slice(h * VW, (h + 1) * VW)
        gated[:, cut] = gate_head(
            local[:, cut] + jnp.concatenate(crosses, axis=1), gain_wide[cut].astype(jnp.float32).reshape(1, -1), gate_wide[:, cut]
        )
    for h in range(heads):
        g, e = h // 2, h % 2
        own = first_head if e == 0 else jnp.logical_not(first_head)
        lifted = rotated[:, heads * KW + g * LANES : heads * KW + (g + 1) * LANES]
        lifted = jnp.where(own, lifted.astype(jnp.float32), 0.0).astype(jnp.bfloat16)
        at = base_wide + g * LANES
        cross = dot(lifted, state_in[at : at + LANES, :], ((1,), (0,)))
        cut = slice(h * VN, (h + 1) * VN)
        spot = slice(wide_rows + h * VN, wide_rows + (h + 1) * VN)
        gated[:, spot] = gate_head(local[:, spot] + cross, gain_narrow[cut].astype(jnp.float32).reshape(1, -1), gate_narrow[:, cut])

    mine_f = []
    chunk = dims["chunk"]
    for n in range(width // chunk):
        cut = slice(n * chunk, (n + 1) * chunk)
        product = dot(gated[...], out_w[:, cut], ((1,), (0,))).astype(jnp.bfloat16)
        low, high = product[:half], product[half:]
        first = core == 0
        mix_sent[:, cut] = jnp.where(first, high.astype(jnp.float32), low.astype(jnp.float32)).astype(jnp.bfloat16)
        resid[:, cut] = jnp.where(first, low.astype(jnp.float32), high.astype(jnp.float32))
    mix_copy = remote(mix_sent, mix_got, mix_sem.at[0], mix_sem.at[1], me, other)
    mix_copy.start()
    mix_copy.wait_recv()
    mixed = resid[...] + mix_got[...].astype(jnp.float32)
    stay = (
        stream[...].astype(jnp.float32) + rms(mixed) * gain_mix[...].astype(jnp.float32).reshape(1, -1)
    ).astype(jnp.bfloat16).astype(jnp.float32)
    resid[...] = stay
    normed = rms(stay) * gain_pre[...].astype(jnp.float32).reshape(1, -1)
    tokens[0, pl.ds(pl.multiple_of(pad + z * half, 16), half), :] = normed.astype(jnp.bfloat16)
    span = reach * width // 16
    for r in range(reach):
        for j in range(16 // reach):
            at = r * (16 // reach) + j
            tail_f[at : at + 1, :] = normed[half - reach + r : half - reach + r + 1, j * span : (j + 1) * span]
    tail[...] = tail_f[...].astype(jnp.bfloat16)

    def block(side, at, q):
        return tokens.at[side, pl.ds(pl.multiple_of(pad + at * half + q * step_rows, 16), step_rows)]

    def flow(at, q, sems, to):
        return remote(block(0, at, q), block(0, at, q), sems.at[at, q], z_recv.at[at, q], to, core)

    def over_y(at, q):
        return remote(block(0, at, q), block(1, at, q), y_send.at[at, q], y_recv.at[at, q], y_mate, core)

    def z_wait(at, q):
        remote(block(0, at, q), block(0, at, q), up_send.at[at, q], z_recv.at[at, q], y_mate, core).wait_recv()

    def pass_on(at, q, up, down):
        if up:
            @pl.when(z < nz - 1)
            def _():
                flow(at, q, up_send, me + 4).start()
        if down:
            @pl.when(z > 0)
            def _():
                flow(at, q, dn_send, me - 4).start()
        over_y(at, q).start()

    for q in range(parts):
        pass_on(z, q, True, True)

    next_chip = jnp.where(core == 0, me, (me + 1) % count)

    def halo_copy(k):
        at = (place + k) % places
        return remote(
            tail, halos.at[next_chip // 2], halo_send.at[k], halo_recv.at[next_chip // 2],
            2 * at + next_chip % 2, other,
        )

    def send_halo(k, carry):
        halo_copy(k).start()
        return carry

    lax.fori_loop(0, places, send_halo, 0)
    forward_weights(0, 1, 2)
    pass_weights(0)
    forward_weights(1)

    for h in range(1, nz):
        for q in range(parts):
            @pl.when(z - h >= 0)
            def _():
                z_wait(z - h, q)
                pass_on(z - h, q, True, False)

            @pl.when(z + h < nz)
            def _():
                z_wait(z + h, q)
                pass_on(z + h, q, False, True)
            if h == nz - 1 and q > 0:
                forward_weights(2, places // 2 + q - 1, 1, places // 2 + q)

        if h == 1:
            send_weights(2)
            forward_weights(2, 0, 1, 1)
        if h == 2:
            forward_weights(2, 1, 1, places // 2)

    def wait_halo(at, carry):
        remote(halos.at[at], halos.at[at], halo_send.at[at], halo_recv.at[at], me, other).wait_recv()
        return carry

    lax.fori_loop(0, places, wait_halo, 0)
    for side in range(2):
        for at in range(nz):
            p = at * 2 + jnp.where(side == 0, y, 1 - y)
            start = jnp.logical_and(jnp.logical_and(p == 0, x == 0), core == 0)
            block_tail = halos[p].astype(jnp.float32)
            block_tail = jnp.where(start, 0.0, block_tail)
            for r in range(reach):
                for j in range(16 // reach):
                    spot = r * (16 // reach) + j
                    halo_f[side, at * reach + r : at * reach + r + 1, j * span : (j + 1) * span] = (
                        block_tail[spot : spot + 1, :]
                    )
        tokens[side, 0:pad, :] = halo_f[side].astype(jnp.bfloat16)
    pass_weights(1)
    taps_copy.wait()
    forward_weights(2, places // 2 + parts - 1)
    across_wait(0)
    across_wait(1)

    def feed(side):
        rows_in = tokens[side]
        ups = []
        for which in range(2):
            ups.append(
                dot(rows_in, weights[which], ((1,), (1,))).astype(jnp.bfloat16).astype(jnp.float32)
            )
        padded[0] = ups[0]
        padded[1] = ups[1]
        taps = taps_own[...] + taps_got[...]
        for at in range(nz):
            for u in range(units // LANES):
                cut = slice(u * LANES, (u + 1) * LANES)
                smooth = []
                for which in range(2):
                    rows_u = padded[which, pad + at * half : pad + (at + 1) * half, cut]
                    place_u = lax.broadcasted_iota(jnp.int32, (half, LANES), 0)
                    total = 0.0
                    for j in range(reach + 1):
                        back = reach - j
                        shifted = rows_u
                        if back:
                            shifted = pltpu.roll(rows_u, back, 0)
                            for r in range(back):
                                spot = at * reach + reach - back + r
                                shifted = jnp.where(
                                    place_u == r, padded[which, spot : spot + 1, cut], shifted
                                )
                        tap = which * (reach + 1) + j
                        total = total + taps[tap : tap + 1, cut] * shifted
                    smooth.append(total)
                hidden[side, at * half : (at + 1) * half, cut] = (silu(smooth[0]) * smooth[1]).astype(jnp.bfloat16)

    def down(side):
        for n in range(width // chunk):
            cut = slice(n * chunk, (n + 1) * chunk)
            terms[side, :, cut] = dot(
                hidden[side], weights[2, :, cut], ((1,), (0,))
            ).astype(jnp.bfloat16)

    feed(0)
    for at in range(nz):
        for q in range(parts):
            remote(block(1, at, q), block(1, at, q), y_send.at[at, q], y_recv.at[at, q], y_mate, core).wait_recv()
    feed(1)
    pass_weights(2)
    across_wait(2)
    down(1)

    def part_of(ref, lead, at, q):
        return ref.at[lead, pl.ds(pl.multiple_of(at * half + q * step_rows, 16), step_rows)]

    def sum_y(at, q):
        return remote(
            part_of(terms, 1, at, q), from_y.at[at, q], ry_send.at[at, q], ry_recv.at[at, q],
            y_mate, core,
        )

    def sum_z(at, q, upward):
        if upward:
            return remote(
                part_of(terms, 0, at, q), from_up.at[at, q], ru_send.at[at, q], ru_recv.at[at, q],
                me + 4, core,
            )
        return remote(
            part_of(terms, 0, at, q), from_down.at[at, q], rd_send.at[at, q], rd_recv.at[at, q],
            me - 4, core,
        )

    for h in list(range(nz - 1, 0, -1)):
        for q in range(parts):
            @pl.when(z + h < nz)
            def _():
                sum_y(z + h, q).start()

            @pl.when(z - h >= 0)
            def _():
                sum_y(z - h, q).start()
    for q in range(parts):
        sum_y(z, q).start()
    down(0)

    def rows_at(at, q):
        return pl.ds(pl.multiple_of(at * half + q * step_rows, 16), step_rows)

    def add_y(at, q):
        sum_y(at, q).wait_recv()
        terms[0, rows_at(at, q), :] = (
            terms[0, rows_at(at, q), :].astype(jnp.float32) + from_y[at, q].astype(jnp.float32)
        ).astype(jnp.bfloat16)

    def add_from(at, q, ref, sem):
        remote(ref.at[at, q], ref.at[at, q], ru_send.at[at, q], sem.at[at, q], y_mate, core).wait_recv()
        terms[0, rows_at(at, q), :] = (
            terms[0, rows_at(at, q), :].astype(jnp.float32) + ref[at, q].astype(jnp.float32)
        ).astype(jnp.bfloat16)

    for h in list(range(nz - 1, 0, -1)):
        for q in range(parts):
            @pl.when(z + h < nz)
            def _():
                add_y(z + h, q)

                @pl.when(z > 0)
                def _():
                    add_from(z + h, q, from_up, ru_recv)
                sum_z(z + h, q, True).start()

            @pl.when(z - h >= 0)
            def _():
                add_y(z - h, q)

                @pl.when(z < nz - 1)
                def _():
                    add_from(z - h, q, from_down, rd_recv)
                sum_z(z - h, q, False).start()
    for q in range(parts):
        add_y(z, q)

        @pl.when(z > 0)
        def _():
            add_from(z, q, from_up, ru_recv)

        @pl.when(z < nz - 1)
        def _():
            add_from(z, q, from_down, rd_recv)
    fed = terms[0, pl.ds(pl.multiple_of(z * half, 16), half), :].astype(jnp.float32)
    result[...] = (resid[...] + rms(fed) * gain_post[...].astype(jnp.float32).reshape(1, -1)).astype(jnp.bfloat16)

    def drain(k, carry):
        log_copy(k).wait_send()
        return carry

    lax.fori_loop(1, count, drain, 0)

    def drain_weights(k, carry):
        for which in range(3):
            weight_copy(which, k).wait_send()
        return carry

    lax.fori_loop(1, places, drain_weights, 0)

    def drain_over(k, carry):
        for which in range(3):
            over_x(which, k).wait_send()
            for side in range(2):
                across(which, side, k).wait_send()
        halo_copy(k).wait_send()
        return carry

    lax.fori_loop(0, places, drain_over, 0)
    for k in range(1, 4):
        one_copy(k).wait_send()
        two_copy(k).wait_send()
    for k in range(1, nz):
        @pl.when(z + k < nz)
        def _():
            plane_copy(k).wait_send()
    mix_copy.wait_send()

    def drain_blocks(at, carry):
        for q in range(parts):
            over_y(at, q).wait_send()
            sum_y(at, q).wait_send()

            @pl.when(jnp.logical_and(z < nz - 1, at <= z))
            def _():
                flow(at, q, up_send, me + 4).wait_send()

            @pl.when(jnp.logical_and(z > 0, at >= z))
            def _():
                flow(at, q, dn_send, me - 4).wait_send()

            @pl.when(at > z)
            def _():
                sum_z(at, q, True).wait_send()

            @pl.when(at < z)
            def _():
                sum_z(at, q, False).wait_send()
        return carry

    lax.fori_loop(0, nz, drain_blocks, 0)


def fused_layer(
    stream, q_wide, k_wide, v_wide, q_narrow, k_narrow, v_narrow, gate_wide, gate_narrow, log_decay,
    gain_wide, gain_narrow, out_wide, out_narrow, gain_mix, gain_pre, gain_post,
    weight_gate, weight_lin, weight_down, taps_gate, taps_lin,
):
    count, n_tp = lax.axis_size("sp"), lax.axis_size("tp")
    rows, width = q_wide.shape[0], stream.shape[1]
    places, nz = count // 2, count // 4
    heads = q_wide.shape[1] // KW
    columns = weight_gate.shape[1]
    share = columns // places
    units = share * n_tp
    reach = taps_gate.shape[0] - 1
    state_rows = heads * (KW * VW + KN * VN) // LANES
    piece = state_rows // 4
    tap_rows = 2 * (reach + 1)
    tap_rows += -tap_rows % 8
    half = rows // n_tp
    parts = 4
    values = out_wide.shape[0] + out_narrow.shape[0]
    dims = dict(
        count=count, n_tp=n_tp, rows=rows, width=width, share=share, piece=piece, reach=reach,
        chunk=512,
    )
    vmem = pl.BlockSpec(memory_space=pltpu.VMEM)
    anywhere = pl.BlockSpec(memory_space=pl.ANY)
    bf, f32 = jnp.bfloat16, jnp.float32
    dma = pltpu.SemaphoreType.DMA
    scratch = [
        pltpu.VMEM(stream.shape, bf),
        pltpu.VMEM(gate_wide.shape, bf),
        pltpu.VMEM(gate_narrow.shape, bf),
        pltpu.VMEM((3, weight_gate.shape[0], columns), bf),
        pltpu.VMEM((3, columns, weight_gate.shape[0]), bf),
        pltpu.VMEM((values, width), bf),
        pltpu.VMEM((3, units, width), bf),
        pltpu.VMEM((2, PAD + nz * half, width), bf),
        pltpu.VMEM((2, nz * half, width), bf),
        pltpu.VMEM((nz, parts, half // parts, width), bf),
        pltpu.VMEM((nz, parts, half // parts, width), bf),
        pltpu.VMEM((nz, parts, half // parts, width), bf),
        pltpu.VMEM((rows, heads * (KW + KN)), bf),
        pltpu.VMEM((rows, values), f32),
        pltpu.VMEM((state_rows, LANES), bf),
        pltpu.VMEM((4, piece, LANES), bf),
        pltpu.VMEM((piece, LANES), bf),
        pltpu.VMEM((nz, piece, LANES), bf),
        pltpu.VMEM((piece, LANES), f32),
        pltpu.VMEM((4, piece, LANES), bf),
        pltpu.VMEM((state_rows, LANES), bf),
        pltpu.VMEM((rows, values), bf),
        pltpu.VMEM((count, 2 * heads, LANES), f32),
        pltpu.VMEM((tap_rows, columns), f32),
        pltpu.VMEM((2 * heads, LANES), f32),
        pltpu.VMEM((count, 2 * heads, LANES), f32),
        pltpu.VMEM((tap_rows, units), f32),
        pltpu.VMEM((tap_rows, units), f32),
        pltpu.VMEM((half, width), bf),
        pltpu.VMEM((half, width), bf),
        pltpu.VMEM((half, width), f32),
        pltpu.VMEM((16, reach * width // 16), f32),
        pltpu.VMEM((16, reach * width // 16), bf),
        pltpu.VMEM((places, 16, reach * width // 16), bf),
        pltpu.VMEM((2, PAD, width), f32),
        pltpu.VMEM((2, PAD + nz * half, units), f32),
        pltpu.VMEM((2, nz * half, units), bf),
        dma((3,)), dma((3,)), dma((2,)), dma((3,)), dma((3, places)), dma((3, places)), dma((3, places)),
        dma((3, places)), dma((3, 2, places)), dma((3, 2, places)),
        dma((count,)), dma((count,)), dma((4,)), dma((4,)), dma((nz,)), dma((nz,)), dma((4,)), dma((4,)),
        dma((2,)), dma((2,)), dma((places,)), dma((places,)),
    ] + [dma((nz, parts)) for _ in range(11)]
    kernel = pl.pallas_call(
        functools.partial(layer_kernel, dims),
        out_shape=jax.ShapeDtypeStruct(stream.shape, bf),
        in_specs=[anywhere] + [vmem] * 6 + [anywhere] * 2 + [vmem] * 9 + [anywhere] * 5,
        out_specs=vmem,
        scratch_shapes=scratch,
        compiler_params=pltpu.CompilerParams(
            collective_id=0, has_side_effects=True, vmem_limit_bytes=VMEM_BYTES
        ),
    )
    return kernel(
        stream, q_wide, k_wide, v_wide, q_narrow, k_narrow, v_narrow, gate_wide, gate_narrow,
        log_decay, gain_wide, gain_narrow, gain_mix, gain_pre, gain_post,
        jnp.asarray(tables_of(count, rows)), taps_gate, taps_lin, out_wide, out_narrow,
        weight_gate, weight_lin, weight_down,
    )


def fits(stream, q_wide, log_decay, weight_gate, taps_gate):
    count, n_tp = lax.axis_size("sp"), lax.axis_size("tp")
    rows, width = q_wide.shape[0], stream.shape[1]
    if n_tp != 2 or count % 4 or count < 8 or rows != BLOCK or q_wide.shape[1] % (2 * KW):
        return False
    heads = q_wide.shape[1] // KW
    units = weight_gate.shape[1]
    state_rows = heads * (KW * VW + KN * VN) // LANES
    reach = taps_gate.shape[0] - 1
    held = units // (count // 2)
    return (
        2 * heads == 8
        and weight_gate.shape[0] == LANES
        and units % (count // 2 * 16) == 0
        and (n_tp * held) % LANES == 0
        and state_rows % (4 * 16) == 0
        and reach == 2
        and (count // 4) * reach <= PAD
        and width % 512 == 0
        and 3 * n_tp * held * width <= 5 * 2 ** 20
    )


def body(
    stream,
    wide_head_query,
    broad_attention_lookup_vectors,
    values_wide,
    query_narrow,
    keys_narrow,
    values_narrow,
    gate_wide,
    gate_narrow,
    log_decay,
    gain_wide,
    gain_narrow,
    out_wide,
    out_narrow,
    gain_mix,
    gain_pre,
    gain_post,
    weight_gate,
    weight_lin,
    weight_down,
    taps_gate,
    taps_lin,
):
    if fits(stream, wide_head_query, log_decay, weight_gate, taps_gate):
        return fused_layer(
            stream, wide_head_query, broad_attention_lookup_vectors, values_wide, query_narrow,
            keys_narrow, values_narrow, gate_wide, gate_narrow, log_decay, gain_wide, gain_narrow,
            out_wide, out_narrow, gain_mix, gain_pre, gain_post, weight_gate, weight_lin,
            weight_down, taps_gate, taps_lin,
        )
    rows = wide_head_query.shape[0]
    count = lax.axis_size("sp")
    n_tp = lax.axis_size("tp")
    width = stream.shape[1]
    units = weight_gate.shape[1]
    by_tokens = 2 * count * rows < 3 * units and units % (count * 16) == 0
    by_tokens = by_tokens and count & (count - 1) == 0
    if by_tokens:
        weights, taps = unit_slices(weight_gate, weight_lin, weight_down, taps_gate, taps_lin)
    offset = lax.axis_index("sp") * rows
    rates_wide = log_decay[0]
    rates_narrow = log_decay[1]
    rot_wide, local_wide, state_wide = kept_nearby_memory(
        wide_head_query, broad_attention_lookup_vectors, values_wide, rates_wide, KW, VW, offset
    )
    rot_narrow, local_narrow, state_narrow = kept_nearby_memory(
        query_narrow, keys_narrow, values_narrow, rates_narrow, KN, VN, offset
    )
    incoming = carried_in(
        (state_wide, state_narrow),
        (jnp.sum(rates_wide, axis=1), jnp.sum(rates_narrow, axis=1)),
        "sp",
    )
    gated_wide = gate_heads(
        local_wide + carried(rot_wide, rates_wide, incoming[0]), gain_wide, gate_wide
    )
    gated_narrow = gate_heads(
        local_narrow + carried(rot_narrow, rates_narrow, incoming[1]), gain_narrow, gate_narrow
    )
    part_wide = jnp.dot(gated_wide, out_wide, preferred_element_type=jnp.float32)
    part_narrow = jnp.dot(gated_narrow, out_narrow, preferred_element_type=jnp.float32)
    mixed = share_rows(
        (part_wide + part_narrow).astype(jnp.bfloat16).reshape(n_tp, rows // n_tp, width), "tp"
    )
    resid = (stream.astype(jnp.float32) + scale_rows(mixed, gain_mix)).astype(jnp.bfloat16)
    normed_in = scale_rows(resid.astype(jnp.float32), gain_pre).astype(jnp.bfloat16)
    if by_tokens:
        fed = feed_by_tokens(normed_in, weights, taps)
    else:
        fed = feed_by_weights(normed_in, weight_gate, weight_lin, weight_down, taps_gate, taps_lin)
    return (resid.astype(jnp.float32) + scale_rows(fed, gain_post)).astype(jnp.bfloat16)


def solution(mesh):
    in_specs = (
        P(("sp", "tp"), None),
        P("sp", "tp"),
        P("sp", "tp"),
        P("sp", "tp"),
        P("sp", "tp"),
        P("sp", "tp"),
        P("sp", "tp"),
        P("sp", "tp"),
        P("sp", "tp"),
        P(None, "tp", "sp"),
        P("tp"),
        P("tp"),
        P("tp", None),
        P("tp", None),
        P(),
        P(),
        P(),
        P("sp", "tp"),
        P("sp", "tp"),
        P("sp", "tp"),
        P(None, "tp"),
        P(None, "tp"),
    )
    out_specs = P(("sp", "tp"), None)
    return jax.shard_map(body, mesh=mesh, in_specs=in_specs, out_specs=out_specs, check_vma=False)
```

```python
import functools

import jax
import jax.numpy as jnp
import numpy as np
from jax import lax
from jax.experimental import pallas as pl
from jax.experimental.pallas import tpu as pltpu
from jax.sharding import PartitionSpec as P

KW = 128
VW = 256
KN = 64
VN = 128
BLOCK = 128


EPS = 1e-06
THETA = 10000.0
LANES = 128
PAD = 16
VMEM_BYTES = 60 * 2**20


def passed_along(value, axis, steps):
    count = lax.axis_size(axis)
    first, last = (max(0, -steps), min(count, count - steps))
    return lax.ppermute(value, axis, [(source, source + steps) for source in range(first, last)])


def rotate(block, positions):
    width = block.shape[-1]
    half = width // 2
    frequency = THETA ** (-(jnp.arange(half, dtype=jnp.float32) * 2.0 / width))
    angles = positions.astype(jnp.float32)[:, None] * frequency[None, :]
    cosine = jnp.cos(angles)[:, None, :]
    sine = jnp.sin(angles)[:, None, :]
    values = block.astype(jnp.float32)
    first = values[..., :half]
    second = values[..., half:]
    return jnp.concatenate(
        [first * cosine - second * sine, second * cosine + first * sine], axis=-1
    )


def block_step(state, inputs):
    query, keys, values, log_rate = inputs
    running = jnp.cumsum(log_rate, axis=1)
    length = running.shape[1]
    index = jnp.arange(length)
    lower = (index[:, None] >= index[None, :])[None]
    spread = jnp.where(
        lower, jnp.exp(jnp.where(lower, running[:, :, None] - running[:, None, :], 0.0)), 0.0
    )
    scores = (
        jnp.einsum("ihd,jhd->hij", query, keys, preferred_element_type=jnp.float32) * spread
    ).astype(jnp.bfloat16)
    inner = jnp.einsum("hij,jhe->ihe", scores, values, preferred_element_type=jnp.float32)
    lifted = query.astype(jnp.float32) * jnp.exp(running).T[:, :, None]
    cross = jnp.einsum("ihd,hde->ihe", lifted, state, precision=lax.Precision.HIGHEST)
    tail = running[:, -1:]
    scaled = (keys.astype(jnp.float32) * jnp.exp(tail - running).T[:, :, None]).astype(jnp.bfloat16)
    update = jnp.einsum("jhd,jhe->hde", scaled, values, preferred_element_type=jnp.float32)
    state = state * jnp.exp(tail)[:, :, None] + update
    return (state, inner + cross)


def kept_nearby_memory(query, keys, values, log_rate, head_dim, value_dim, offset):
    rows = query.shape[0]
    heads = query.shape[1] // head_dim
    positions = offset + jnp.arange(rows, dtype=jnp.int32)
    rotated_query = rotate(query.reshape(rows, heads, head_dim), positions).astype(jnp.bfloat16)
    rotated_keys = (
        rotate(keys.reshape(rows, heads, head_dim), positions) * head_dim ** (-0.5)
    ).astype(jnp.bfloat16)
    layer_groups_list = rows // BLOCK

    def split(array):
        return array.reshape(layer_groups_list, BLOCK, heads, array.shape[-1])

    rates = jnp.transpose(log_rate.reshape(heads, layer_groups_list, BLOCK), (1, 0, 2))
    start = jnp.zeros((heads, head_dim, value_dim), jnp.float32)
    inputs = (
        split(rotated_query),
        split(rotated_keys),
        split(values.reshape(rows, heads, value_dim)),
        rates,
    )
    state, outs = lax.scan(block_step, start, inputs)
    return (rotated_query, outs.reshape(rows, heads, value_dim), state)


def carried(rotated_query, log_rate, state_in):
    lifted = rotated_query.astype(jnp.float32) * jnp.exp(jnp.cumsum(log_rate, axis=1)).T[:, :, None]
    return jnp.einsum("ihd,hde->ihe", lifted, state_in, precision=lax.Precision.HIGHEST)


def gate_heads(retained, gain, gate):
    mean = jnp.mean(retained, axis=-1, keepdims=True)
    centred = retained - mean
    variance = jnp.mean(centred * centred, axis=-1, keepdims=True)
    normed = (centred * lax.rsqrt(variance + EPS)).reshape(retained.shape[0], -1)
    return (normed * gain.astype(jnp.float32) * jax.nn.silu(gate.astype(jnp.float32))).astype(
        jnp.bfloat16
    )


def scale_rows(rows, gain):
    return (
        rows
        * lax.rsqrt(jnp.mean(rows * rows, axis=-1, keepdims=True) + EPS)
        * gain.astype(jnp.float32)
    )


def causal_taps(upward, before, taps):
    width = taps.shape[0]
    total = upward.shape[0]
    padded_rows = jnp.concatenate([before, upward], axis=0).astype(jnp.float32)
    smooth = jnp.zeros((total, upward.shape[1]), jnp.float32)
    for tap_index in range(width):
        smooth = (
            smooth
            + taps[tap_index].astype(jnp.float32)[None, :]
            * padded_rows[tap_index : tap_index + total]
        )
    return smooth


def swap_blocks(blocks, axis):
    return lax.all_to_all(blocks, axis, 0, 0, tiled=False)


def share_rows(parts, axis):
    count = lax.axis_size(axis)
    place = lax.axis_index(axis)
    total = lax.dynamic_index_in_dim(parts, place, 0, False).astype(jnp.float32)
    for step in range(1, count):
        piece = lax.dynamic_index_in_dim(parts, (place + step) % count, 0, False)
        moved = lax.ppermute(piece, axis, [(i, (i + step) % count) for i in range(count)])
        total = total + moved.astype(jnp.float32)
    return total


def carried_in(states, totals, axis):
    count = lax.axis_size(axis)
    lanes = states[-1].shape[-1]
    flat = jnp.concatenate([s.reshape(-1, lanes) for s in states]).astype(jnp.bfloat16)
    rates = jnp.concatenate(
        [jnp.repeat(d, s.size // s.shape[0] // lanes) for s, d in zip(states, totals)]
    )
    share = flat.shape[0] // count
    rates = rates.reshape(count, share)
    rates = jnp.pad(rates, ((0, 0), (0, -share % lanes)))
    parts, left = [], rates
    for _ in range(3):
        parts.append(left.astype(jnp.bfloat16))
        left = left - parts[-1].astype(jnp.float32)
    parts = [part.reshape(count, -1, lanes) for part in parts]
    sent = jnp.concatenate([flat.reshape(count, share, lanes)] + parts, axis=1)
    got = swap_blocks(sent, axis).astype(jnp.float32)
    parts = jnp.split(got[:, share:], 3, axis=1)
    logs = (parts[0] + parts[1] + parts[2]).reshape(count, -1)[:, :share]
    own = got[:, :share]
    steps = jnp.arange(count)
    between = (steps[None, None] > steps[None, :, None]) & (
        steps[None, None] < steps[:, None, None]
    )
    span = jnp.sum(jnp.where(between[..., None], logs[None, None], 0.0), axis=2)
    factor = jnp.where((steps[None] < steps[:, None])[..., None], jnp.exp(span), 0.0)
    before = sum(factor[:, step, :, None] * own[step][None] for step in range(count))
    back = swap_blocks(before.astype(jnp.bfloat16), axis).reshape(-1, lanes).astype(jnp.float32)
    outs, at = [], 0
    for s in states:
        rows = s.size // lanes
        outs.append(back[at : at + rows].reshape(s.shape))
        at += rows
    return outs


def feed_by_weights(normed_in, weight_gate, weight_lin, weight_down, taps_gate, taps_lin):
    normed_all = lax.all_gather(normed_in, "tp", axis=0, tiled=True)
    rows = normed_all.shape[0]
    whole_gate, whole_lin = (
        lax.all_gather(weight_gate, "sp", axis=0, tiled=True),
        lax.all_gather(weight_lin, "sp", axis=0, tiled=True),
    )
    up_gate = jnp.dot(normed_all, whole_gate, preferred_element_type=jnp.float32).astype(
        jnp.bfloat16
    )
    up_lin = jnp.dot(normed_all, whole_lin, preferred_element_type=jnp.float32).astype(jnp.bfloat16)
    reach = taps_gate.shape[0] - 1
    before_gate, before_lin = passed_along(
        (up_gate[rows - reach :], up_lin[rows - reach :]), "sp", 1
    )
    smooth_gate = causal_taps(up_gate, before_gate, taps_gate)
    smooth_lin = causal_taps(up_lin, before_lin, taps_lin)
    hidden = (jax.nn.silu(smooth_gate) * smooth_lin).astype(jnp.bfloat16)
    terms = lax.dot_general(
        hidden,
        lax.all_gather(weight_down, "sp", axis=0, tiled=True),
        (((1,), (1,)), ((), ())),
        preferred_element_type=jnp.float32,
    )
    return lax.psum_scatter(
        terms.astype(jnp.bfloat16), "tp", scatter_dimension=0, tiled=True
    ).astype(jnp.float32)


def from_all(value, axis, dim):
    count = lax.axis_size(axis)
    found = [value]
    for step in range(1, count):
        found.append(lax.ppermute(value, axis, [(i, (i + step) % count) for i in range(count)]))
    return jnp.concatenate(found, axis=dim)


def unit_slices(weight_gate, weight_lin, weight_down, taps_gate, taps_lin):
    count = lax.axis_size("sp")
    place = lax.axis_index("sp")
    deep, units = weight_gate.shape
    share = units // count
    turned = jnp.stack([weight_gate.T, weight_lin.T, weight_down.T])
    blocks = turned.reshape(3, count, share, deep).transpose(1, 0, 2, 3)
    got = swap_blocks(blocks, "sp")
    mine = got.transpose(1, 2, 0, 3).reshape(3, share, count * deep)
    taps = jnp.stack([taps_gate, taps_lin])
    taps = lax.dynamic_slice_in_dim(taps, place * share, share, 2)
    return from_all(mine, "tp", 1), from_all(taps, "tp", 2)


def flip(value, axis, bit):
    return lax.ppermute(
        value, axis, [(i, i ^ (1 << bit)) for i in range(lax.axis_size(axis))]
    )


def bits_of(count, swapped):
    bits = list(range(count.bit_length() - 1))
    if swapped:
        bits[:2] = bits[:2][::-1]
    return bits


def gather_around(value, axis, swapped):
    bits = bits_of(lax.axis_size(axis), swapped)
    for bit in bits[::-1]:
        value = jnp.stack([value, flip(value, axis, bit)])
    order = [bits.index(bit) for bit in sorted(bits, reverse=True)]
    value = value.transpose(*order, *range(len(bits), value.ndim))
    return value.reshape(-1, *value.shape[len(bits) :])


def add_around(value, axis, swapped):
    bits = bits_of(lax.axis_size(axis), swapped)
    value = value.reshape(*[2] * len(bits), *value.shape[1:])
    dims = sorted(bits, reverse=True)
    for bit in bits:
        at = dims.index(bit)
        dims.remove(bit)
        kept = lax.index_in_dim(value, 0, at, False).astype(jnp.float32)
        sent = lax.index_in_dim(value, 1, at, False).astype(jnp.bfloat16)
        value = kept + flip(sent, axis, bit).astype(jnp.float32)
        if dims:
            value = value.astype(jnp.bfloat16)
    return value


def feed_by_tokens(normed_in, weights, taps):
    count = lax.axis_size("sp")
    n_tp = lax.axis_size("tp")
    rows, width = normed_in.shape
    place = lax.axis_index("sp")
    half = width // 2
    flat = weights[:2].reshape(-1, width)
    units = flat.shape[0] // 2
    ups = 0.0
    for part in range(2):
        cut = slice(part * half, (part + 1) * half)
        tokens = gather_around(normed_in[:, cut], "sp", part == 1)
        ups = ups + lax.dot_general(
            tokens.reshape(count * rows, half),
            flat[:, cut],
            (((1,), (1,)), ((), ())),
            preferred_element_type=jnp.float32,
        )
    ups = ups.astype(jnp.bfloat16).reshape(count, rows, 2 * units)
    reach = taps.shape[1] - 1
    tails = ups[:, rows - reach :]
    prior = lax.ppermute(tails, "tp", [(i, (i + 1) % n_tp) for i in range(n_tp)])
    prior = jnp.roll(prior.reshape(count, reach, 2, n_tp, -1), 1, axis=3).reshape(prior.shape)
    blocks = place ^ jnp.arange(count)
    follows = (blocks[:, None] == blocks[None, :] + 1).astype(jnp.bfloat16)
    shifted = jnp.dot(
        follows, prior.reshape(count, -1), preferred_element_type=jnp.float32
    ).astype(jnp.bfloat16).reshape(prior.shape)
    prior = jnp.where(lax.axis_index("tp") == 0, shifted, prior)
    padded = jnp.concatenate([prior, ups], axis=1).astype(jnp.float32)
    taps = jnp.concatenate([taps[0], taps[1]], axis=1).astype(jnp.float32)
    smooth = sum(taps[j] * padded[:, j : j + rows] for j in range(reach + 1))
    hidden = (jax.nn.silu(smooth[..., :units]) * smooth[..., units:]).astype(jnp.bfloat16)
    hidden = hidden.reshape(count * rows, units)
    sums = []
    for part in range(2):
        cut = slice(part * half, (part + 1) * half)
        terms = jnp.dot(hidden, weights[2][:, cut], preferred_element_type=jnp.float32)
        terms = terms.astype(jnp.bfloat16).reshape(count, rows, half)
        sums.append(add_around(terms, "sp", part == 1))
    return jnp.concatenate(sums, axis=1)


def tables_of(count, rows):
    def angles(positions, width):
        half = width // 2
        frequency = THETA ** (-(np.arange(half, dtype=np.float64) * 2.0 / width))
        return np.tile(positions[:, None] * frequency[None, :], (1, LANES // half))

    positions = np.concatenate([np.arange(rows), np.arange(count) * rows]).astype(np.float64)
    found = []
    for width in (KW, KN):
        turned = angles(positions, width)
        found += [np.cos(turned), np.sin(turned)]
    return np.stack(found).astype(np.float32)


def remote(source, target, sent, got, sp, tp):
    return pltpu.make_async_remote_copy(
        src_ref=source, dst_ref=target, send_sem=sent, recv_sem=got,
        device_id=(sp, tp), device_id_type=pl.DeviceIdType.MESH,
    )


def silu(value):
    return value / (1.0 + jnp.exp(-value))


def rms(value):
    return value * lax.rsqrt(jnp.mean(value * value, axis=-1, keepdims=True) + EPS)


def layer_kernel(
    dims,
    stream_hbm, q_wide, k_wide, v_wide, q_narrow, k_narrow, v_narrow, gate_wide_hbm, gate_narrow_hbm,
    decay, gain_wide, gain_narrow, gain_mix, gain_pre, gain_post, tables, taps_gate, taps_lin,
    out_wide_hbm, out_narrow_hbm, weight_gate, weight_lin, weight_down,
    result,
    stream, gate_wide, gate_narrow, raw, turned, out_w, weights, tokens, terms, from_y, from_up, from_down, rotated, local, states,
    got, plane_sum, planes, carry, before, state_in, gated, fades, taps_all, logs_own, logs, taps_own, taps_got, mix_sent, mix_got, resid, tail_f, tail, halos, halo_f,
    padded, hidden,
    late_sem, raw_sem, out_sem, own_sem, w_send, w_recv, xw_send, xw_recv, dw_send, dw_recv,
    log_send, log_recv, one_send, one_recv, z_sum_send, z_sum_recv, two_send, two_recv, tap_sem, mix_sem,
    halo_send, halo_recv, up_send, dn_send, y_send, z_recv, y_recv,
    ry_send, ry_recv, ru_send, ru_recv, rd_send, rd_recv,
):
    count, n_tp = dims["count"], dims["n_tp"]
    rows, width = dims["rows"], dims["width"]
    half = rows // n_tp
    places = count // 2
    nz = count // 4
    share = dims["share"]
    n_tiles = share * places // LANES
    units = n_tp * share
    piece = dims["piece"]
    reach = dims["reach"]
    parts = 4
    step_rows = half // parts
    pad = PAD
    me = lax.axis_index("sp")
    core = lax.axis_index("tp")
    other = 1 - core
    x = me % 2
    y = (me // 2) % 2
    z = me // 4
    place = me // 2
    x_mate = me + 1 - 2 * x
    y_mate = me + 2 - 4 * y
    mine = pl.multiple_of(me * LANES, LANES)

    def in_plane(k):
        at = (place + k) % places
        return at, 2 * at + x

    barrier = pltpu.get_barrier_semaphore()

    def greet(k, carry):
        to = (me * n_tp + core + k) % (count * n_tp)
        pl.semaphore_signal(
            barrier, inc=1, device_id=(to // n_tp, to % n_tp),
            device_id_type=pl.DeviceIdType.MESH,
        )
        return carry

    lax.fori_loop(1, count * n_tp, greet, 0)

    wide_rows = out_wide_hbm.shape[0]
    narrow_rows = out_narrow_hbm.shape[0]
    out_copies = [
        pltpu.make_async_copy(out_wide_hbm, out_w.at[pl.ds(0, wide_rows)], out_sem.at[0]),
        pltpu.make_async_copy(out_narrow_hbm, out_w.at[pl.ds(wide_rows, narrow_rows)], out_sem.at[1]),
    ]
    raw_copies = [
        pltpu.make_async_copy(source, raw.at[which], raw_sem.at[which])
        for which, source in enumerate((weight_gate, weight_lin, weight_down))
    ]
    late_copies = [
        pltpu.make_async_copy(gate_wide_hbm, gate_wide, late_sem.at[0]),
        pltpu.make_async_copy(gate_narrow_hbm, gate_narrow, late_sem.at[1]),
        pltpu.make_async_copy(stream_hbm, stream, late_sem.at[2]),
    ]
    for copy in raw_copies + late_copies + out_copies:
        copy.start()

    def own_rows(at):
        return pl.ds(pl.multiple_of(at * share, 16), share)

    core_rows = pl.ds(pl.multiple_of(core * share, 16), share)

    def weight_copy(which, k):
        at, to = in_plane(k)
        return remote(
            turned.at[which, own_rows(at)], weights.at[which, core_rows, pl.ds(mine, LANES)],
            w_send.at[which, k], w_recv.at[which, k], to, core,
        )

    def weight_wait(which, k):
        from_at = (place + places - k) % places
        columns = pl.ds(pl.multiple_of((2 * from_at + x) * LANES, LANES), LANES)
        spot = weights.at[which, core_rows, columns]
        remote(spot, spot, w_send.at[which, k], w_recv.at[which, k], x_mate, core).wait_recv()

    def over_x(which, k):
        from_at = (place + places - k) % places
        columns = pl.ds(pl.multiple_of((2 * from_at + x) * LANES, LANES), LANES)
        spot = weights.at[which, core_rows, columns]
        return remote(spot, spot, xw_send.at[which, k], xw_recv.at[which, k], x_mate, core)

    def over_x_wait(which, k):
        from_at = (place + places - k) % places
        columns = pl.ds(pl.multiple_of((2 * from_at + 1 - x) * LANES, LANES), LANES)
        spot = weights.at[which, core_rows, columns]
        remote(spot, spot, xw_send.at[which, k], xw_recv.at[which, k], x_mate, core).wait_recv()

    def columns_of(side, k):
        from_at = (place + places - k) % places
        column = 2 * from_at + (x if side == 0 else 1 - x)
        return pl.ds(pl.multiple_of(column * LANES, LANES), LANES)

    def across(which, side, k):
        spot = weights.at[which, core_rows, columns_of(side, k)]
        return remote(spot, spot, dw_send.at[which, side, k], dw_recv.at[which, side, k], me, other)

    def across_wait(which):
        other_rows = pl.ds(pl.multiple_of(other * share, 16), share)
        for side in range(2):
            def go(k, carried_):
                spot = weights.at[which, other_rows, columns_of(side, k)]
                remote(
                    spot, spot, dw_send.at[which, side, k], dw_recv.at[which, side, k], me, other
                ).wait_recv()
                return carried_
            lax.fori_loop(0, places, go, 0)

    def own_copy(which):
        return pltpu.make_async_copy(
            turned.at[which, own_rows(place)], weights.at[which, core_rows, pl.ds(mine, LANES)],
            own_sem.at[which],
        )

    def send_weights(which, first=1, step=1):
        def go(i, carried_):
            weight_copy(which, first + step * i).start()
            return carried_
        lax.fori_loop(0, (places - 1 - first) // step + 1, go, 0)

    def forward_weights(which, first=0, step=1, last=places):
        if first == 0:
            own_copy(which).wait()
            over_x(which, 0).start()
            across(which, 0, 0).start()
            first = step

        def go(i, carried_):
            k = first + step * i
            weight_wait(which, k)
            over_x(which, k).start()
            across(which, 0, k).start()
            return carried_
        lax.fori_loop(0, (last - 1 - first) // step + 1, go, 0)

    def pass_weights(which, first=0, last=places):
        def go(k, carried_):
            over_x_wait(which, k)
            across(which, 1, k).start()
            return carried_
        lax.fori_loop(first, last, go, 0)

    def turn(which):
        raw_copies[which].wait()
        for at in range(n_tiles):
            cut = slice(at * LANES, (at + 1) * LANES)
            turned[which, cut, :] = raw[which, :, cut].T
        own_copy(which).start()

    i_at = lax.broadcasted_iota(jnp.int32, (rows, rows), 0)
    j_at = lax.broadcasted_iota(jnp.int32, (rows, rows), 1)
    lower = i_at >= j_at
    lower_f = lower.astype(jnp.float32)
    upper_f = (i_at <= j_at).astype(jnp.float32)
    rates = decay[...].reshape(-1, rows)
    run_rows = lax.dot_general(
        rates, upper_f, (((1,), (0,)), ((), ())), precision=lax.Precision.HIGHEST,
        preferred_element_type=jnp.float32,
    )
    run_cols = lax.dot_general(
        lower_f, rates, (((1,), (1,)), ((), ())), precision=lax.Precision.HIGHEST,
        preferred_element_type=jnp.float32,
    )
    totals = run_rows[:, rows - 1 : rows]
    logs_own[...] = jnp.broadcast_to(totals, logs_own.shape)
    logs[me] = jnp.broadcast_to(totals, logs_own.shape)

    def peer(k):
        return (me + k) % count

    def log_copy(k):
        return remote(logs_own, logs.at[me], log_send.at[k], log_recv.at[k], peer(k), core)

    def send_logs(k, carry):
        log_copy(k).start()
        return carry

    heads = wide_rows // VW
    lane = lax.broadcasted_iota(jnp.int32, (rows, LANES), 1)

    def angle_table(first, half_width):
        cos_i, sin_i = tables[first, 0:rows, :], tables[first + 1, 0:rows, :]
        cos_o = tables[first, pl.ds(rows + me, 1), :]
        sin_o = tables[first + 1, pl.ds(rows + me, 1), :]
        cosine = cos_o * cos_i - sin_o * sin_i
        sine = sin_o * cos_i + cos_o * sin_i
        early = lane % (2 * half_width) < half_width
        return cosine, jnp.where(early, -sine, sine), early

    cos_w, sin_w, _ = angle_table(0, KW // 2)

    def dot(a, b, dims_):
        return lax.dot_general(a, b, (dims_, ((), ())), preferred_element_type=jnp.float32)

    def spread_of(column, row):
        return jnp.where(lower, jnp.exp(jnp.where(lower, column - row, 0.0)), 0.0)

    for h in range(heads):
        cut = slice(h * KW, (h + 1) * KW)
        query = q_wide[:, cut].astype(jnp.float32)
        query = (query * cos_w + pltpu.roll(query, KW // 2, 1) * sin_w).astype(jnp.bfloat16)
        keys = k_wide[:, cut].astype(jnp.float32)
        keys = ((keys * cos_w + pltpu.roll(keys, KW // 2, 1) * sin_w) * KW ** (-0.5)).astype(jnp.bfloat16)
        column, row = run_cols[:, h : h + 1], run_rows[h : h + 1, :]
        scores = (dot(query, keys, ((1,), (1,))) * spread_of(column, row)).astype(jnp.bfloat16)
        values = v_wide[:, h * VW : (h + 1) * VW]
        local[:, h * VW : (h + 1) * VW] = dot(scores, values, ((1,), (0,)))
        last = totals[h : h + 1, :]
        scaled = (keys.astype(jnp.float32) * jnp.exp(last - column)).astype(jnp.bfloat16)
        state = dot(scaled, values, ((0,), (0,))).astype(jnp.bfloat16)
        for e in range(VW // LANES):
            at = (h * (VW // LANES) + e) * KW
            states[at : at + KW, :] = state[:, e * LANES : (e + 1) * LANES]
        rotated[:, cut] = (query.astype(jnp.float32) * jnp.exp(column)).astype(jnp.bfloat16)

    cos_n, sin_n, early_n = angle_table(2, KN // 2)

    def swap_narrow(value):
        return jnp.where(
            early_n, pltpu.roll(value, LANES - KN // 2, 1), pltpu.roll(value, KN // 2, 1)
        )

    base_wide = wide_rows // LANES * KW
    first_head = lane < KN
    for g in range(heads // 2):
        cut = slice(g * LANES, (g + 1) * LANES)
        query = q_narrow[:, cut].astype(jnp.float32)
        query = (query * cos_n + swap_narrow(query) * sin_n).astype(jnp.bfloat16)
        keys = k_narrow[:, cut].astype(jnp.float32)
        keys = ((keys * cos_n + swap_narrow(keys) * sin_n) * KN ** (-0.5)).astype(jnp.bfloat16)
        spot = heads + 2 * g
        columns = [run_cols[:, spot + e : spot + e + 1] for e in range(2)]
        lasts = [totals[spot + e : spot + e + 1, :] for e in range(2)]
        falls = jnp.where(
            first_head, jnp.exp(lasts[0] - columns[0]), jnp.exp(lasts[1] - columns[1])
        )
        scaled = (keys.astype(jnp.float32) * falls).astype(jnp.bfloat16)
        rises = jnp.where(first_head, jnp.exp(columns[0]), jnp.exp(columns[1]))
        query_f = query.astype(jnp.float32)
        rotated[:, heads * KW + g * LANES : heads * KW + (g + 1) * LANES] = (
            query_f * rises
        ).astype(jnp.bfloat16)
        for e in range(2):
            h = 2 * g + e
            own = first_head if e == 0 else jnp.logical_not(first_head)
            masked = jnp.where(own, query_f, 0.0).astype(jnp.bfloat16)
            scores = (
                dot(masked, keys, ((1,), (1,)))
                * spread_of(columns[e], run_rows[spot + e : spot + e + 1, :])
            ).astype(jnp.bfloat16)
            values = v_narrow[:, h * VN : (h + 1) * VN]
            local[:, wide_rows + h * VN : wide_rows + (h + 1) * VN] = dot(scores, values, ((1,), (0,)))
            state = dot(scaled, values, ((0,), (0,))).astype(jnp.bfloat16)
            at = base_wide + h * KN
            states[at : at + KN, :] = state[e * KN : (e + 1) * KN, :]

    pl.semaphore_wait(barrier, count * n_tp - 1)
    spot_in = me % 4
    plane_at = z * 4

    def piece_rows(at):
        return pl.ds(pl.multiple_of(at * piece, 16), piece)

    def mate(k):
        return (spot_in + k) % 4

    def one_copy(k):
        return remote(
            states.at[piece_rows(mate(k))], got.at[spot_in], one_send.at[k], one_recv.at[k],
            plane_at + mate(k), core,
        )

    for k in range(1, 4):
        one_copy(k).start()
    lax.fori_loop(1, count, send_logs, 0)
    got[spot_in] = states[piece_rows(spot_in), :]
    turn(0)
    send_weights(0, 2, 2)
    taps_all[...] = jnp.zeros_like(taps_all)
    taps_all[0 : reach + 1, :] = taps_gate[...].astype(jnp.float32)
    taps_all[reach + 1 : 2 * (reach + 1), :] = taps_lin[...].astype(jnp.float32)
    taps_mine = pltpu.roll(taps_all[...], (share * places - place * share) % (share * places), 1)[:, :units]
    taps_lane = lax.broadcasted_iota(jnp.int32, taps_own.shape, 1)
    taps_mine = jnp.where(taps_lane < share, taps_mine, 0.0)
    taps_own[...] = jnp.where(core == 0, taps_mine, pltpu.roll(taps_mine, share, 1))
    taps_copy = remote(taps_own, taps_got, tap_sem.at[0], tap_sem.at[1], me, other)
    taps_copy.start()

    def source(k):
        return (me + count - k) % count

    def wait_logs(k, carried_):
        at = source(k)
        remote(logs.at[at], logs.at[at], log_send.at[k], log_recv.at[k], at, core).wait_recv()
        return carried_

    for k in range(1, 4):
        at = (spot_in + 4 - k) % 4
        remote(got.at[at], got.at[at], one_send.at[k], one_recv.at[k], plane_at + at, core).wait_recv()
    lax.fori_loop(1, count, wait_logs, 0)
    fades[...] = jnp.exp(logs[...])
    groups_wide = VW // LANES * KW // 16
    groups_narrow = KN // 16

    def head_of(i):
        g = spot_in * (piece // 16) + i
        head = jnp.where(
            g < heads * groups_wide, g // groups_wide,
            heads + (g - heads * groups_wide) // groups_narrow,
        )
        return jnp.minimum(head, 2 * heads - 1)

    def fade_of(chip, i):
        return fades[chip, pl.ds(head_of(i), 1), :]

    for i in range(piece // 16):
        cut = slice(i * 16, (i + 1) * 16)
        total = got[0, cut, :].astype(jnp.float32)
        for t in range(1, 4):
            total = total * fade_of(plane_at + t, i) + got[t, cut, :].astype(jnp.float32)
        plane_sum[cut, :] = total.astype(jnp.bfloat16)

    def plane_copy(k):
        return remote(plane_sum, planes.at[z], z_sum_send.at[k], z_sum_recv.at[k], me + 4 * k, core)

    for k in range(1, nz):
        @pl.when(z + k < nz)
        def _():
            plane_copy(k).start()
    carry[...] = jnp.zeros_like(carry)
    turn(1)
    turn(2)

    def add_plane(at, carried_):
        k = z - at
        remote(planes.at[at], planes.at[at], z_sum_send.at[k], z_sum_recv.at[k], me - 4 * k, core).wait_recv()
        for i in range(piece // 16):
            cut = slice(i * 16, (i + 1) * 16)
            fade = fade_of(at * 4, i)
            for t in range(1, 4):
                fade = fade * fade_of(at * 4 + t, i)
            carry[cut, :] = carry[cut, :] * fade + planes[at, cut, :].astype(jnp.float32)
        return carried_

    lax.fori_loop(0, z, add_plane, 0)
    for i in range(piece // 16):
        cut = slice(i * 16, (i + 1) * 16)
        total = carry[cut, :]
        for t in range(4):
            before[t, cut, :] = total.astype(jnp.bfloat16)
            if t < 3:
                total = total * fade_of(plane_at + t, i) + got[t, cut, :].astype(jnp.float32)

    def two_copy(k):
        return remote(
            before.at[mate(k)], state_in.at[piece_rows(spot_in)], two_send.at[k], two_recv.at[k],
            plane_at + mate(k), core,
        )

    for k in range(1, 4):
        two_copy(k).start()
    state_in[piece_rows(spot_in), :] = before[spot_in]
    send_weights(0, 1, 2)
    send_weights(1)
    forward_weights(0, 0, 2)
    for copy in late_copies + out_copies:
        copy.wait()

    for k in range(1, 4):
        at = (spot_in + 4 - k) % 4
        spot = state_in.at[piece_rows(at)]
        remote(spot, spot, two_send.at[k], two_recv.at[k], plane_at + at, core).wait_recv()

    def gate_head(retained, gain, gate):
        centred = retained - jnp.mean(retained, axis=-1, keepdims=True)
        variance = jnp.mean(centred * centred, axis=-1, keepdims=True)
        normed = centred * lax.rsqrt(variance + EPS)
        return (normed * gain * silu(gate.astype(jnp.float32))).astype(jnp.bfloat16)

    for h in range(heads):
        lifted = rotated[:, h * KW : (h + 1) * KW]
        crosses = []
        for e in range(VW // LANES):
            at = (h * (VW // LANES) + e) * KW
            crosses.append(dot(lifted, state_in[at : at + KW, :], ((1,), (0,))))
        cut = slice(h * VW, (h + 1) * VW)
        gated[:, cut] = gate_head(
            local[:, cut] + jnp.concatenate(crosses, axis=1), gain_wide[cut].astype(jnp.float32).reshape(1, -1), gate_wide[:, cut]
        )
    for h in range(heads):
        g, e = h // 2, h % 2
        own = first_head if e == 0 else jnp.logical_not(first_head)
        lifted = rotated[:, heads * KW + g * LANES : heads * KW + (g + 1) * LANES]
        lifted = jnp.where(own, lifted.astype(jnp.float32), 0.0).astype(jnp.bfloat16)
        at = base_wide + g * LANES
        cross = dot(lifted, state_in[at : at + LANES, :], ((1,), (0,)))
        cut = slice(h * VN, (h + 1) * VN)
        spot = slice(wide_rows + h * VN, wide_rows + (h + 1) * VN)
        gated[:, spot] = gate_head(local[:, spot] + cross, gain_narrow[cut].astype(jnp.float32).reshape(1, -1), gate_narrow[:, cut])

    mine_f = []
    chunk = dims["chunk"]
    for n in range(width // chunk):
        cut = slice(n * chunk, (n + 1) * chunk)
        product = dot(gated[...], out_w[:, cut], ((1,), (0,))).astype(jnp.bfloat16)
        low, high = product[:half], product[half:]
        first = core == 0
        mix_sent[:, cut] = jnp.where(first, high.astype(jnp.float32), low.astype(jnp.float32)).astype(jnp.bfloat16)
        resid[:, cut] = jnp.where(first, low.astype(jnp.float32), high.astype(jnp.float32))
    mix_copy = remote(mix_sent, mix_got, mix_sem.at[0], mix_sem.at[1], me, other)
    mix_copy.start()
    mix_copy.wait_recv()
    mixed = resid[...] + mix_got[...].astype(jnp.float32)
    stay = (
        stream[...].astype(jnp.float32) + rms(mixed) * gain_mix[...].astype(jnp.float32).reshape(1, -1)
    ).astype(jnp.bfloat16).astype(jnp.float32)
    resid[...] = stay
    normed = rms(stay) * gain_pre[...].astype(jnp.float32).reshape(1, -1)
    tokens[0, pl.ds(pl.multiple_of(pad + z * half, 16), half), :] = normed.astype(jnp.bfloat16)
    span = reach * width // 16
    for r in range(reach):
        for j in range(16 // reach):
            at = r * (16 // reach) + j
            tail_f[at : at + 1, :] = normed[half - reach + r : half - reach + r + 1, j * span : (j + 1) * span]
    tail[...] = tail_f[...].astype(jnp.bfloat16)

    def block(side, at, q):
        return tokens.at[side, pl.ds(pl.multiple_of(pad + at * half + q * step_rows, 16), step_rows)]

    def flow(at, q, sems, to):
        return remote(block(0, at, q), block(0, at, q), sems.at[at, q], z_recv.at[at, q], to, core)

    def over_y(at, q):
        return remote(block(0, at, q), block(1, at, q), y_send.at[at, q], y_recv.at[at, q], y_mate, core)

    def z_wait(at, q):
        remote(block(0, at, q), block(0, at, q), up_send.at[at, q], z_recv.at[at, q], y_mate, core).wait_recv()

    def pass_on(at, q, up, down):
        if up:
            @pl.when(z < nz - 1)
            def _():
                flow(at, q, up_send, me + 4).start()
        if down:
            @pl.when(z > 0)
            def _():
                flow(at, q, dn_send, me - 4).start()
        over_y(at, q).start()

    for q in range(parts):
        pass_on(z, q, True, True)

    next_chip = jnp.where(core == 0, me, (me + 1) % count)

    def halo_copy(k):
        at = (place + k) % places
        return remote(
            tail, halos.at[next_chip // 2], halo_send.at[k], halo_recv.at[next_chip // 2],
            2 * at + next_chip % 2, other,
        )

    def send_halo(k, carry):
        halo_copy(k).start()
        return carry

    lax.fori_loop(0, places, send_halo, 0)
    forward_weights(0, 1, 2)
    pass_weights(0)
    forward_weights(1)

    for h in range(1, nz):
        for q in range(parts):
            @pl.when(z - h >= 0)
            def _():
                z_wait(z - h, q)
                pass_on(z - h, q, True, False)

            @pl.when(z + h < nz)
            def _():
                z_wait(z + h, q)
                pass_on(z + h, q, False, True)
            if h == nz - 1 and q > 0:
                forward_weights(2, places // 2 + q - 1, 1, places // 2 + q)

        if h == 1:
            send_weights(2)
            forward_weights(2, 0, 1, 1)
        if h == 2:
            forward_weights(2, 1, 1, places // 2)

    def wait_halo(at, carry):
        remote(halos.at[at], halos.at[at], halo_send.at[at], halo_recv.at[at], me, other).wait_recv()
        return carry

    lax.fori_loop(0, places, wait_halo, 0)
    for side in range(2):
        for at in range(nz):
            p = at * 2 + jnp.where(side == 0, y, 1 - y)
            start = jnp.logical_and(jnp.logical_and(p == 0, x == 0), core == 0)
            block_tail = halos[p].astype(jnp.float32)
            block_tail = jnp.where(start, 0.0, block_tail)
            for r in range(reach):
                for j in range(16 // reach):
                    spot = r * (16 // reach) + j
                    halo_f[side, at * reach + r : at * reach + r + 1, j * span : (j + 1) * span] = (
                        block_tail[spot : spot + 1, :]
                    )
        tokens[side, 0:pad, :] = halo_f[side].astype(jnp.bfloat16)
    pass_weights(1)
    taps_copy.wait()
    forward_weights(2, places // 2 + parts - 1)
    across_wait(0)
    across_wait(1)

    def feed(side):
        rows_in = tokens[side]
        ups = []
        for which in range(2):
            ups.append(
                dot(rows_in, weights[which], ((1,), (1,))).astype(jnp.bfloat16).astype(jnp.float32)
            )
        padded[0] = ups[0]
        padded[1] = ups[1]
        taps = taps_own[...] + taps_got[...]
        for at in range(nz):
            for u in range(units // LANES):
                cut = slice(u * LANES, (u + 1) * LANES)
                smooth = []
                for which in range(2):
                    rows_u = padded[which, pad + at * half : pad + (at + 1) * half, cut]
                    place_u = lax.broadcasted_iota(jnp.int32, (half, LANES), 0)
                    total = 0.0
                    for j in range(reach + 1):
                        back = reach - j
                        shifted = rows_u
                        if back:
                            shifted = pltpu.roll(rows_u, back, 0)
                            for r in range(back):
                                spot = at * reach + reach - back + r
                                shifted = jnp.where(
                                    place_u == r, padded[which, spot : spot + 1, cut], shifted
                                )
                        tap = which * (reach + 1) + j
                        total = total + taps[tap : tap + 1, cut] * shifted
                    smooth.append(total)
                hidden[side, at * half : (at + 1) * half, cut] = (silu(smooth[0]) * smooth[1]).astype(jnp.bfloat16)

    def down(side):
        for n in range(width // chunk):
            cut = slice(n * chunk, (n + 1) * chunk)
            terms[side, :, cut] = dot(
                hidden[side], weights[2, :, cut], ((1,), (0,))
            ).astype(jnp.bfloat16)

    feed(0)
    for at in range(nz):
        for q in range(parts):
            remote(block(1, at, q), block(1, at, q), y_send.at[at, q], y_recv.at[at, q], y_mate, core).wait_recv()
    pass_weights(2, 0, places // 2)
    feed(1)
    pass_weights(2, places // 2)
    across_wait(2)
    down(1)

    def part_of(ref, lead, at, q):
        return ref.at[lead, pl.ds(pl.multiple_of(at * half + q * step_rows, 16), step_rows)]

    def sum_y(at, q):
        return remote(
            part_of(terms, 1, at, q), from_y.at[at, q], ry_send.at[at, q], ry_recv.at[at, q],
            y_mate, core,
        )

    def sum_z(at, q, upward):
        if upward:
            return remote(
                part_of(terms, 0, at, q), from_up.at[at, q], ru_send.at[at, q], ru_recv.at[at, q],
                me + 4, core,
            )
        return remote(
            part_of(terms, 0, at, q), from_down.at[at, q], rd_send.at[at, q], rd_recv.at[at, q],
            me - 4, core,
        )

    for h in list(range(nz - 1, 0, -1)):
        for q in range(parts):
            @pl.when(z + h < nz)
            def _():
                sum_y(z + h, q).start()

            @pl.when(z - h >= 0)
            def _():
                sum_y(z - h, q).start()
    for q in range(parts):
        sum_y(z, q).start()
    down(0)

    def rows_at(at, q):
        return pl.ds(pl.multiple_of(at * half + q * step_rows, 16), step_rows)

    def add_y(at, q):
        sum_y(at, q).wait_recv()
        terms[0, rows_at(at, q), :] = (
            terms[0, rows_at(at, q), :].astype(jnp.float32) + from_y[at, q].astype(jnp.float32)
        ).astype(jnp.bfloat16)

    def add_from(at, q, ref, sem):
        remote(ref.at[at, q], ref.at[at, q], ru_send.at[at, q], sem.at[at, q], y_mate, core).wait_recv()
        terms[0, rows_at(at, q), :] = (
            terms[0, rows_at(at, q), :].astype(jnp.float32) + ref[at, q].astype(jnp.float32)
        ).astype(jnp.bfloat16)

    for h in list(range(nz - 1, 0, -1)):
        for q in range(parts):
            @pl.when(z + h < nz)
            def _():
                add_y(z + h, q)

                @pl.when(z > 0)
                def _():
                    add_from(z + h, q, from_up, ru_recv)
                sum_z(z + h, q, True).start()

            @pl.when(z - h >= 0)
            def _():
                add_y(z - h, q)

                @pl.when(z < nz - 1)
                def _():
                    add_from(z - h, q, from_down, rd_recv)
                sum_z(z - h, q, False).start()
    for q in range(parts):
        add_y(z, q)

        @pl.when(z > 0)
        def _():
            add_from(z, q, from_up, ru_recv)

        @pl.when(z < nz - 1)
        def _():
            add_from(z, q, from_down, rd_recv)
    fed = terms[0, pl.ds(pl.multiple_of(z * half, 16), half), :].astype(jnp.float32)
    result[...] = (resid[...] + rms(fed) * gain_post[...].astype(jnp.float32).reshape(1, -1)).astype(jnp.bfloat16)

    def drain(k, carry):
        log_copy(k).wait_send()
        return carry

    lax.fori_loop(1, count, drain, 0)

    def drain_weights(k, carry):
        for which in range(3):
            weight_copy(which, k).wait_send()
        return carry

    lax.fori_loop(1, places, drain_weights, 0)

    def drain_over(k, carry):
        for which in range(3):
            over_x(which, k).wait_send()
            for side in range(2):
                across(which, side, k).wait_send()
        halo_copy(k).wait_send()
        return carry

    lax.fori_loop(0, places, drain_over, 0)
    for k in range(1, 4):
        one_copy(k).wait_send()
        two_copy(k).wait_send()
    for k in range(1, nz):
        @pl.when(z + k < nz)
        def _():
            plane_copy(k).wait_send()
    mix_copy.wait_send()

    def drain_blocks(at, carry):
        for q in range(parts):
            over_y(at, q).wait_send()
            sum_y(at, q).wait_send()

            @pl.when(jnp.logical_and(z < nz - 1, at <= z))
            def _():
                flow(at, q, up_send, me + 4).wait_send()

            @pl.when(jnp.logical_and(z > 0, at >= z))
            def _():
                flow(at, q, dn_send, me - 4).wait_send()

            @pl.when(at > z)
            def _():
                sum_z(at, q, True).wait_send()

            @pl.when(at < z)
            def _():
                sum_z(at, q, False).wait_send()
        return carry

    lax.fori_loop(0, nz, drain_blocks, 0)


def fused_layer(
    stream, q_wide, k_wide, v_wide, q_narrow, k_narrow, v_narrow, gate_wide, gate_narrow, log_decay,
    gain_wide, gain_narrow, out_wide, out_narrow, gain_mix, gain_pre, gain_post,
    weight_gate, weight_lin, weight_down, taps_gate, taps_lin,
):
    count, n_tp = lax.axis_size("sp"), lax.axis_size("tp")
    rows, width = q_wide.shape[0], stream.shape[1]
    places, nz = count // 2, count // 4
    heads = q_wide.shape[1] // KW
    columns = weight_gate.shape[1]
    share = columns // places
    units = share * n_tp
    reach = taps_gate.shape[0] - 1
    state_rows = heads * (KW * VW + KN * VN) // LANES
    piece = state_rows // 4
    tap_rows = 2 * (reach + 1)
    tap_rows += -tap_rows % 8
    half = rows // n_tp
    parts = 4
    values = out_wide.shape[0] + out_narrow.shape[0]
    dims = dict(
        count=count, n_tp=n_tp, rows=rows, width=width, share=share, piece=piece, reach=reach,
        chunk=512,
    )
    vmem = pl.BlockSpec(memory_space=pltpu.VMEM)
    anywhere = pl.BlockSpec(memory_space=pl.ANY)
    bf, f32 = jnp.bfloat16, jnp.float32
    dma = pltpu.SemaphoreType.DMA
    scratch = [
        pltpu.VMEM(stream.shape, bf),
        pltpu.VMEM(gate_wide.shape, bf),
        pltpu.VMEM(gate_narrow.shape, bf),
        pltpu.VMEM((3, weight_gate.shape[0], columns), bf),
        pltpu.VMEM((3, columns, weight_gate.shape[0]), bf),
        pltpu.VMEM((values, width), bf),
        pltpu.VMEM((3, units, width), bf),
        pltpu.VMEM((2, PAD + nz * half, width), bf),
        pltpu.VMEM((2, nz * half, width), bf),
        pltpu.VMEM((nz, parts, half // parts, width), bf),
        pltpu.VMEM((nz, parts, half // parts, width), bf),
        pltpu.VMEM((nz, parts, half // parts, width), bf),
        pltpu.VMEM((rows, heads * (KW + KN)), bf),
        pltpu.VMEM((rows, values), f32),
        pltpu.VMEM((state_rows, LANES), bf),
        pltpu.VMEM((4, piece, LANES), bf),
        pltpu.VMEM((piece, LANES), bf),
        pltpu.VMEM((nz, piece, LANES), bf),
        pltpu.VMEM((piece, LANES), f32),
        pltpu.VMEM((4, piece, LANES), bf),
        pltpu.VMEM((state_rows, LANES), bf),
        pltpu.VMEM((rows, values), bf),
        pltpu.VMEM((count, 2 * heads, LANES), f32),
        pltpu.VMEM((tap_rows, columns), f32),
        pltpu.VMEM((2 * heads, LANES), f32),
        pltpu.VMEM((count, 2 * heads, LANES), f32),
        pltpu.VMEM((tap_rows, units), f32),
        pltpu.VMEM((tap_rows, units), f32),
        pltpu.VMEM((half, width), bf),
        pltpu.VMEM((half, width), bf),
        pltpu.VMEM((half, width), f32),
        pltpu.VMEM((16, reach * width // 16), f32),
        pltpu.VMEM((16, reach * width // 16), bf),
        pltpu.VMEM((places, 16, reach * width // 16), bf),
        pltpu.VMEM((2, PAD, width), f32),
        pltpu.VMEM((2, PAD + nz * half, units), f32),
        pltpu.VMEM((2, nz * half, units), bf),
        dma((3,)), dma((3,)), dma((2,)), dma((3,)), dma((3, places)), dma((3, places)), dma((3, places)),
        dma((3, places)), dma((3, 2, places)), dma((3, 2, places)),
        dma((count,)), dma((count,)), dma((4,)), dma((4,)), dma((nz,)), dma((nz,)), dma((4,)), dma((4,)),
        dma((2,)), dma((2,)), dma((places,)), dma((places,)),
    ] + [dma((nz, parts)) for _ in range(11)]
    kernel = pl.pallas_call(
        functools.partial(layer_kernel, dims),
        out_shape=jax.ShapeDtypeStruct(stream.shape, bf),
        in_specs=[anywhere] + [vmem] * 6 + [anywhere] * 2 + [vmem] * 9 + [anywhere] * 5,
        out_specs=vmem,
        scratch_shapes=scratch,
        compiler_params=pltpu.CompilerParams(
            collective_id=0, has_side_effects=True, vmem_limit_bytes=VMEM_BYTES
        ),
    )
    return kernel(
        stream, q_wide, k_wide, v_wide, q_narrow, k_narrow, v_narrow, gate_wide, gate_narrow,
        log_decay, gain_wide, gain_narrow, gain_mix, gain_pre, gain_post,
        jnp.asarray(tables_of(count, rows)), taps_gate, taps_lin, out_wide, out_narrow,
        weight_gate, weight_lin, weight_down,
    )


def fits(stream, q_wide, log_decay, weight_gate, taps_gate):
    count, n_tp = lax.axis_size("sp"), lax.axis_size("tp")
    rows, width = q_wide.shape[0], stream.shape[1]
    if n_tp != 2 or count % 4 or count < 8 or rows != BLOCK or q_wide.shape[1] % (2 * KW):
        return False
    heads = q_wide.shape[1] // KW
    units = weight_gate.shape[1]
    state_rows = heads * (KW * VW + KN * VN) // LANES
    reach = taps_gate.shape[0] - 1
    held = units // (count // 2)
    return (
        2 * heads == 8
        and weight_gate.shape[0] == LANES
        and units % (count // 2 * 16) == 0
        and (n_tp * held) % LANES == 0
        and state_rows % (4 * 16) == 0
        and reach == 2
        and (count // 4) * reach <= PAD
        and width % 512 == 0
        and 3 * n_tp * held * width <= 5 * 2 ** 20
    )


def body(
    stream,
    wide_head_query,
    broad_attention_lookup_vectors,
    values_wide,
    query_narrow,
    keys_narrow,
    values_narrow,
    gate_wide,
    gate_narrow,
    log_decay,
    gain_wide,
    gain_narrow,
    out_wide,
    out_narrow,
    gain_mix,
    gain_pre,
    gain_post,
    weight_gate,
    weight_lin,
    weight_down,
    taps_gate,
    taps_lin,
):
    if fits(stream, wide_head_query, log_decay, weight_gate, taps_gate):
        return fused_layer(
            stream, wide_head_query, broad_attention_lookup_vectors, values_wide, query_narrow,
            keys_narrow, values_narrow, gate_wide, gate_narrow, log_decay, gain_wide, gain_narrow,
            out_wide, out_narrow, gain_mix, gain_pre, gain_post, weight_gate, weight_lin,
            weight_down, taps_gate, taps_lin,
        )
    rows = wide_head_query.shape[0]
    count = lax.axis_size("sp")
    n_tp = lax.axis_size("tp")
    width = stream.shape[1]
    units = weight_gate.shape[1]
    by_tokens = 2 * count * rows < 3 * units and units % (count * 16) == 0
    by_tokens = by_tokens and count & (count - 1) == 0
    if by_tokens:
        weights, taps = unit_slices(weight_gate, weight_lin, weight_down, taps_gate, taps_lin)
    offset = lax.axis_index("sp") * rows
    rates_wide = log_decay[0]
    rates_narrow = log_decay[1]
    rot_wide, local_wide, state_wide = kept_nearby_memory(
        wide_head_query, broad_attention_lookup_vectors, values_wide, rates_wide, KW, VW, offset
    )
    rot_narrow, local_narrow, state_narrow = kept_nearby_memory(
        query_narrow, keys_narrow, values_narrow, rates_narrow, KN, VN, offset
    )
    incoming = carried_in(
        (state_wide, state_narrow),
        (jnp.sum(rates_wide, axis=1), jnp.sum(rates_narrow, axis=1)),
        "sp",
    )
    gated_wide = gate_heads(
        local_wide + carried(rot_wide, rates_wide, incoming[0]), gain_wide, gate_wide
    )
    gated_narrow = gate_heads(
        local_narrow + carried(rot_narrow, rates_narrow, incoming[1]), gain_narrow, gate_narrow
    )
    part_wide = jnp.dot(gated_wide, out_wide, preferred_element_type=jnp.float32)
    part_narrow = jnp.dot(gated_narrow, out_narrow, preferred_element_type=jnp.float32)
    mixed = share_rows(
        (part_wide + part_narrow).astype(jnp.bfloat16).reshape(n_tp, rows // n_tp, width), "tp"
    )
    resid = (stream.astype(jnp.float32) + scale_rows(mixed, gain_mix)).astype(jnp.bfloat16)
    normed_in = scale_rows(resid.astype(jnp.float32), gain_pre).astype(jnp.bfloat16)
    if by_tokens:
        fed = feed_by_tokens(normed_in, weights, taps)
    else:
        fed = feed_by_weights(normed_in, weight_gate, weight_lin, weight_down, taps_gate, taps_lin)
    return (resid.astype(jnp.float32) + scale_rows(fed, gain_post)).astype(jnp.bfloat16)


def solution(mesh):
    in_specs = (
        P(("sp", "tp"), None),
        P("sp", "tp"),
        P("sp", "tp"),
        P("sp", "tp"),
        P("sp", "tp"),
        P("sp", "tp"),
        P("sp", "tp"),
        P("sp", "tp"),
        P("sp", "tp"),
        P(None, "tp", "sp"),
        P("tp"),
        P("tp"),
        P("tp", None),
        P("tp", None),
        P(),
        P(),
        P(),
        P("sp", "tp"),
        P("sp", "tp"),
        P("sp", "tp"),
        P(None, "tp"),
        P(None, "tp"),
    )
    out_specs = P(("sp", "tp"), None)
    return jax.shard_map(body, mesh=mesh, in_specs=in_specs, out_specs=out_specs, check_vma=False)
```
